128 devices in a mesh: sp: 16 (over z, y), tp: 8 (over x, core).
Axes of the slice: x: 4, y: 4, z: 4, core: 2. Of those that a mesh axis runs over, the one named last changes fastest.
Arguments:
- tokens: bfloat16 [4, 8192, 1024], P(None, ('sp', 'tp')), may hold values from -6 to 6
- norm_gain: float32 [1024], replicated, may hold values from 0.1 to 1.9
- x_weight: bfloat16 [1024, 1024], P('sp', 'tp'), may hold values from -0.1875 to 0.1875
- z_weight: bfloat16 [1024, 1024], P('sp', 'tp'), may hold values from -0.1875 to 0.1875
- b_weight: bfloat16 [1024, 1024], P('sp', 'tp'), may hold values from -0.1875 to 0.1875
- c_weight: bfloat16 [1024, 1024], P('sp', 'tp'), may hold values from -0.1875 to 0.1875
- dt_weight: bfloat16 [1024, 16], P('sp', 'tp'), may hold values from -0.1875 to 0.1875
- x_conv: float32 [4, 1024], P(None, 'tp'), may hold values from -3 to 3
- b_conv: float32 [4, 1024], P(None, 'tp'), may hold values from -3 to 3
- c_conv: float32 [4, 1024], P(None, 'tp'), may hold values from -3 to 3
- dt_bias: float32 [16], P('tp'), may hold values from -1 to 1
- decay_rate: float32 [16], P('tp'), may hold values from 0.15 to 3.5
- out_gain: float32 [1024], P('tp'), may hold values from 0.1 to 1.9
- out_weight: bfloat16 [1024, 1024], P('tp', 'sp'), may hold values from -0.1875 to 0.1875
Outputs:
- mixed: bfloat16 [4, 8192, 1024], P(None, ('sp', 'tp'))
The draws below stay inside these ranges and needn't reach their ends.
All inputs are finite; a program needn't handle non-finite values.
Results may differ from the reference program's by a relative error of at most 0.02.
Values may be sent and summed in bfloat16 or wider, within the bound.
A program may use at most 64 MiB of HBM per device.

```python
import math
import jax
import jax.numpy as jnp
from jax import lax

D = 1024
HEADS = 16
HEAD_P = 64
STATE = 128
GROUPS = 8
CONV = 4
BLOCK = 32
SEQS = 4
INNER = 1024
LENGTH = 8192


def shard_levels(own_key, shape, split, low, largest):
    def one(dim, shards_of):
        heights = jax.random.uniform(jax.random.fold_in(jax.random.fold_in(own_key, 6), dim), (shards_of,), jnp.float32, low / len(split), largest / len(split))
        return jnp.repeat(jnp.exp(heights), shape[dim] // shards_of).reshape((-1,) + (1,) * (len(shape) - dim - 1))

    gain = one(*split[0])
    for cut in split[1:]:
        gain = gain * one(*cut)
    return gain


def centred(rng, dims, deviation, most, split=(), kind=jnp.bfloat16):
    array = jax.random.normal(rng, dims, jnp.float32) * deviation
    if len(split) > 0:
        array = shard_levels(rng, dims, split, -0.22, 0.18) * array
    return jnp.clip(array, min=-most, max=most).astype(kind)


def setup_inputs(seed: int = 0) -> dict:
    arg_keys = jax.random.split(jax.random.key(seed), 15)
    tokens = centred(arg_keys[0], (SEQS, LENGTH, D), 1.0, 6.0, ((1, 128),))
    norm_gain = jnp.clip(1.0 + 0.18 * jax.random.normal(arg_keys[1], (D,), jnp.float32), 0.1, 1.9)
    x_weight = centred(arg_keys[2], (D, INNER), D ** -0.5, 0.1875, ((0, 16), (1, 8)))
    z_weight = centred(arg_keys[3], (D, INNER), D ** -0.5, 0.1875, ((0, 16), (1, 8)))
    b_weight = centred(arg_keys[4], (D, GROUPS * STATE), D ** -0.5, 0.1875, ((0, 16), (1, 8)))
    c_weight = centred(arg_keys[5], (D, GROUPS * STATE), D ** -0.5, 0.1875, ((0, 16), (1, 8)))
    dt_weight = centred(arg_keys[6], (D, HEADS), D ** -0.5, 0.1875, ((0, 16), (1, 8)))
    x_conv = centred(arg_keys[7], (CONV, INNER), CONV ** -0.5, 3.0, ((1, 8),), jnp.float32)
    b_conv = centred(arg_keys[8], (CONV, GROUPS * STATE), CONV ** -0.5, 3.0, ((1, 8),), jnp.float32)
    c_conv = centred(arg_keys[9], (CONV, GROUPS * STATE), CONV ** -0.5, 3.0, ((1, 8),), jnp.float32)
    dt_bias = jnp.clip(jax.random.uniform(arg_keys[10], (HEADS,), jnp.float32, -1.0, 1.0) * shard_levels(arg_keys[10], (HEADS,), ((0, 8),), -0.4, 0.0), -1.0, 1.0)
    decay_rate = jnp.clip(jnp.exp(math.log(3.5) - 3.149883 * jax.random.uniform(arg_keys[11], (HEADS,), jnp.float32) ** shard_levels(arg_keys[11], (HEADS,), ((0, 8),), -0.2, 0.2)), 0.15, 3.5)
    out_gain = jnp.clip(1.0 + 0.18 * jax.random.normal(arg_keys[12], (INNER,), jnp.float32), 0.1, 1.9)
    out_weight = centred(arg_keys[13], (INNER, D), INNER ** -0.5, 0.1875, ((0, 8), (1, 16)))
    return dict(tokens=tokens, norm_gain=norm_gain, x_weight=x_weight, z_weight=z_weight, b_weight=b_weight, c_weight=c_weight, dt_weight=dt_weight, x_conv=x_conv, b_conv=b_conv, c_conv=c_conv, dt_bias=dt_bias, decay_rate=decay_rate, out_gain=out_gain, out_weight=out_weight)


epsilon = 1e-05
precise = lax.Precision.HIGHEST

def short_conv(projected, taps):
    tap_count = taps.shape[0]
    source = projected.astype(jnp.float32)
    padded = jnp.pad(source, ((0, 0), (tap_count - 1, 0), (0, 0)))
    span_len = source.shape[1]
    running = jnp.zeros_like(source)
    for offset in range(tap_count):
        running = running + taps[offset] * padded[:, offset:offset + span_len]
    return jax.nn.silu(running)

def block_pass(inputs_dt, logdecay, b_state, c_state, per_group):
    seq_count, span_len, head_count, head_width = inputs_dt.shape
    groups, state_width = (b_state.shape[2], b_state.shape[3])
    blocks = span_len // BLOCK
    x_blocks = inputs_dt.reshape(seq_count, blocks, BLOCK, groups, per_group, head_width)
    b_blocks = b_state.reshape(seq_count, blocks, BLOCK, groups, state_width)
    c_blocks = c_state.reshape(seq_count, blocks, BLOCK, groups, state_width)
    log_blocks = logdecay.reshape(seq_count, blocks, BLOCK, groups, per_group)
    within = jnp.moveaxis(jnp.cumsum(log_blocks, axis=2), 2, -1)
    scores = jnp.einsum('sclgn,scmgn->scglm', c_blocks, b_blocks, precision=precise)
    lower_mask = jnp.tril(jnp.ones((BLOCK, BLOCK), dtype=bool))
    log_gaps = jnp.where(lower_mask, within[..., :, None] - within[..., None, :], -jnp.inf)
    weights = scores[:, :, :, None] * jnp.exp(log_gaps)
    diagonal_part = jnp.einsum('scghlm,scmghp->sclghp', weights, x_blocks, precision=precise)
    end_decay = jnp.moveaxis(jnp.exp(within[..., -1:] - within), -1, 2)
    block_states = jnp.einsum('sclgn,sclghp->scghpn', b_blocks, x_blocks * end_decay[..., None], precision=precise)
    block_decay = jnp.exp(within[..., -1])

    def advance(running_state, inputs):
        fresh_state, shrink = inputs
        return (running_state * shrink[..., None, None] + fresh_state, running_state)
    start_state = jnp.zeros((seq_count, groups, per_group, head_width, state_width), jnp.float32)
    final_state, entering = lax.scan(advance, start_state, (jnp.moveaxis(block_states, 1, 0), jnp.moveaxis(block_decay, 1, 0)))
    entering = jnp.moveaxis(entering, 0, 1)
    start_decay = jnp.moveaxis(jnp.exp(within), -1, 2)
    carried_part = jnp.einsum('sclgn,scghpn->sclghp', c_blocks, entering, precision=precise) * start_decay[..., None]
    return ((diagonal_part + carried_part).reshape(seq_count, span_len, head_count, head_width), final_state)

def reference(tokens, norm_gain, x_weight, z_weight, b_weight, c_weight, dt_weight, x_conv, b_conv, c_conv, dt_bias, decay_rate, out_gain, out_weight):
    source = tokens.astype(jnp.float32)
    normed = (source * lax.rsqrt(lax.optimization_barrier(jnp.mean(source * source, axis=-1, keepdims=True)) + epsilon) * norm_gain).astype(jnp.bfloat16)
    flattened = normed.reshape(SEQS * LENGTH, D)

    def project(weight):
        product = jnp.dot(flattened, weight, preferred_element_type=jnp.float32)
        return product.astype(jnp.bfloat16).reshape(SEQS, LENGTH, weight.shape[1])
    x_conv_out = short_conv(project(x_weight), x_conv).reshape(SEQS, LENGTH, HEADS, HEAD_P)
    b_state = short_conv(project(b_weight), b_conv).reshape(SEQS, LENGTH, GROUPS, STATE)
    c_state = short_conv(project(c_weight), c_conv).reshape(SEQS, LENGTH, GROUPS, STATE)
    z_proj = project(z_weight)
    step_dt = jax.nn.softplus(project(dt_weight).astype(jnp.float32) + dt_bias)
    logdecay = -(step_dt * decay_rate) / LENGTH
    y_all, final_state = block_pass(x_conv_out * step_dt[..., None], logdecay, b_state, c_state, HEADS // GROUPS)
    gate_act = jax.nn.silu(z_proj.astype(jnp.float32))
    gated = (y_all.reshape(SEQS, LENGTH, INNER) * gate_act).reshape(SEQS, LENGTH, GROUPS, INNER // GROUPS)
    gated = gated * lax.rsqrt(lax.optimization_barrier(jnp.mean(gated * gated, axis=-1, keepdims=True)) + epsilon)
    gated = (gated.reshape(SEQS, LENGTH, INNER) * out_gain).astype(jnp.bfloat16)
    mixed = jnp.dot(gated.reshape(SEQS * LENGTH, INNER), out_weight, preferred_element_type=jnp.float32)
    return mixed.astype(jnp.bfloat16).reshape(SEQS, LENGTH, D)
```

```python
import functools

import jax
import jax.numpy as jnp
from jax import lax
from jax.experimental import pallas as pl
from jax.experimental.pallas import tpu as pltpu
from jax.sharding import Mesh
from jax.sharding import PartitionSpec as P

CONV = 4
SP = ("sp_0", "sp_1")
TP = ("tp_0", "tp_1")
SP_TP = ("sp_0", "sp_1", "tp_0", "tp_1")
LENGTH = 8192
SEQS = 4
SPAN = 512
ROWS = 64
WIDTH = 1024
CHUNK = 256
LANES = 128
epsilon = 1e-05
MESH = pl.DeviceIdType.MESH
F32 = jnp.float32
BF16 = jnp.bfloat16


def remote(src, dst, send, recv, device):
    return pltpu.make_async_remote_copy(
        src_ref=src,
        dst_ref=dst,
        send_sem=send,
        recv_sem=recv,
        device_id=device,
        device_id_type=MESH,
    )


class Ring:
    def __init__(self, place, axis, block, sends, recvs, number):
        self.block, self.sends, self.recvs, self.number = block, sends, recvs, number
        self.me = place[axis]
        self.right, self.left = lax.rem(self.me + 1, 4), lax.rem(self.me + 3, 4)
        self.far = lax.rem(self.me + 2, 4)
        to = lambda i: tuple(i if k == axis else p for k, p in enumerate(place))
        self.to_right, self.to_left = to(self.right), to(self.left)

    def copy(self, ref, lane, device):
        return remote(
            ref, ref, self.sends.at[self.number, lane], self.recvs.at[self.number, lane], device
        )

    def own(self):
        self.copy(self.block(self.me, None), 0, self.to_right).start()
        self.copy(self.block(self.me, None), 1, self.to_left).start()

    def near(self):
        self.copy(self.block(self.left, None), 0, self.to_right).wait_recv()
        self.copy(self.block(self.left, 0), 2, self.to_right).start()
        self.copy(self.block(self.right, None), 1, self.to_left).wait_recv()
        self.copy(self.block(self.right, 1), 3, self.to_left).start()

    def last(self):
        self.copy(self.block(self.far, 0), 2, self.to_right).wait_recv()
        self.copy(self.block(self.far, 1), 3, self.to_left).wait_recv()

    def drain(self):
        self.copy(self.block(self.me, None), 0, self.to_right).wait_send()
        self.copy(self.block(self.me, None), 1, self.to_left).wait_send()
        self.copy(self.block(self.left, 0), 2, self.to_right).wait_send()
        self.copy(self.block(self.right, 1), 3, self.to_left).wait_send()


def half_rows(half):
    return slice(None) if half is None else slice(32 * half, 32 * half + 32)


def half_blocks(half):
    return slice(None) if half is None else slice(2 * half, 2 * half + 2)


def matmul(a, b, dims=((1,), (0,)), precision=None):
    return lax.dot_general(a, b, (dims, ((), ())), precision=precision, preferred_element_type=F32)


def silu(value):
    return value / (1.0 + jnp.exp(-value))


def kernel(
    bias_ref,
    rate_ref,
    tokens_ref,
    gain_ref,
    xw_ref,
    zw_ref,
    bw_ref,
    cw_ref,
    dw_ref,
    xt_ref,
    bt_ref,
    ct_ref,
    og_ref,
    ow_ref,
    out_ref,
    T,
    W,
    OT,
    E,
    Z,
    DT,
    CUM,
    XS,
    BS,
    CS,
    Y,
    U,
    SS,
    RS,
    SR,
    RR,
    GT,
    G,
    ring_send,
    ring_recv,
    pair_send,
    pair_recv,
    halo_send,
    halo_recv,
    state_send,
    state_recv,
    back_send,
    back_recv,
    mix_send,
    mix_recv,
    local_sem,
):
    z, y = lax.axis_index("sp_0"), lax.axis_index("sp_1")
    x, c = lax.axis_index("tp_0"), lax.axis_index("tp_1")
    place = (z, y, x, c)
    sp, tp = z * 4 + y, x * 2 + c
    other = 1 - c
    partner = (z, y, x, other)

    def sp_device(i):
        return (i // 4, lax.rem(i, 4), x, c)

    def tp_device(i):
        return (z, y, i // 2, lax.rem(i, 2))

    barrier = pltpu.get_barrier_semaphore()

    def greet_sp(k, _):
        pl.semaphore_signal(
            barrier, inc=1, device_id=sp_device(lax.rem(sp + k, 16)), device_id_type=MESH
        )
        return 0

    def greet_tp(k, _):
        pl.semaphore_signal(
            barrier, inc=1, device_id=tp_device(lax.rem(tp + k, 8)), device_id_type=MESH
        )
        return 0

    lax.fori_loop(1, 16, greet_sp, 0)
    lax.fori_loop(1, 8, greet_tp, 0)

    lane = lax.broadcasted_iota(jnp.int32, (1, LANES), 1)
    low = lane < 64

    W[z, y, :, 0:128] = xw_ref[...]
    W[z, y, :, 128:256] = bw_ref[...]
    W[z, y, :, 256:384] = cw_ref[...]
    W[z, y, :, 384:512] = zw_ref[...]
    dt_columns = dw_ref[...].astype(F32)
    W[z, y, :, 512:640] = jnp.where(low, dt_columns[:, 0:1], dt_columns[:, 1:2]).astype(BF16)

    def normed(s):
        source = tokens_ref[s].astype(F32)
        scale = lax.rsqrt(jnp.mean(source * source, axis=-1, keepdims=True) + epsilon)
        T[s, pl.ds(pl.multiple_of(tp * ROWS, ROWS), ROWS), :] = (
            source * scale * gain_ref[...]
        ).astype(BF16)

    normed(0)
    own_columns = pl.multiple_of((c * 4 + x) * LANES, LANES)
    OT[z, y, :, pl.ds(own_columns, LANES)] = ow_ref[...].astype(F32).T.astype(BF16)
    pl.semaphore_wait(barrier, 22)

    def token_block(s):
        def block(i, half):
            start = (i * 2 + c) * ROWS + (0 if half is None else 32 * half)
            rows = ROWS if half is None else 32
            return T.at[s, pl.ds(pl.multiple_of(start, 32), rows), :]

        return block

    half_start = pl.multiple_of(c * 512, 512)
    cols_a = pl.ds(half_start, 256)
    cols_b = pl.ds(pl.multiple_of(half_start + 256, 256), 256)

    ring = lambda axis, block, number: Ring(place, axis, block, ring_send, ring_recv, number)
    tokens = [ring(2, token_block(s), s) for s in range(SEQS)]
    wa1 = ring(1, lambda i, h: W.at[z, i, half_rows(h), 0:256], 4)
    wb1 = ring(0, lambda i, h: W.at[i, y, half_rows(h), 256:640], 5)
    wa2 = ring(0, lambda i, h: W.at[i, half_blocks(h), :, 0:256], 6)
    wb2 = ring(1, lambda i, h: W.at[half_blocks(h), i, :, 256:640], 7)
    ox = ring(
        2,
        lambda i, h: OT.at[
            z, y, half_rows(h), pl.ds(pl.multiple_of((c * 4 + i) * LANES, LANES), LANES)
        ],
        8,
    )
    oa1 = ring(1, lambda i, h: OT.at[z, i, half_rows(h), cols_a], 9)
    ob1 = ring(0, lambda i, h: OT.at[i, y, half_rows(h), cols_b], 10)
    oa2 = ring(0, lambda i, h: OT.at[i, half_blocks(h), :, cols_a], 11)
    ob2 = ring(1, lambda i, h: OT.at[half_blocks(h), i, :, cols_b], 12)

    def pair_copy(s, k, core):
        i, half = (
            (x, None),
            (tokens[s].left, None),
            (tokens[s].right, None),
            (tokens[s].far, 0),
            (tokens[s].far, 1),
        )[k]
        start = (i * 2 + core) * ROWS + (0 if half is None else 32 * half)
        rows = ROWS if half is None else 32
        ref = T.at[s, pl.ds(pl.multiple_of(start, 32), rows), :]
        return remote(ref, ref, pair_send.at[s, k], pair_recv.at[s, k], partner)

    def out_pair(core):
        ref = OT.at[:, :, :, pl.ds(pl.multiple_of(core * 512, 512), 512)]
        return remote(ref, ref, pair_send.at[SEQS, 0], pair_recv.at[SEQS, 0], partner)

    def token_own(s):
        tokens[s].own()
        pair_copy(s, 0, c).start()

    def token_near(s):
        tokens[s].near()
        pair_copy(s, 1, c).start()
        pair_copy(s, 2, c).start()

    def token_last(s):
        tokens[s].last()
        pair_copy(s, 3, c).start()
        pair_copy(s, 4, c).start()

    token_start = token_own
    wa1.own()
    wb1.own()
    token_start(0)
    normed(1)
    token_start(1)
    ox.own()
    normed(2)
    normed(3)
    wa1.near()
    wb1.near()
    token_near(0)
    token_start(2)
    wa1.last()
    wb1.last()
    wa2.own()
    wb2.own()
    ox.near()
    token_near(1)
    token_start(3)
    wa2.near()
    wb2.near()
    token_last(0)
    ox.last()
    oa1.own()
    ob1.own()
    token_near(2)

    bias = jnp.where(low, bias_ref[0], bias_ref[1])
    rate = jnp.where(low, rate_ref[0], rate_ref[1])
    row_at = lax.broadcasted_iota(jnp.int32, (CHUNK, CHUNK), 0)
    column_at = lax.broadcasted_iota(jnp.int32, (CHUNK, CHUNK), 1)
    lower = row_at >= column_at
    ones_below = lower.astype(F32)
    following = sp_device(lax.rem(sp + 1, 16))

    def halo(s):
        return remote(
            E.at[s, SPAN : SPAN + 8, :],
            E.at[s, 0:8, :],
            halo_send.at[s],
            halo_recv.at[s],
            following,
        )

    def project(s):
        for k in range(5):
            pair_copy(s, k, other).wait_recv()
        weights = W[...].reshape(WIDTH, 640)
        product = matmul(T[s], weights)
        E[s, 8 : SPAN + 8, :] = product[:, 0:384]
        halo(s).start()
        Z[s] = silu(product[:, 384:512])
        step = product[:, 512:640] + bias
        step = jnp.maximum(step, 0.0) + jnp.log1p(jnp.exp(-jnp.abs(step)))
        DT[s] = step
        logdecay = -(step * rate) / LENGTH
        for k in range(2):
            rows = slice(k * CHUNK, (k + 1) * CHUNK)
            CUM[s, rows, :] = matmul(ones_below, logdecay[rows], precision=lax.Precision.HIGHEST)

    def convolve(s):
        halo(s).wait_recv()
        E[s, 0:8, :] = jnp.where(sp == 0, 0.0, E[s, 0:8, :])
        for k, taps_ref in enumerate((xt_ref, bt_ref, ct_ref)):
            columns = slice(k * LANES, (k + 1) * LANES)
            running = taps_ref[0:1, :] * E[s, 5 : 5 + SPAN, columns]
            for offset in range(1, CONV):
                running = (
                    running
                    + taps_ref[offset : offset + 1, :] * E[s, 5 + offset : 5 + offset + SPAN, columns]
                )
            running = silu(running)
            if k == 0:
                XS[s] = (running * DT[s] * jnp.exp(-CUM[s])).astype(BF16)
            elif k == 1:
                BS[s] = running.astype(BF16)
            else:
                CS[s] = running.astype(BF16)

    def states(s):
        for k in range(2):
            rows = slice(k * CHUNK, (k + 1) * CHUNK)
            U[s, k] = matmul(BS[s, rows, :], XS[s, rows, :], ((0,), (0,)))
        first, second = CUM[s, CHUNK - 1 : CHUNK, :], CUM[s, SPAN - 1 : SPAN, :]
        final = jnp.exp(second) * (jnp.exp(first) * U[s, 0] + U[s, 1])
        total = jnp.broadcast_to((first + second).reshape(1, 1, LANES), (16, 8, LANES))
        SS[s] = jnp.concatenate([final.reshape(16, 8, LANES), total], axis=1).astype(BF16)

        def send(k, _):
            i = lax.rem(sp + k, 16)
            remote(
                SS.at[s, i], RS.at[s, sp], state_send.at[s], state_recv.at[s], sp_device(i)
            ).start()
            return 0

        lax.fori_loop(1, 16, send, 0)
        RS[s, sp] = SS[s, sp]

    def inside(s):
        for k in range(2):
            rows = slice(k * CHUNK, (k + 1) * CHUNK)
            scores = matmul(CS[s, rows, :], BS[s, rows, :], ((1,), (1,)))
            scores = jnp.where(lower, scores, 0.0).astype(BF16)
            Y[s, rows, :] = matmul(scores, XS[s, rows, :])

    def scan(s):
        remote(
            SS.at[s, 0:15], RS.at[s, 0:15], state_send.at[s], state_recv.at[s], partner
        ).wait_recv()
        entering = jnp.zeros((8, LANES), F32)
        for i in range(16):
            SR[s, i] = entering
            piece = RS[s, i].astype(F32)
            entering = jnp.exp(piece[8:16]) * entering + piece[0:8]

        def send(k, _):
            i = lax.rem(sp + k, 16)
            remote(
                SR.at[s, i], RR.at[s, sp], back_send.at[s], back_recv.at[s], sp_device(i)
            ).start()
            return 0

        lax.fori_loop(1, 16, send, 0)
        RR[s, sp] = SR[s, sp]

    def finish(s):
        remote(
            SR.at[s, 0:15], RR.at[s, 0:15], back_send.at[s], back_recv.at[s], partner
        ).wait_recv()
        entering = RR[s].reshape(LANES, LANES)
        for k in range(2):
            rows = slice(k * CHUNK, (k + 1) * CHUNK)
            grown = jnp.exp(CUM[s, rows, :])
            whole = grown * (Y[s, rows, :] + matmul(CS[s, rows, :], entering.astype(BF16)))
            if k == 0:
                entering = grown[CHUNK - 1 : CHUNK, :] * (entering + U[s, 0])
            gated = whole * Z[s, rows, :]
            scale = lax.rsqrt(jnp.mean(gated * gated, axis=-1, keepdims=True) + epsilon)
            GT[s, rows, :] = (gated * scale * og_ref[...]).astype(BF16)

        def send(k, _):
            i = lax.rem(tp + k, 8)
            remote(
                GT.at[s, pl.ds(pl.multiple_of(i * ROWS, ROWS), ROWS), :],
                G.at[s, :, pl.ds(own_columns, LANES)],
                mix_send.at[s],
                mix_recv.at[s],
                tp_device(i),
            ).start()
            return 0

        lax.fori_loop(1, 8, send, 0)
        own(s).start()

    def own(s):
        return pltpu.make_async_copy(
            GT.at[s, pl.ds(pl.multiple_of(tp * ROWS, ROWS), ROWS), :],
            G.at[s, :, pl.ds(own_columns, LANES)],
            local_sem.at[s],
        )

    def mixed_in(s):
        remote(
            G.at[s, :, 0:896], G.at[s, :, 0:896], mix_send.at[s], mix_recv.at[s], partner
        ).wait_recv()
        own(s).wait()

    wa2.last()
    wb2.last()
    oa1.near()
    ob1.near()
    token_last(1)
    project(0)
    token_near(3)
    oa1.last()
    ob1.last()
    oa2.own()
    ob2.own()
    convolve(0)
    states(0)
    token_last(2)
    project(1)
    oa2.near()
    ob2.near()
    convolve(1)
    states(1)
    project(2)
    token_last(3)
    convolve(2)
    states(2)
    scan(0)
    inside(0)
    scan(1)
    oa2.last()
    ob2.last()
    out_pair(c).start()
    inside(1)
    project(3)
    finish(0)
    convolve(3)
    states(3)
    scan(2)
    finish(1)
    inside(2)
    inside(3)
    finish(2)
    scan(3)
    out_pair(other).wait_recv()
    finish(3)
    for s in range(SEQS):
        mixed_in(s)
    out_weight = OT[...].reshape(WIDTH, WIDTH)
    result = matmul(G[...].reshape(SEQS * ROWS, WIDTH), out_weight, ((1,), (1,)))
    out_ref[...] = result.astype(BF16).reshape(SEQS, ROWS, WIDTH)

    for each in (*tokens, wa1, wb1, wa2, wb2, ox, oa1, ob1, oa2, ob2):
        each.drain()
    out_pair(c).wait_send()
    for s in range(SEQS):
        for k in range(5):
            pair_copy(s, k, c).wait_send()
        halo(s).wait_send()
        remote(
            SS.at[s, 0:15], RS.at[s, 0:15], state_send.at[s], state_recv.at[s], partner
        ).wait_send()
        remote(
            SR.at[s, 0:15], RR.at[s, 0:15], back_send.at[s], back_recv.at[s], partner
        ).wait_send()
        remote(
            G.at[s, :, 0:896], G.at[s, :, 0:896], mix_send.at[s], mix_recv.at[s], partner
        ).wait_send()


def local(
    tokens,
    norm_gain,
    x_weight,
    z_weight,
    b_weight,
    c_weight,
    dt_weight,
    x_conv,
    b_conv,
    c_conv,
    dt_bias,
    decay_rate,
    out_gain,
    out_weight,
):
    smem = pl.BlockSpec(memory_space=pltpu.SMEM)
    vmem = pl.BlockSpec(memory_space=pltpu.VMEM)
    dma = pltpu.SemaphoreType.DMA
    return pl.pallas_call(
        kernel,
        out_shape=jax.ShapeDtypeStruct(tokens.shape, BF16),
        in_specs=[smem, smem] + [vmem] * 12,
        out_specs=vmem,
        scratch_shapes=[
            pltpu.VMEM((SEQS, SPAN, WIDTH), BF16),
            pltpu.VMEM((4, 4, ROWS, 640), BF16),
            pltpu.VMEM((4, 4, ROWS, WIDTH), BF16),
            pltpu.VMEM((SEQS, SPAN + 8, 384), F32),
            pltpu.VMEM((SEQS, SPAN, LANES), F32),
            pltpu.VMEM((SEQS, SPAN, LANES), F32),
            pltpu.VMEM((SEQS, SPAN, LANES), F32),
            pltpu.VMEM((SEQS, SPAN, LANES), BF16),
            pltpu.VMEM((SEQS, SPAN, LANES), BF16),
            pltpu.VMEM((SEQS, SPAN, LANES), BF16),
            pltpu.VMEM((SEQS, SPAN, LANES), F32),
            pltpu.VMEM((SEQS, 2, LANES, LANES), F32),
            pltpu.VMEM((SEQS, 16, 16, LANES), BF16),
            pltpu.VMEM((SEQS, 16, 16, LANES), BF16),
            pltpu.VMEM((SEQS, 16, 8, LANES), F32),
            pltpu.VMEM((SEQS, 16, 8, LANES), F32),
            pltpu.VMEM((SEQS, SPAN, LANES), BF16),
            pltpu.VMEM((SEQS, ROWS, WIDTH), BF16),
            dma((13, 4)),
            dma((13, 4)),
            dma((SEQS + 1, 5)),
            dma((SEQS + 1, 5)),
            dma((SEQS,)),
            dma((SEQS,)),
            dma((SEQS,)),
            dma((SEQS,)),
            dma((SEQS,)),
            dma((SEQS,)),
            dma((SEQS,)),
            dma((SEQS,)),
            dma((SEQS,)),
        ],
        compiler_params=pltpu.CompilerParams(
            collective_id=0, has_side_effects=True, vmem_limit_bytes=56 * 1024 * 1024
        ),
        name="mixer",
    )(
        dt_bias,
        decay_rate,
        tokens,
        norm_gain.reshape(1, -1),
        x_weight,
        z_weight,
        b_weight,
        c_weight,
        dt_weight,
        x_conv,
        b_conv,
        c_conv,
        out_gain.reshape(1, -1),
        out_weight,
    )


def solution(mesh):
    torus = Mesh(mesh.devices.reshape(4, 4, 4, 2), SP_TP)
    return jax.shard_map(
        local,
        mesh=torus,
        in_specs=(
            P(None, SP_TP, None),
            P(),
            P(SP, TP),
            P(SP, TP),
            P(SP, TP),
            P(SP, TP),
            P(SP, TP),
            P(None, TP),
            P(None, TP),
            P(None, TP),
            P(TP),
            P(TP),
            P(TP),
            P(TP, SP),
        ),
        out_specs=P(None, SP_TP, None),
        check_vma=False,
    )
```

```python
import functools

import jax
import jax.numpy as jnp
from jax import lax
from jax.experimental import pallas as pl
from jax.experimental.pallas import tpu as pltpu
from jax.sharding import Mesh
from jax.sharding import PartitionSpec as P

CONV = 4
SP = ("sp_0", "sp_1")
TP = ("tp_0", "tp_1")
SP_TP = ("sp_0", "sp_1", "tp_0", "tp_1")
LENGTH = 8192
SEQS = 4
SPAN = 512
ROWS = 64
WIDTH = 1024
CHUNK = 256
LANES = 128
epsilon = 1e-05
MESH = pl.DeviceIdType.MESH
F32 = jnp.float32
BF16 = jnp.bfloat16


def remote(src, dst, send, recv, device):
    return pltpu.make_async_remote_copy(
        src_ref=src,
        dst_ref=dst,
        send_sem=send,
        recv_sem=recv,
        device_id=device,
        device_id_type=MESH,
    )


class Ring:
    def __init__(self, place, axis, block, sends, recvs, number):
        self.block, self.sends, self.recvs, self.number = block, sends, recvs, number
        self.me = place[axis]
        self.right, self.left = lax.rem(self.me + 1, 4), lax.rem(self.me + 3, 4)
        self.far = lax.rem(self.me + 2, 4)
        to = lambda i: tuple(i if k == axis else p for k, p in enumerate(place))
        self.to_right, self.to_left = to(self.right), to(self.left)

    def copy(self, ref, lane, device):
        return remote(
            ref, ref, self.sends.at[self.number, lane], self.recvs.at[self.number, lane], device
        )

    def own(self):
        self.copy(self.block(self.me, None), 0, self.to_right).start()
        self.copy(self.block(self.me, None), 1, self.to_left).start()

    def near(self):
        self.copy(self.block(self.left, None), 0, self.to_right).wait_recv()
        self.copy(self.block(self.left, 0), 2, self.to_right).start()
        self.copy(self.block(self.right, None), 1, self.to_left).wait_recv()
        self.copy(self.block(self.right, 1), 3, self.to_left).start()

    def last(self):
        self.copy(self.block(self.far, 0), 2, self.to_right).wait_recv()
        self.copy(self.block(self.far, 1), 3, self.to_left).wait_recv()

    def drain(self):
        self.copy(self.block(self.me, None), 0, self.to_right).wait_send()
        self.copy(self.block(self.me, None), 1, self.to_left).wait_send()
        self.copy(self.block(self.left, 0), 2, self.to_right).wait_send()
        self.copy(self.block(self.right, 1), 3, self.to_left).wait_send()


def half_rows(half):
    return slice(None) if half is None else slice(32 * half, 32 * half + 32)


def half_blocks(half):
    return slice(None) if half is None else slice(2 * half, 2 * half + 2)


def matmul(a, b, dims=((1,), (0,)), precision=None):
    return lax.dot_general(a, b, (dims, ((), ())), precision=precision, preferred_element_type=F32)


def silu(value):
    half = 0.5 * value
    return half + half * jnp.tanh(half)


def kernel(
    bias_ref,
    rate_ref,
    tokens_ref,
    gain_ref,
    xw_ref,
    zw_ref,
    bw_ref,
    cw_ref,
    dw_ref,
    xt_ref,
    bt_ref,
    ct_ref,
    og_ref,
    ow_ref,
    out_ref,
    T,
    W,
    OT,
    E,
    Z,
    DT,
    CUM,
    XS,
    BS,
    CS,
    Y,
    U,
    SS,
    RS,
    SR,
    RR,
    GT,
    G,
    ring_send,
    ring_recv,
    pair_send,
    pair_recv,
    halo_send,
    halo_recv,
    state_send,
    state_recv,
    back_send,
    back_recv,
    mix_send,
    mix_recv,
    local_sem,
):
    z, y = lax.axis_index("sp_0"), lax.axis_index("sp_1")
    x, c = lax.axis_index("tp_0"), lax.axis_index("tp_1")
    place = (z, y, x, c)
    sp, tp = z * 4 + y, x * 2 + c
    other = 1 - c
    partner = (z, y, x, other)

    def sp_device(i):
        return (i // 4, lax.rem(i, 4), x, c)

    def tp_device(i):
        return (z, y, i // 2, lax.rem(i, 2))

    barrier = pltpu.get_barrier_semaphore()
    for step in (1, 3):
        for axis in range(3):
            near = tuple(lax.rem(p + step, 4) if k == axis else p for k, p in enumerate(place))
            pl.semaphore_signal(barrier, inc=1, device_id=near, device_id_type=MESH)
    pl.semaphore_signal(barrier, inc=1, device_id=partner, device_id_type=MESH)

    lane = lax.broadcasted_iota(jnp.int32, (1, LANES), 1)
    low = lane < 64

    W[z, y, :, 0:128] = xw_ref[...]
    W[z, y, :, 128:256] = bw_ref[...]
    W[z, y, :, 256:384] = cw_ref[...]
    W[z, y, :, 384:512] = zw_ref[...]
    head_at = lax.broadcasted_iota(jnp.int32, (2, LANES), 0)
    lane_at = lax.broadcasted_iota(jnp.int32, (2, LANES), 1)
    spread = (lane_at // 64 == head_at).astype(BF16)
    W[z, y, :, 512:640] = matmul(dw_ref[...], spread, ((0,), (0,))).astype(BF16)

    def normed(s):
        source = tokens_ref[s].astype(F32)
        scale = lax.rsqrt(jnp.mean(source * source, axis=-1, keepdims=True) + epsilon)
        T[s, pl.ds(pl.multiple_of(tp * ROWS, ROWS), ROWS), :] = (
            source * scale * gain_ref[...]
        ).astype(BF16)

    normed(0)
    own_columns = pl.multiple_of((c * 4 + x) * LANES, LANES)
    OT[z, y, :, pl.ds(own_columns, LANES)] = ow_ref[...]
    pl.semaphore_wait(barrier, 7)

    def token_block(s):
        def block(i, half):
            start = (i * 2 + c) * ROWS + (0 if half is None else 32 * half)
            rows = ROWS if half is None else 32
            return T.at[s, pl.ds(pl.multiple_of(start, 32), rows), :]

        return block

    half_start = pl.multiple_of(c * 512, 512)
    cols_a = pl.ds(half_start, 256)
    cols_b = pl.ds(pl.multiple_of(half_start + 256, 256), 256)

    ring = lambda axis, block, number: Ring(place, axis, block, ring_send, ring_recv, number)
    tokens = [ring(2, token_block(s), s) for s in range(SEQS)]
    wa1 = ring(1, lambda i, h: W.at[z, i, half_rows(h), 0:256], 4)
    wb1 = ring(0, lambda i, h: W.at[i, y, half_rows(h), 256:640], 5)
    wa2 = ring(0, lambda i, h: W.at[i, half_blocks(h), :, 0:256], 6)
    wb2 = ring(1, lambda i, h: W.at[half_blocks(h), i, :, 256:640], 7)
    ox = ring(
        2,
        lambda i, h: OT.at[
            z, y, half_rows(h), pl.ds(pl.multiple_of((c * 4 + i) * LANES, LANES), LANES)
        ],
        8,
    )
    oa1 = ring(1, lambda i, h: OT.at[z, i, half_rows(h), cols_a], 9)
    ob1 = ring(0, lambda i, h: OT.at[i, y, half_rows(h), cols_b], 10)
    oa2 = ring(0, lambda i, h: OT.at[i, half_blocks(h), :, cols_a], 11)
    ob2 = ring(1, lambda i, h: OT.at[half_blocks(h), i, :, cols_b], 12)

    def pair_copy(s, k, core):
        i, half = (
            (x, None),
            (tokens[s].left, None),
            (tokens[s].right, None),
            (tokens[s].far, 0),
            (tokens[s].far, 1),
        )[k]
        start = (i * 2 + core) * ROWS + (0 if half is None else 32 * half)
        rows = ROWS if half is None else 32
        ref = T.at[s, pl.ds(pl.multiple_of(start, 32), rows), :]
        return remote(ref, ref, pair_send.at[s, k], pair_recv.at[s, k], partner)

    def out_pair(core):
        ref = OT.at[:, :, :, pl.ds(pl.multiple_of(core * 512, 512), 512)]
        return remote(ref, ref, pair_send.at[SEQS, 0], pair_recv.at[SEQS, 0], partner)

    def token_own(s):
        tokens[s].own()
        pair_copy(s, 0, c).start()

    def token_near(s):
        tokens[s].near()
        pair_copy(s, 1, c).start()
        pair_copy(s, 2, c).start()

    def token_last(s):
        tokens[s].last()
        pair_copy(s, 3, c).start()
        pair_copy(s, 4, c).start()

    wa1.own()
    wb1.own()
    ox.own()
    token_own(0)
    normed(1)
    token_own(1)
    normed(2)
    normed(3)
    wa1.near()
    wb1.near()
    wa1.last()
    wa2.own()
    wb1.last()
    wb2.own()
    token_near(0)
    token_own(2)
    ox.near()
    wa2.near()
    wb2.near()
    token_near(1)
    token_own(3)
    token_last(0)
    ox.last()
    oa1.own()
    ob1.own()
    wa2.last()
    wb2.last()

    bias = jnp.where(low, bias_ref[0], bias_ref[1])
    rate = jnp.where(low, rate_ref[0], rate_ref[1])
    row_at = lax.broadcasted_iota(jnp.int32, (CHUNK, CHUNK), 0)
    column_at = lax.broadcasted_iota(jnp.int32, (CHUNK, CHUNK), 1)
    lower = row_at >= column_at
    ones_below = lower.astype(BF16)
    tiles = [slice(k * ROWS, (k + 1) * ROWS) for k in range(SPAN // ROWS)]
    following = sp_device(lax.rem(sp + 1, 16))

    def halo(s):
        return remote(
            E.at[s, :, SPAN : SPAN + 8, :],
            E.at[s, :, 0:8, :],
            halo_send.at[s],
            halo_recv.at[s],
            following,
        )

    def project(s):
        for k in range(5):
            pair_copy(s, k, other).wait_recv()
        weights = W[...].reshape(WIDTH, 640)
        product = matmul(T[s], weights)
        for k in range(3):
            E[s, k, 8 : SPAN + 8, :] = product[:, k * LANES : (k + 1) * LANES]
        Z[s] = product[:, 384:512]
        DT[s] = product[:, 512:640]
        halo(s).start()
        for rows in tiles:
            Z[s, rows, :] = silu(Z[s, rows, :])
            step = DT[s, rows, :] + bias
            step = jnp.maximum(step, 0.0) + jnp.log1p(jnp.exp(-jnp.abs(step)))
            DT[s, rows, :] = step
            XS[s, rows, :] = (-(step * rate) / LENGTH).astype(BF16)
        for k in range(2):
            rows = slice(k * CHUNK, (k + 1) * CHUNK)
            CUM[s, rows, :] = matmul(ones_below, XS[s, rows, :])

    def convolve(s):
        halo(s).wait_recv()
        for k in range(3):
            E[s, k, 0:8, :] = jnp.where(sp == 0, 0.0, E[s, k, 0:8, :])
        for k, taps_ref in enumerate((xt_ref, bt_ref, ct_ref)):
            taps = [taps_ref[offset : offset + 1, :] for offset in range(CONV)]
            for rows in tiles:
                start = rows.start + 5
                running = taps[0] * E[s, k, start : start + ROWS, :]
                for offset in range(1, CONV):
                    first = start + offset
                    running = running + taps[offset] * E[s, k, first : first + ROWS, :]
                running = silu(running)
                if k == 0:
                    decayed = DT[s, rows, :] * jnp.exp(-CUM[s, rows, :])
                    XS[s, rows, :] = (running * decayed).astype(BF16)
                elif k == 1:
                    BS[s, rows, :] = running.astype(BF16)
                else:
                    CS[s, rows, :] = running.astype(BF16)

    def states(s):
        for k in range(2):
            rows = slice(k * CHUNK, (k + 1) * CHUNK)
            U[s, k] = matmul(BS[s, rows, :], XS[s, rows, :], ((0,), (0,)))
        first, second = CUM[s, CHUNK - 1 : CHUNK, :], CUM[s, SPAN - 1 : SPAN, :]
        final = jnp.exp(second) * (jnp.exp(first) * U[s, 0] + U[s, 1])
        total = jnp.broadcast_to((first + second).reshape(1, 1, LANES), (16, 8, LANES))
        SS[s] = jnp.concatenate([final.reshape(16, 8, LANES), total], axis=1).astype(BF16)

        def send(k, _):
            i = lax.rem(sp + k, 16)
            remote(
                SS.at[s, i], RS.at[s, sp], state_send.at[s], state_recv.at[s], sp_device(i)
            ).start()
            return 0

        lax.fori_loop(1, 16, send, 0)
        RS[s, sp] = SS[s, sp]

    def inside(s):
        for k in range(2):
            rows = slice(k * CHUNK, (k + 1) * CHUNK)
            scores = matmul(CS[s, rows, :], BS[s, rows, :], ((1,), (1,)))
            scores = jnp.where(lower, scores, 0.0).astype(BF16)
            Y[s, rows, :] = matmul(scores, XS[s, rows, :])

    def scan(s):
        remote(
            SS.at[s, 0:15], RS.at[s, 0:15], state_send.at[s], state_recv.at[s], partner
        ).wait_recv()
        entering = jnp.zeros((8, LANES), F32)
        for i in range(16):
            SR[s, i] = entering
            piece = RS[s, i].astype(F32)
            entering = jnp.exp(piece[8:16]) * entering + piece[0:8]

        def send(k, _):
            i = lax.rem(sp + k, 16)
            remote(
                SR.at[s, i], RR.at[s, sp], back_send.at[s], back_recv.at[s], sp_device(i)
            ).start()
            return 0

        lax.fori_loop(1, 16, send, 0)
        RR[s, sp] = SR[s, sp]

    def finish(s):
        remote(
            SR.at[s, 0:15], RR.at[s, 0:15], back_send.at[s], back_recv.at[s], partner
        ).wait_recv()
        entering = RR[s].reshape(LANES, LANES)
        for k in range(2):
            rows = slice(k * CHUNK, (k + 1) * CHUNK)
            Y[s, rows, :] += matmul(CS[s, rows, :], entering.astype(BF16))
            if k == 0:
                grown = jnp.exp(CUM[s, CHUNK - 1 : CHUNK, :])
                entering = grown * (entering + U[s, 0])
        for rows in tiles:
            gated = Y[s, rows, :] * jnp.exp(CUM[s, rows, :]) * Z[s, rows, :]
            scale = lax.rsqrt(jnp.mean(gated * gated, axis=-1, keepdims=True) + epsilon)
            GT[s, rows, :] = (gated * scale * og_ref[...]).astype(BF16)

        def send(k, _):
            i = lax.rem(tp + k, 8)
            remote(
                GT.at[s, pl.ds(pl.multiple_of(i * ROWS, ROWS), ROWS), :],
                G.at[s, :, pl.ds(own_columns, LANES)],
                mix_send.at[s],
                mix_recv.at[s],
                tp_device(i),
            ).start()
            return 0

        lax.fori_loop(1, 8, send, 0)
        own(s).start()

    def own(s):
        return pltpu.make_async_copy(
            GT.at[s, pl.ds(pl.multiple_of(tp * ROWS, ROWS), ROWS), :],
            G.at[s, :, pl.ds(own_columns, LANES)],
            local_sem.at[s],
        )

    def mixed_in(s):
        remote(
            G.at[s, :, 0:896], G.at[s, :, 0:896], mix_send.at[s], mix_recv.at[s], partner
        ).wait_recv()
        own(s).wait()

    def multiply(first, last):
        for s in range(first, last):
            mixed_in(s)
        gathered = G[first:last].reshape((last - first) * ROWS, WIDTH)
        result = matmul(gathered, OT[...].reshape(WIDTH, WIDTH), ((1,), (1,)))
        out_ref[first:last] = result.astype(BF16).reshape(last - first, ROWS, WIDTH)

    project(0)
    token_near(2)
    oa1.near()
    ob1.near()
    token_last(1)
    project(1)
    convolve(0)
    states(0)
    oa1.last()
    ob1.last()
    oa2.own()
    ob2.own()
    token_near(3)
    convolve(1)
    states(1)
    token_last(2)
    inside(0)
    project(2)
    scan(0)
    oa2.near()
    ob2.near()
    inside(1)
    scan(1)
    token_last(3)
    project(3)
    convolve(2)
    states(2)
    finish(0)
    convolve(3)
    states(3)
    oa2.last()
    ob2.last()
    out_pair(c).start()
    scan(2)
    finish(1)
    inside(2)
    scan(3)
    inside(3)
    finish(2)
    out_pair(other).wait_recv()
    multiply(0, 3)
    finish(3)
    multiply(3, 4)

    for each in (*tokens, wa1, wb1, wa2, wb2, ox, oa1, ob1, oa2, ob2):
        each.drain()
    out_pair(c).wait_send()
    for s in range(SEQS):
        for k in range(5):
            pair_copy(s, k, c).wait_send()
        halo(s).wait_send()
        remote(
            SS.at[s, 0:15], RS.at[s, 0:15], state_send.at[s], state_recv.at[s], partner
        ).wait_send()
        remote(
            SR.at[s, 0:15], RR.at[s, 0:15], back_send.at[s], back_recv.at[s], partner
        ).wait_send()
        remote(
            G.at[s, :, 0:896], G.at[s, :, 0:896], mix_send.at[s], mix_recv.at[s], partner
        ).wait_send()


def local(
    tokens,
    norm_gain,
    x_weight,
    z_weight,
    b_weight,
    c_weight,
    dt_weight,
    x_conv,
    b_conv,
    c_conv,
    dt_bias,
    decay_rate,
    out_gain,
    out_weight,
):
    smem = pl.BlockSpec(memory_space=pltpu.SMEM)
    vmem = pl.BlockSpec(memory_space=pltpu.VMEM)
    dma = pltpu.SemaphoreType.DMA
    return pl.pallas_call(
        kernel,
        out_shape=jax.ShapeDtypeStruct(tokens.shape, BF16),
        in_specs=[smem, smem] + [vmem] * 12,
        out_specs=vmem,
        scratch_shapes=[
            pltpu.VMEM((SEQS, SPAN, WIDTH), BF16),
            pltpu.VMEM((4, 4, ROWS, 640), BF16),
            pltpu.VMEM((4, 4, ROWS, WIDTH), BF16),
            pltpu.VMEM((SEQS, 3, SPAN + 8, LANES), F32),
            pltpu.VMEM((SEQS, SPAN, LANES), F32),
            pltpu.VMEM((SEQS, SPAN, LANES), F32),
            pltpu.VMEM((SEQS, SPAN, LANES), F32),
            pltpu.VMEM((SEQS, SPAN, LANES), BF16),
            pltpu.VMEM((SEQS, SPAN, LANES), BF16),
            pltpu.VMEM((SEQS, SPAN, LANES), BF16),
            pltpu.VMEM((SEQS, SPAN, LANES), F32),
            pltpu.VMEM((SEQS, 2, LANES, LANES), F32),
            pltpu.VMEM((SEQS, 16, 16, LANES), BF16),
            pltpu.VMEM((SEQS, 16, 16, LANES), BF16),
            pltpu.VMEM((SEQS, 16, 8, LANES), F32),
            pltpu.VMEM((SEQS, 16, 8, LANES), F32),
            pltpu.VMEM((SEQS, SPAN, LANES), BF16),
            pltpu.VMEM((SEQS, ROWS, WIDTH), BF16),
            dma((13, 4)),
            dma((13, 4)),
            dma((SEQS + 1, 5)),
            dma((SEQS + 1, 5)),
            dma((SEQS,)),
            dma((SEQS,)),
            dma((SEQS,)),
            dma((SEQS,)),
            dma((SEQS,)),
            dma((SEQS,)),
            dma((SEQS,)),
            dma((SEQS,)),
            dma((SEQS,)),
        ],
        compiler_params=pltpu.CompilerParams(
            collective_id=0, has_side_effects=True, vmem_limit_bytes=56 * 1024 * 1024
        ),
        name="mixer",
    )(
        dt_bias,
        decay_rate,
        tokens,
        norm_gain.reshape(1, -1),
        x_weight,
        z_weight,
        b_weight,
        c_weight,
        dt_weight.T,
        x_conv,
        b_conv,
        c_conv,
        out_gain.reshape(1, -1),
        out_weight.T,
    )


def solution(mesh):
    torus = Mesh(mesh.devices.reshape(4, 4, 4, 2), SP_TP)
    return jax.shard_map(
        local,
        mesh=torus,
        in_specs=(
            P(None, SP_TP, None),
            P(),
            P(SP, TP),
            P(SP, TP),
            P(SP, TP),
            P(SP, TP),
            P(SP, TP),
            P(None, TP),
            P(None, TP),
            P(None, TP),
            P(TP),
            P(TP),
            P(TP),
            P(TP, SP),
        ),
        out_specs=P(None, SP_TP, None),
        check_vma=False,
    )
```

```python
import functools

import jax
import jax.numpy as jnp
from jax import lax
from jax.experimental import pallas as pl
from jax.experimental.pallas import tpu as pltpu
from jax.sharding import Mesh
from jax.sharding import PartitionSpec as P

CONV = 4
SP = ("sp_0", "sp_1")
TP = ("tp_0", "tp_1")
SP_TP = ("sp_0", "sp_1", "tp_0", "tp_1")
LENGTH = 8192
SEQS = 4
SPAN = 512
ROWS = 64
WIDTH = 1024
CHUNK = 256
LANES = 128
epsilon = 1e-05
MESH = pl.DeviceIdType.MESH
F32 = jnp.float32
BF16 = jnp.bfloat16


def remote(src, dst, send, recv, device):
    return pltpu.make_async_remote_copy(
        src_ref=src,
        dst_ref=dst,
        send_sem=send,
        recv_sem=recv,
        device_id=device,
        device_id_type=MESH,
    )


class Ring:
    def __init__(self, place, axis, block, sends, recvs, number):
        self.block, self.sends, self.recvs, self.number = block, sends, recvs, number
        self.me = place[axis]
        self.right, self.left = lax.rem(self.me + 1, 4), lax.rem(self.me + 3, 4)
        self.far = lax.rem(self.me + 2, 4)
        to = lambda i: tuple(i if k == axis else p for k, p in enumerate(place))
        self.to_right, self.to_left = to(self.right), to(self.left)

    def copy(self, ref, lane, device):
        return remote(
            ref, ref, self.sends.at[self.number, lane], self.recvs.at[self.number, lane], device
        )

    def own(self):
        self.copy(self.block(self.me, None), 0, self.to_right).start()
        self.copy(self.block(self.me, None), 1, self.to_left).start()

    def near(self):
        self.copy(self.block(self.left, None), 0, self.to_right).wait_recv()
        self.copy(self.block(self.left, 0), 2, self.to_right).start()
        self.copy(self.block(self.right, None), 1, self.to_left).wait_recv()
        self.copy(self.block(self.right, 1), 3, self.to_left).start()

    def last(self):
        self.copy(self.block(self.far, 0), 2, self.to_right).wait_recv()
        self.copy(self.block(self.far, 1), 3, self.to_left).wait_recv()

    def drain(self):
        self.copy(self.block(self.me, None), 0, self.to_right).wait_send()
        self.copy(self.block(self.me, None), 1, self.to_left).wait_send()
        self.copy(self.block(self.left, 0), 2, self.to_right).wait_send()
        self.copy(self.block(self.right, 1), 3, self.to_left).wait_send()


def half_rows(half):
    return slice(None) if half is None else slice(32 * half, 32 * half + 32)


def half_blocks(half):
    return slice(None) if half is None else slice(2 * half, 2 * half + 2)


def matmul(a, b, dims=((1,), (0,)), precision=None):
    return lax.dot_general(a, b, (dims, ((), ())), precision=precision, preferred_element_type=F32)


def silu(value):
    half = 0.5 * value
    return half + half * jnp.tanh(half)


def kernel(
    bias_ref,
    rate_ref,
    tokens_ref,
    gain_ref,
    xw_ref,
    zw_ref,
    bw_ref,
    cw_ref,
    dw_ref,
    xt_ref,
    bt_ref,
    ct_ref,
    og_ref,
    ow_ref,
    out_ref,
    T,
    WA,
    WB,
    OY,
    O,
    E,
    Z,
    DT,
    CUM,
    XS,
    BS,
    CS,
    Y,
    U,
    SS,
    RS,
    SR,
    RR,
    GT,
    G,
    ring_send,
    ring_recv,
    pair_send,
    pair_recv,
    halo_send,
    halo_recv,
    state_send,
    state_recv,
    back_send,
    back_recv,
    mix_send,
    mix_recv,
    local_sem,
):
    z, y = lax.axis_index("sp_0"), lax.axis_index("sp_1")
    x, c = lax.axis_index("tp_0"), lax.axis_index("tp_1")
    place = (z, y, x, c)
    sp, tp = z * 4 + y, x * 2 + c
    other = 1 - c
    partner = (z, y, x, other)

    def sp_device(i):
        return (i // 4, lax.rem(i, 4), x, c)

    def tp_device(i):
        return (z, y, i // 2, lax.rem(i, 2))

    barrier = pltpu.get_barrier_semaphore()
    for step in (1, 3):
        for axis in range(3):
            near = tuple(lax.rem(p + step, 4) if k == axis else p for k, p in enumerate(place))
            pl.semaphore_signal(barrier, inc=1, device_id=near, device_id_type=MESH)
    pl.semaphore_signal(barrier, inc=1, device_id=partner, device_id_type=MESH)

    lane = lax.broadcasted_iota(jnp.int32, (1, LANES), 1)
    low = lane < 64

    WA[z, y, :, 0:128] = xw_ref[...]
    WA[z, y, :, 128:256] = bw_ref[...]
    WB[z, y, :, 0:128] = cw_ref[...]
    WB[z, y, :, 128:256] = zw_ref[...]
    head_at = lax.broadcasted_iota(jnp.int32, (2, LANES), 0)
    lane_at = lax.broadcasted_iota(jnp.int32, (2, LANES), 1)
    spread = (lane_at // 64 == head_at).astype(BF16)
    WB[z, y, :, 256:384] = matmul(dw_ref[...], spread, ((0,), (0,))).astype(BF16)

    def normed(s):
        source = tokens_ref[s].astype(F32)
        scale = lax.rsqrt(jnp.mean(source * source, axis=-1, keepdims=True) + epsilon)
        T[s, pl.ds(pl.multiple_of(tp * ROWS, ROWS), ROWS), :] = (
            source * scale * gain_ref[...]
        ).astype(BF16)

    normed(0)
    own_columns = pl.multiple_of((c * 4 + x) * LANES, LANES)
    OY[y, :, pl.ds(pl.multiple_of(x * LANES, LANES), LANES)] = ow_ref[...]
    pl.semaphore_wait(barrier, 7)

    def token_block(s):
        def block(i, half):
            start = (i * 2 + c) * ROWS + (0 if half is None else 32 * half)
            rows = ROWS if half is None else 32
            return T.at[s, pl.ds(pl.multiple_of(start, 32), rows), :]

        return block

    ring = lambda axis, block, number: Ring(place, axis, block, ring_send, ring_recv, number)
    tokens = [ring(2, token_block(s), s) for s in range(SEQS)]
    wa1 = ring(1, lambda i, h: WA.at[z, i, half_rows(h)], 4)
    wb1 = ring(0, lambda i, h: WB.at[i, y, half_rows(h)], 5)
    shifted = lambda i, k: lax.rem(i + k, 4)
    wa2 = [ring(0, lambda i, h, k=k: WA.at[i, shifted(y, k), half_rows(h)], 6 + k) for k in range(4)]
    wb2 = [ring(1, lambda i, h, k=k: WB.at[shifted(z, k), i, half_rows(h)], 10 + k) for k in range(4)]
    ox = ring(
        2,
        lambda i, h: OY.at[y, half_rows(h), pl.ds(pl.multiple_of(i * LANES, LANES), LANES)],
        14,
    )
    oy = ring(1, lambda i, h: OY.at[i, half_rows(h)], 15)
    oz = ring(
        0,
        lambda i, h: O.at[
            c,
            slice(None) if h is None else slice(256 * h, 256 * h + 256),
            pl.ds(pl.multiple_of(i * 256, 256), 256),
        ],
        16,
    )

    def pair_copy(s, k, core):
        i, half = (
            (x, None),
            (tokens[s].left, None),
            (tokens[s].right, None),
            (tokens[s].far, 0),
            (tokens[s].far, 1),
        )[k]
        start = (i * 2 + core) * ROWS + (0 if half is None else 32 * half)
        rows = ROWS if half is None else 32
        ref = T.at[s, pl.ds(pl.multiple_of(start, 32), rows), :]
        return remote(ref, ref, pair_send.at[s, k], pair_recv.at[s, k], partner)

    def out_pair(core):
        ref = O.at[core]
        return remote(ref, ref, pair_send.at[SEQS, 0], pair_recv.at[SEQS, 0], partner)

    def token_own(s):
        tokens[s].own()
        pair_copy(s, 0, c).start()

    def token_near(s):
        tokens[s].near()
        pair_copy(s, 1, c).start()
        pair_copy(s, 2, c).start()

    def token_last(s):
        tokens[s].last()
        pair_copy(s, 3, c).start()
        pair_copy(s, 4, c).start()

    wa1.own()
    wb1.own()
    wa2[0].own()
    wb2[0].own()
    ox.own()
    token_own(0)
    normed(1)
    token_own(1)
    normed(2)
    normed(3)
    wa1.near()
    wa2[1].own()
    wa2[3].own()
    wb1.near()
    wb2[1].own()
    wb2[3].own()
    wa2[0].near()
    wb2[0].near()
    ox.near()
    token_near(0)
    token_own(2)
    wa1.last()
    wa2[2].own()
    wb1.last()
    wb2[2].own()
    wa2[1].near()
    wa2[3].near()
    wb2[1].near()
    wb2[3].near()
    ox.last()
    oy.own()
    wa2[2].near()
    wb2[2].near()
    token_last(0)
    token_near(1)
    token_own(3)
    oy.near()
    wa2[0].last()
    wa2[1].last()
    wa2[3].last()
    wa2[2].last()
    wb2[0].last()
    wb2[1].last()
    wb2[3].last()
    wb2[2].last()

    bias = jnp.where(low, bias_ref[0], bias_ref[1])
    rate = jnp.where(low, rate_ref[0], rate_ref[1])
    row_at = lax.broadcasted_iota(jnp.int32, (CHUNK, CHUNK), 0)
    column_at = lax.broadcasted_iota(jnp.int32, (CHUNK, CHUNK), 1)
    lower = row_at >= column_at
    ones_below = lower.astype(BF16)
    tiles = [slice(k * ROWS, (k + 1) * ROWS) for k in range(SPAN // ROWS)]
    following = sp_device(lax.rem(sp + 1, 16))

    def halo(s):
        return remote(
            E.at[s, :, SPAN : SPAN + 8, :],
            E.at[s, :, 0:8, :],
            halo_send.at[s],
            halo_recv.at[s],
            following,
        )

    def project(s):
        for k in range(5):
            pair_copy(s, k, other).wait_recv()
        product = matmul(T[s], WA[...].reshape(WIDTH, 256))
        E[s, 0, 8 : SPAN + 8, :] = product[:, 0:128]
        E[s, 1, 8 : SPAN + 8, :] = product[:, 128:256]
        product = matmul(T[s], WB[...].reshape(WIDTH, 384))
        E[s, 2, 8 : SPAN + 8, :] = product[:, 0:128]
        Z[s] = product[:, 128:256]
        DT[s] = product[:, 256:384]
        halo(s).start()
        for rows in tiles:
            Z[s, rows, :] = silu(Z[s, rows, :])
            step = DT[s, rows, :] + bias
            step = jnp.maximum(step, 0.0) + jnp.log1p(jnp.exp(-jnp.abs(step)))
            DT[s, rows, :] = step
            XS[s, rows, :] = (-(step * rate) / LENGTH).astype(BF16)
        for k in range(2):
            rows = slice(k * CHUNK, (k + 1) * CHUNK)
            CUM[s, rows, :] = matmul(ones_below, XS[s, rows, :])

    def convolve(s):
        halo(s).wait_recv()
        for k in range(3):
            E[s, k, 0:8, :] = jnp.where(sp == 0, 0.0, E[s, k, 0:8, :])
        for k, taps_ref in enumerate((xt_ref, bt_ref, ct_ref)):
            taps = [taps_ref[offset : offset + 1, :] for offset in range(CONV)]
            for rows in tiles:
                start = rows.start + 5
                running = taps[0] * E[s, k, start : start + ROWS, :]
                for offset in range(1, CONV):
                    first = start + offset
                    running = running + taps[offset] * E[s, k, first : first + ROWS, :]
                running = silu(running)
                if k == 0:
                    decayed = DT[s, rows, :] * jnp.exp(-CUM[s, rows, :])
                    XS[s, rows, :] = (running * decayed).astype(BF16)
                elif k == 1:
                    BS[s, rows, :] = running.astype(BF16)
                else:
                    CS[s, rows, :] = running.astype(BF16)

    def states(s):
        for k in range(2):
            rows = slice(k * CHUNK, (k + 1) * CHUNK)
            U[s, k] = matmul(BS[s, rows, :], XS[s, rows, :], ((0,), (0,)))
        first, second = CUM[s, CHUNK - 1 : CHUNK, :], CUM[s, SPAN - 1 : SPAN, :]
        final = jnp.exp(second) * (jnp.exp(first) * U[s, 0] + U[s, 1])
        total = jnp.broadcast_to((first + second).reshape(1, 1, LANES), (16, 8, LANES))
        SS[s] = jnp.concatenate([final.reshape(16, 8, LANES), total], axis=1).astype(BF16)

        def send(k, _):
            i = lax.rem(sp + k, 16)
            remote(
                SS.at[s, i], RS.at[s, sp], state_send.at[s], state_recv.at[s], sp_device(i)
            ).start()
            return 0

        lax.fori_loop(1, 16, send, 0)
        RS[s, sp] = SS[s, sp]

    def inside(s):
        for k in range(2):
            rows = slice(k * CHUNK, (k + 1) * CHUNK)
            scores = matmul(CS[s, rows, :], BS[s, rows, :], ((1,), (1,)))
            scores = jnp.where(lower, scores, 0.0).astype(BF16)
            Y[s, rows, :] = matmul(scores, XS[s, rows, :])

    def scan(s):
        remote(
            SS.at[s, 0:15], RS.at[s, 0:15], state_send.at[s], state_recv.at[s], partner
        ).wait_recv()
        entering = jnp.zeros((8, LANES), F32)
        for i in range(16):
            SR[s, i] = entering
            piece = RS[s, i].astype(F32)
            entering = jnp.exp(piece[8:16]) * entering + piece[0:8]

        def send(k, _):
            i = lax.rem(sp + k, 16)
            remote(
                SR.at[s, i], RR.at[s, sp], back_send.at[s], back_recv.at[s], sp_device(i)
            ).start()
            return 0

        lax.fori_loop(1, 16, send, 0)
        RR[s, sp] = SR[s, sp]

    def finish(s):
        remote(
            SR.at[s, 0:15], RR.at[s, 0:15], back_send.at[s], back_recv.at[s], partner
        ).wait_recv()
        entering = RR[s].reshape(LANES, LANES)
        for k in range(2):
            rows = slice(k * CHUNK, (k + 1) * CHUNK)
            Y[s, rows, :] += matmul(CS[s, rows, :], entering.astype(BF16))
            if k == 0:
                grown = jnp.exp(CUM[s, CHUNK - 1 : CHUNK, :])
                entering = grown * (entering + U[s, 0])
        for rows in tiles:
            gated = Y[s, rows, :] * jnp.exp(CUM[s, rows, :]) * Z[s, rows, :]
            scale = lax.rsqrt(jnp.mean(gated * gated, axis=-1, keepdims=True) + epsilon)
            GT[s, rows, :] = (gated * scale * og_ref[...]).astype(BF16)

        def send(k, _):
            i = lax.rem(tp + k, 8)
            remote(
                GT.at[s, pl.ds(pl.multiple_of(i * ROWS, ROWS), ROWS), :],
                G.at[s, :, pl.ds(own_columns, LANES)],
                mix_send.at[s],
                mix_recv.at[s],
                tp_device(i),
            ).start()
            return 0

        lax.fori_loop(1, 8, send, 0)
        own(s).start()

    def own(s):
        return pltpu.make_async_copy(
            GT.at[s, pl.ds(pl.multiple_of(tp * ROWS, ROWS), ROWS), :],
            G.at[s, :, pl.ds(own_columns, LANES)],
            local_sem.at[s],
        )

    def mixed_in(s):
        remote(
            G.at[s, :, 0:896], G.at[s, :, 0:896], mix_send.at[s], mix_recv.at[s], partner
        ).wait_recv()
        own(s).wait()

    def multiply(first, last):
        for s in range(first, last):
            mixed_in(s)
        gathered = G[first:last].reshape((last - first) * ROWS, WIDTH)
        result = matmul(gathered, O[...].reshape(WIDTH, WIDTH))
        out_ref[first:last] = result.astype(BF16).reshape(last - first, ROWS, WIDTH)

    def turn():
        block = OY[...].reshape(256, 512).astype(F32).T.astype(BF16)
        O[c, :, pl.ds(pl.multiple_of(z * 256, 256), 256)] = block

    project(0)
    token_near(2)
    oy.last()
    turn()
    oz.own()
    token_last(1)
    project(1)
    convolve(0)
    states(0)
    token_near(3)
    oz.near()
    convolve(1)
    states(1)
    inside(0)
    token_last(2)
    project(2)
    scan(0)
    inside(1)
    scan(1)
    convolve(2)
    states(2)
    oz.last()
    out_pair(c).start()
    token_last(3)
    project(3)
    finish(0)
    finish(1)
    convolve(3)
    states(3)
    scan(2)
    inside(2)
    inside(3)
    finish(2)
    scan(3)
    out_pair(other).wait_recv()
    multiply(0, 3)
    finish(3)
    multiply(3, 4)

    for each in (*tokens, wa1, wb1, *wa2, *wb2, ox, oy, oz):
        each.drain()
    out_pair(c).wait_send()
    for s in range(SEQS):
        for k in range(5):
            pair_copy(s, k, c).wait_send()
        halo(s).wait_send()
        remote(
            SS.at[s, 0:15], RS.at[s, 0:15], state_send.at[s], state_recv.at[s], partner
        ).wait_send()
        remote(
            SR.at[s, 0:15], RR.at[s, 0:15], back_send.at[s], back_recv.at[s], partner
        ).wait_send()
        remote(
            G.at[s, :, 0:896], G.at[s, :, 0:896], mix_send.at[s], mix_recv.at[s], partner
        ).wait_send()


def local(
    tokens,
    norm_gain,
    x_weight,
    z_weight,
    b_weight,
    c_weight,
    dt_weight,
    x_conv,
    b_conv,
    c_conv,
    dt_bias,
    decay_rate,
    out_gain,
    out_weight,
):
    smem = pl.BlockSpec(memory_space=pltpu.SMEM)
    vmem = pl.BlockSpec(memory_space=pltpu.VMEM)
    dma = pltpu.SemaphoreType.DMA
    return pl.pallas_call(
        kernel,
        out_shape=jax.ShapeDtypeStruct(tokens.shape, BF16),
        in_specs=[smem, smem] + [vmem] * 12,
        out_specs=vmem,
        scratch_shapes=[
            pltpu.VMEM((SEQS, SPAN, WIDTH), BF16),
            pltpu.VMEM((4, 4, ROWS, 256), BF16),
            pltpu.VMEM((4, 4, ROWS, 384), BF16),
            pltpu.VMEM((4, ROWS, 512), BF16),
            pltpu.VMEM((2, 512, WIDTH), BF16),
            pltpu.VMEM((SEQS, 3, SPAN + 8, LANES), F32),
            pltpu.VMEM((SEQS, SPAN, LANES), F32),
            pltpu.VMEM((SEQS, SPAN, LANES), F32),
            pltpu.VMEM((SEQS, SPAN, LANES), F32),
            pltpu.VMEM((SEQS, SPAN, LANES), BF16),
            pltpu.VMEM((SEQS, SPAN, LANES), BF16),
            pltpu.VMEM((SEQS, SPAN, LANES), BF16),
            pltpu.VMEM((SEQS, SPAN, LANES), F32),
            pltpu.VMEM((SEQS, 2, LANES, LANES), F32),
            pltpu.VMEM((SEQS, 16, 16, LANES), BF16),
            pltpu.VMEM((SEQS, 16, 16, LANES), BF16),
            pltpu.VMEM((SEQS, 16, 8, LANES), F32),
            pltpu.VMEM((SEQS, 16, 8, LANES), F32),
            pltpu.VMEM((SEQS, SPAN, LANES), BF16),
            pltpu.VMEM((SEQS, ROWS, WIDTH), BF16),
            dma((17, 4)),
            dma((17, 4)),
            dma((SEQS + 1, 5)),
            dma((SEQS + 1, 5)),
            dma((SEQS,)),
            dma((SEQS,)),
            dma((SEQS,)),
            dma((SEQS,)),
            dma((SEQS,)),
            dma((SEQS,)),
            dma((SEQS,)),
            dma((SEQS,)),
            dma((SEQS,)),
        ],
        compiler_params=pltpu.CompilerParams(
            collective_id=0, has_side_effects=True, vmem_limit_bytes=56 * 1024 * 1024
        ),
        name="mixer",
    )(
        dt_bias,
        decay_rate,
        tokens,
        norm_gain.reshape(1, -1),
        x_weight,
        z_weight,
        b_weight,
        c_weight,
        dt_weight.T,
        x_conv,
        b_conv,
        c_conv,
        out_gain.reshape(1, -1),
        out_weight.T,
    )


def solution(mesh):
    torus = Mesh(mesh.devices.reshape(4, 4, 4, 2), SP_TP)
    return jax.shard_map(
        local,
        mesh=torus,
        in_specs=(
            P(None, SP_TP, None),
            P(),
            P(SP, TP),
            P(SP, TP),
            P(SP, TP),
            P(SP, TP),
            P(SP, TP),
            P(None, TP),
            P(None, TP),
            P(None, TP),
            P(TP),
            P(TP),
            P(TP),
            P(TP, SP),
        ),
        out_specs=P(None, SP_TP, None),
        check_vma=False,
    )
```

```python
import functools

import jax
import jax.numpy as jnp
from jax import lax
from jax.experimental import pallas as pl
from jax.experimental.pallas import tpu as pltpu
from jax.sharding import Mesh
from jax.sharding import PartitionSpec as P

CONV = 4
SP = ("sp_0", "sp_1")
TP = ("tp_0", "tp_1")
SP_TP = ("sp_0", "sp_1", "tp_0", "tp_1")
LENGTH = 8192
SEQS = 4
SPAN = 512
ROWS = 64
WIDTH = 1024
CHUNK = 256
LANES = 128
epsilon = 1e-05
MESH = pl.DeviceIdType.MESH
F32 = jnp.float32
BF16 = jnp.bfloat16


def remote(src, dst, send, recv, device):
    return pltpu.make_async_remote_copy(
        src_ref=src,
        dst_ref=dst,
        send_sem=send,
        recv_sem=recv,
        device_id=device,
        device_id_type=MESH,
    )


class Ring:
    def __init__(self, place, axis, block, sends, recvs, number, direct=False):
        self.block, self.sends, self.recvs, self.number = block, sends, recvs, number
        self.direct = direct
        self.me = place[axis]
        self.right, self.left = lax.rem(self.me + 1, 4), lax.rem(self.me + 3, 4)
        self.far = lax.rem(self.me + 2, 4)
        to = lambda i: tuple(i if k == axis else p for k, p in enumerate(place))
        self.to_right, self.to_left, self.to_far = to(self.right), to(self.left), to(self.far)

    def copy(self, ref, lane, device):
        return remote(
            ref, ref, self.sends.at[self.number, lane], self.recvs.at[self.number, lane], device
        )

    def own(self):
        self.copy(self.block(self.me, None), 0, self.to_right).start()
        self.copy(self.block(self.me, None), 1, self.to_left).start()
        if self.direct:
            self.copy(self.block(self.me, None), 2, self.to_far).start()

    def near(self):
        self.copy(self.block(self.left, None), 0, self.to_right).wait_recv()
        if not self.direct:
            self.copy(self.block(self.left, 0), 2, self.to_right).start()
        self.copy(self.block(self.right, None), 1, self.to_left).wait_recv()
        if not self.direct:
            self.copy(self.block(self.right, 1), 3, self.to_left).start()

    def last(self):
        if self.direct:
            self.copy(self.block(self.far, None), 2, self.to_far).wait_recv()
        else:
            self.copy(self.block(self.far, 0), 2, self.to_right).wait_recv()
            self.copy(self.block(self.far, 1), 3, self.to_left).wait_recv()

    def drain(self):
        self.copy(self.block(self.me, None), 0, self.to_right).wait_send()
        self.copy(self.block(self.me, None), 1, self.to_left).wait_send()
        if self.direct:
            self.copy(self.block(self.me, None), 2, self.to_far).wait_send()
        else:
            self.copy(self.block(self.left, 0), 2, self.to_right).wait_send()
            self.copy(self.block(self.right, 1), 3, self.to_left).wait_send()


def half_rows(half):
    return slice(None) if half is None else slice(32 * half, 32 * half + 32)


def half_blocks(half):
    return slice(None) if half is None else slice(2 * half, 2 * half + 2)


def matmul(a, b, dims=((1,), (0,)), precision=None):
    return lax.dot_general(a, b, (dims, ((), ())), precision=precision, preferred_element_type=F32)


def silu(value):
    half = 0.5 * value
    return half + half * jnp.tanh(half)


def kernel(
    bias_ref,
    rate_ref,
    tokens_ref,
    gain_ref,
    xw_ref,
    zw_ref,
    bw_ref,
    cw_ref,
    dw_ref,
    xt_ref,
    bt_ref,
    ct_ref,
    og_ref,
    ow_ref,
    out_ref,
    T,
    WA,
    WB,
    OY,
    O,
    E,
    Z,
    DT,
    CUM,
    XS,
    BS,
    CS,
    Y,
    U,
    SS,
    RS,
    SR,
    RR,
    GT,
    G,
    ring_send,
    ring_recv,
    pair_send,
    pair_recv,
    halo_send,
    halo_recv,
    state_send,
    state_recv,
    back_send,
    back_recv,
    mix_send,
    mix_recv,
    local_sem,
):
    z, y = lax.axis_index("sp_0"), lax.axis_index("sp_1")
    x, c = lax.axis_index("tp_0"), lax.axis_index("tp_1")
    place = (z, y, x, c)
    sp, tp = z * 4 + y, x * 2 + c
    other = 1 - c
    partner = (z, y, x, other)

    def sp_device(i):
        return (i // 4, lax.rem(i, 4), x, c)

    def tp_device(i):
        return (z, y, i // 2, lax.rem(i, 2))

    barrier = pltpu.get_barrier_semaphore()
    for step in (1, 2, 3):
        for axis in range(3):
            near = tuple(lax.rem(p + step, 4) if k == axis else p for k, p in enumerate(place))
            pl.semaphore_signal(barrier, inc=1, device_id=near, device_id_type=MESH)
    pl.semaphore_signal(barrier, inc=1, device_id=partner, device_id_type=MESH)

    lane = lax.broadcasted_iota(jnp.int32, (1, LANES), 1)
    low = lane < 64

    WA[z, y, :, 0:128] = xw_ref[...]
    WA[z, y, :, 128:256] = bw_ref[...]
    WB[z, y, :, 0:128] = cw_ref[...]
    WB[z, y, :, 128:256] = zw_ref[...]
    head_at = lax.broadcasted_iota(jnp.int32, (2, LANES), 0)
    lane_at = lax.broadcasted_iota(jnp.int32, (2, LANES), 1)
    spread = (lane_at // 64 == head_at).astype(BF16)
    WB[z, y, :, 256:384] = matmul(dw_ref[...], spread, ((0,), (0,))).astype(BF16)

    def normed(s):
        source = tokens_ref[s].astype(F32)
        scale = lax.rsqrt(jnp.mean(source * source, axis=-1, keepdims=True) + epsilon)
        T[s, pl.ds(pl.multiple_of(tp * ROWS, ROWS), ROWS), :] = (
            source * scale * gain_ref[...]
        ).astype(BF16)

    normed(0)
    own_columns = pl.multiple_of((c * 4 + x) * LANES, LANES)
    OY[y, :, pl.ds(pl.multiple_of(x * LANES, LANES), LANES)] = ow_ref[...]
    pl.semaphore_wait(barrier, 10)

    def token_block(s):
        def block(i, half):
            start = (i * 2 + c) * ROWS + (0 if half is None else 32 * half)
            rows = ROWS if half is None else 32
            return T.at[s, pl.ds(pl.multiple_of(start, 32), rows), :]

        return block

    ring = lambda axis, block, number, direct=False: Ring(
        place, axis, block, ring_send, ring_recv, number, direct
    )
    tokens = [ring(2, token_block(s), s) for s in range(SEQS)]
    wa1 = ring(1, lambda i, h: WA.at[z, i, half_rows(h)], 4, True)
    wb1 = ring(0, lambda i, h: WB.at[i, y, half_rows(h)], 5, True)
    shifted = lambda i, k: lax.rem(i + k, 4)
    wa2 = [ring(0, lambda i, h, k=k: WA.at[i, shifted(y, k), half_rows(h)], 6 + k) for k in range(4)]
    wb2 = [ring(1, lambda i, h, k=k: WB.at[shifted(z, k), i, half_rows(h)], 10 + k) for k in range(4)]
    ox = ring(
        2,
        lambda i, h: OY.at[y, half_rows(h), pl.ds(pl.multiple_of(i * LANES, LANES), LANES)],
        14,
        True,
    )
    oy = ring(1, lambda i, h: OY.at[i, half_rows(h)], 15)
    def out_block(p):
        def block(i, half):
            rows = slice(256 * p, 256 * p + 256)
            if half is not None:
                rows = slice(256 * p + 128 * half, 256 * p + 128 * half + 128)
            return O.at[c, rows, pl.ds(pl.multiple_of(i * 256, 256), 256)]

        return block

    oz = [ring(0, out_block(p), 16 + p) for p in range(2)]

    def pair_copy(s, k, core):
        i, half = (
            (x, None),
            (tokens[s].left, None),
            (tokens[s].right, None),
            (tokens[s].far, 0),
            (tokens[s].far, 1),
        )[k]
        start = (i * 2 + core) * ROWS + (0 if half is None else 32 * half)
        rows = ROWS if half is None else 32
        ref = T.at[s, pl.ds(pl.multiple_of(start, 32), rows), :]
        return remote(ref, ref, pair_send.at[s, k], pair_recv.at[s, k], partner)

    def out_pair(core):
        ref = O.at[core]
        return remote(ref, ref, pair_send.at[SEQS, 0], pair_recv.at[SEQS, 0], partner)

    def token_own(s):
        tokens[s].own()
        pair_copy(s, 0, c).start()

    def token_near(s):
        tokens[s].near()
        pair_copy(s, 1, c).start()
        pair_copy(s, 2, c).start()

    def token_last(s):
        tokens[s].last()
        pair_copy(s, 3, c).start()
        pair_copy(s, 4, c).start()

    wa1.own()
    wb1.own()
    wa2[0].own()
    wb2[0].own()
    ox.own()
    token_own(0)
    normed(1)
    token_own(1)
    normed(2)
    normed(3)
    wa1.near()
    wa2[1].own()
    wa2[3].own()
    wb1.near()
    wb2[1].own()
    wb2[3].own()
    wa1.last()
    wa2[2].own()
    wb1.last()
    wb2[2].own()
    wa2[0].near()
    wb2[0].near()
    ox.near()
    ox.last()
    token_near(0)
    token_own(2)
    wa2[1].near()
    wa2[3].near()
    wb2[1].near()
    wb2[3].near()
    oy.own()
    token_near(1)
    token_own(3)
    wa2[2].near()
    wb2[2].near()
    token_last(0)
    wa2[0].last()
    wa2[1].last()
    wa2[3].last()
    wa2[2].last()
    wb2[0].last()
    wb2[1].last()
    wb2[3].last()
    wb2[2].last()

    bias = jnp.where(low, bias_ref[0], bias_ref[1])
    rate = jnp.where(low, rate_ref[0], rate_ref[1])
    row_at = lax.broadcasted_iota(jnp.int32, (CHUNK, CHUNK), 0)
    column_at = lax.broadcasted_iota(jnp.int32, (CHUNK, CHUNK), 1)
    lower = row_at >= column_at
    ones_below = lower.astype(BF16)
    tiles = [slice(k * ROWS, (k + 1) * ROWS) for k in range(SPAN // ROWS)]
    following = sp_device(lax.rem(sp + 1, 16))

    def halo(s):
        return remote(
            E.at[s, :, SPAN : SPAN + 8, :],
            E.at[s, :, 0:8, :],
            halo_send.at[s],
            halo_recv.at[s],
            following,
        )

    def token_pair(s, first, last):
        for k in range(first, last):
            pair_copy(s, k, other).wait_recv()

    def halo_in(s):
        halo(s).wait_recv()

    def state_in(s):
        remote(
            SS.at[s, 0:15], RS.at[s, 0:15], state_send.at[s], state_recv.at[s], partner
        ).wait_recv()

    def back_in(s):
        remote(
            SR.at[s, 0:15], RR.at[s, 0:15], back_send.at[s], back_recv.at[s], partner
        ).wait_recv()

    def project(s):
        product = matmul(T[s], WA[...].reshape(WIDTH, 256))
        E[s, 0, 8 : SPAN + 8, :] = product[:, 0:128]
        E[s, 1, 8 : SPAN + 8, :] = product[:, 128:256]
        product = matmul(T[s], WB[...].reshape(WIDTH, 384))
        E[s, 2, 8 : SPAN + 8, :] = product[:, 0:128]
        Z[s] = product[:, 128:256]
        DT[s] = product[:, 256:384]
        halo(s).start()
        for rows in tiles:
            Z[s, rows, :] = silu(Z[s, rows, :])
            step = DT[s, rows, :] + bias
            step = jnp.maximum(step, 0.0) + jnp.log1p(jnp.exp(-jnp.abs(step)))
            DT[s, rows, :] = step
            XS[s, rows, :] = (-(step * rate) / LENGTH).astype(BF16)
        for k in range(2):
            rows = slice(k * CHUNK, (k + 1) * CHUNK)
            CUM[s, rows, :] = matmul(ones_below, XS[s, rows, :])

    def convolve(s):
        for k in range(3):
            E[s, k, 0:8, :] = jnp.where(sp == 0, 0.0, E[s, k, 0:8, :])
        for k, taps_ref in enumerate((xt_ref, bt_ref, ct_ref)):
            taps = [taps_ref[offset : offset + 1, :] for offset in range(CONV)]
            for rows in tiles:
                start = rows.start + 5
                running = taps[0] * E[s, k, start : start + ROWS, :]
                for offset in range(1, CONV):
                    first = start + offset
                    running = running + taps[offset] * E[s, k, first : first + ROWS, :]
                running = silu(running)
                if k == 0:
                    decayed = DT[s, rows, :] * jnp.exp(-CUM[s, rows, :])
                    XS[s, rows, :] = (running * decayed).astype(BF16)
                elif k == 1:
                    BS[s, rows, :] = running.astype(BF16)
                else:
                    CS[s, rows, :] = running.astype(BF16)

    def states(s):
        for k in range(2):
            rows = slice(k * CHUNK, (k + 1) * CHUNK)
            U[s, k] = matmul(BS[s, rows, :], XS[s, rows, :], ((0,), (0,)))
        first, second = CUM[s, CHUNK - 1 : CHUNK, :], CUM[s, SPAN - 1 : SPAN, :]
        final = jnp.exp(second) * (jnp.exp(first) * U[s, 0] + U[s, 1])
        total = jnp.broadcast_to((first + second).reshape(1, 1, LANES), (16, 8, LANES))
        SS[s] = jnp.concatenate([final.reshape(16, 8, LANES), total], axis=1).astype(BF16)

        def send(k, _):
            i = lax.rem(sp + k, 16)
            remote(
                SS.at[s, i], RS.at[s, sp], state_send.at[s], state_recv.at[s], sp_device(i)
            ).start()
            return 0

        lax.fori_loop(1, 16, send, 0)
        RS[s, sp] = SS[s, sp]

    def inside(s):
        for k in range(2):
            rows = slice(k * CHUNK, (k + 1) * CHUNK)
            scores = matmul(CS[s, rows, :], BS[s, rows, :], ((1,), (1,)))
            scores = jnp.where(lower, scores, 0.0).astype(BF16)
            Y[s, rows, :] = matmul(scores, XS[s, rows, :])

    def scan(s):
        entering = jnp.zeros((8, LANES), F32)
        for i in range(16):
            SR[s, i] = entering
            piece = RS[s, i].astype(F32)
            entering = jnp.exp(piece[8:16]) * entering + piece[0:8]

        def send(k, _):
            i = lax.rem(sp + k, 16)
            remote(
                SR.at[s, i], RR.at[s, sp], back_send.at[s], back_recv.at[s], sp_device(i)
            ).start()
            return 0

        lax.fori_loop(1, 16, send, 0)
        RR[s, sp] = SR[s, sp]

    def finish(s):
        entering = RR[s].reshape(LANES, LANES)
        for k in range(2):
            rows = slice(k * CHUNK, (k + 1) * CHUNK)
            Y[s, rows, :] += matmul(CS[s, rows, :], entering.astype(BF16))
            if k == 0:
                grown = jnp.exp(CUM[s, CHUNK - 1 : CHUNK, :])
                entering = grown * (entering + U[s, 0])
        for rows in tiles:
            gated = Y[s, rows, :] * jnp.exp(CUM[s, rows, :]) * Z[s, rows, :]
            scale = lax.rsqrt(jnp.mean(gated * gated, axis=-1, keepdims=True) + epsilon)
            GT[s, rows, :] = (gated * scale * og_ref[...]).astype(BF16)

        def send(k, _):
            i = lax.rem(tp + k, 8)
            remote(
                GT.at[s, pl.ds(pl.multiple_of(i * ROWS, ROWS), ROWS), :],
                G.at[s, :, pl.ds(own_columns, LANES)],
                mix_send.at[s],
                mix_recv.at[s],
                tp_device(i),
            ).start()
            return 0

        lax.fori_loop(1, 8, send, 0)
        own(s).start()

    def own(s):
        return pltpu.make_async_copy(
            GT.at[s, pl.ds(pl.multiple_of(tp * ROWS, ROWS), ROWS), :],
            G.at[s, :, pl.ds(own_columns, LANES)],
            local_sem.at[s],
        )

    def mixed_in(s):
        remote(
            G.at[s, :, 0:896], G.at[s, :, 0:896], mix_send.at[s], mix_recv.at[s], partner
        ).wait_recv()
        own(s).wait()

    def multiply(first, last):
        gathered = G[first:last].reshape((last - first) * ROWS, WIDTH)
        result = matmul(gathered, O[...].reshape(WIDTH, WIDTH))
        out_ref[first:last] = result.astype(BF16).reshape(last - first, ROWS, WIDTH)

    def turn():
        block = OY[...].reshape(256, 512).astype(F32).T.astype(BF16)
        O[c, :, pl.ds(pl.multiple_of(z * 256, 256), 256)] = block

    token_pair(0, 0, 5)
    project(0)
    token_near(2)
    token_last(1)
    oy.near()
    token_pair(1, 0, 5)
    project(1)
    token_near(3)
    token_last(2)
    oy.last()
    turn()
    oz[0].own()
    halo_in(0)
    convolve(0)
    states(0)
    token_pair(2, 0, 5)
    project(2)
    token_last(3)
    oz[1].own()
    halo_in(1)
    convolve(1)
    states(1)
    oz[0].near()
    token_pair(3, 0, 5)
    project(3)
    halo_in(2)
    convolve(2)
    states(2)
    oz[1].near()
    state_in(0)
    scan(0)
    inside(0)
    state_in(1)
    scan(1)
    halo_in(3)
    convolve(3)
    states(3)
    state_in(2)
    scan(2)
    inside(1)
    inside(2)
    inside(3)
    back_in(0)
    finish(0)
    back_in(1)
    finish(1)
    oz[0].last()
    oz[1].last()
    out_pair(c).start()
    state_in(3)
    scan(3)
    back_in(2)
    finish(2)
    out_pair(other).wait_recv()
    mixed_in(0)
    mixed_in(1)
    mixed_in(2)
    multiply(0, 3)
    back_in(3)
    finish(3)
    mixed_in(3)
    multiply(3, 4)

    for each in (*tokens, wa1, wb1, *wa2, *wb2, ox, oy, *oz):
        each.drain()
    out_pair(c).wait_send()
    for s in range(SEQS):
        for k in range(5):
            pair_copy(s, k, c).wait_send()
        halo(s).wait_send()
        remote(
            SS.at[s, 0:15], RS.at[s, 0:15], state_send.at[s], state_recv.at[s], partner
        ).wait_send()
        remote(
            SR.at[s, 0:15], RR.at[s, 0:15], back_send.at[s], back_recv.at[s], partner
        ).wait_send()
        remote(
            G.at[s, :, 0:896], G.at[s, :, 0:896], mix_send.at[s], mix_recv.at[s], partner
        ).wait_send()


def local(
    tokens,
    norm_gain,
    x_weight,
    z_weight,
    b_weight,
    c_weight,
    dt_weight,
    x_conv,
    b_conv,
    c_conv,
    dt_bias,
    decay_rate,
    out_gain,
    out_weight,
):
    smem = pl.BlockSpec(memory_space=pltpu.SMEM)
    vmem = pl.BlockSpec(memory_space=pltpu.VMEM)
    dma = pltpu.SemaphoreType.DMA
    return pl.pallas_call(
        kernel,
        out_shape=jax.ShapeDtypeStruct(tokens.shape, BF16),
        in_specs=[smem, smem] + [vmem] * 12,
        out_specs=vmem,
        scratch_shapes=[
            pltpu.VMEM((SEQS, SPAN, WIDTH), BF16),
            pltpu.VMEM((4, 4, ROWS, 256), BF16),
            pltpu.VMEM((4, 4, ROWS, 384), BF16),
            pltpu.VMEM((4, ROWS, 512), BF16),
            pltpu.VMEM((2, 512, WIDTH), BF16),
            pltpu.VMEM((SEQS, 3, SPAN + 8, LANES), F32),
            pltpu.VMEM((SEQS, SPAN, LANES), F32),
            pltpu.VMEM((SEQS, SPAN, LANES), F32),
            pltpu.VMEM((SEQS, SPAN, LANES), F32),
            pltpu.VMEM((SEQS, SPAN, LANES), BF16),
            pltpu.VMEM((SEQS, SPAN, LANES), BF16),
            pltpu.VMEM((SEQS, SPAN, LANES), BF16),
            pltpu.VMEM((SEQS, SPAN, LANES), F32),
            pltpu.VMEM((SEQS, 2, LANES, LANES), F32),
            pltpu.VMEM((SEQS, 16, 16, LANES), BF16),
            pltpu.VMEM((SEQS, 16, 16, LANES), BF16),
            pltpu.VMEM((SEQS, 16, 8, LANES), F32),
            pltpu.VMEM((SEQS, 16, 8, LANES), F32),
            pltpu.VMEM((SEQS, SPAN, LANES), BF16),
            pltpu.VMEM((SEQS, ROWS, WIDTH), BF16),
            dma((18, 4)),
            dma((18, 4)),
            dma((SEQS + 1, 5)),
            dma((SEQS + 1, 5)),
            dma((SEQS,)),
            dma((SEQS,)),
            dma((SEQS,)),
            dma((SEQS,)),
            dma((SEQS,)),
            dma((SEQS,)),
            dma((SEQS,)),
            dma((SEQS,)),
            dma((SEQS,)),
        ],
        compiler_params=pltpu.CompilerParams(
            collective_id=0, has_side_effects=True, vmem_limit_bytes=56 * 1024 * 1024
        ),
        name="mixer",
    )(
        dt_bias,
        decay_rate,
        tokens,
        norm_gain.reshape(1, -1),
        x_weight,
        z_weight,
        b_weight,
        c_weight,
        dt_weight.T,
        x_conv,
        b_conv,
        c_conv,
        out_gain.reshape(1, -1),
        out_weight.T,
    )


def solution(mesh):
    torus = Mesh(mesh.devices.reshape(4, 4, 4, 2), SP_TP)
    return jax.shard_map(
        local,
        mesh=torus,
        in_specs=(
            P(None, SP_TP, None),
            P(),
            P(SP, TP),
            P(SP, TP),
            P(SP, TP),
            P(SP, TP),
            P(SP, TP),
            P(None, TP),
            P(None, TP),
            P(None, TP),
            P(TP),
            P(TP),
            P(TP),
            P(TP, SP),
        ),
        out_specs=P(None, SP_TP, None),
        check_vma=False,
    )
```

```python
import functools

import jax
import jax.numpy as jnp
from jax import lax
from jax.experimental import pallas as pl
from jax.experimental.pallas import tpu as pltpu
from jax.sharding import Mesh
from jax.sharding import PartitionSpec as P

CONV = 4
SP = ("sp_0", "sp_1")
TP = ("tp_0", "tp_1")
SP_TP = ("sp_0", "sp_1", "tp_0", "tp_1")
LENGTH = 8192
SEQS = 4
SPAN = 512
ROWS = 64
WIDTH = 1024
CHUNK = 256
LANES = 128
epsilon = 1e-05
MESH = pl.DeviceIdType.MESH
F32 = jnp.float32
BF16 = jnp.bfloat16


def remote(src, dst, send, recv, device):
    return pltpu.make_async_remote_copy(
        src_ref=src,
        dst_ref=dst,
        send_sem=send,
        recv_sem=recv,
        device_id=device,
        device_id_type=MESH,
    )


class Ring:
    def __init__(self, place, axis, block, sends, recvs, number, direct=False):
        self.block, self.sends, self.recvs, self.number = block, sends, recvs, number
        self.direct = direct
        self.me = place[axis]
        self.right, self.left = lax.rem(self.me + 1, 4), lax.rem(self.me + 3, 4)
        self.far = lax.rem(self.me + 2, 4)
        to = lambda i: tuple(i if k == axis else p for k, p in enumerate(place))
        self.to_right, self.to_left, self.to_far = to(self.right), to(self.left), to(self.far)

    def copy(self, ref, lane, device):
        return remote(
            ref, ref, self.sends.at[self.number, lane], self.recvs.at[self.number, lane], device
        )

    def own(self):
        self.copy(self.block(self.me, None), 0, self.to_right).start()
        self.copy(self.block(self.me, None), 1, self.to_left).start()
        if self.direct:
            self.copy(self.block(self.me, None), 2, self.to_far).start()

    def near(self):
        self.copy(self.block(self.left, None), 0, self.to_right).wait_recv()
        if not self.direct:
            self.copy(self.block(self.left, 0), 2, self.to_right).start()
        self.copy(self.block(self.right, None), 1, self.to_left).wait_recv()
        if not self.direct:
            self.copy(self.block(self.right, 1), 3, self.to_left).start()

    def last(self):
        if self.direct:
            self.copy(self.block(self.far, None), 2, self.to_far).wait_recv()
        else:
            self.copy(self.block(self.far, 0), 2, self.to_right).wait_recv()
            self.copy(self.block(self.far, 1), 3, self.to_left).wait_recv()

    def drain(self):
        self.copy(self.block(self.me, None), 0, self.to_right).wait_send()
        self.copy(self.block(self.me, None), 1, self.to_left).wait_send()
        if self.direct:
            self.copy(self.block(self.me, None), 2, self.to_far).wait_send()
        else:
            self.copy(self.block(self.left, 0), 2, self.to_right).wait_send()
            self.copy(self.block(self.right, 1), 3, self.to_left).wait_send()


def half_rows(half):
    return slice(None) if half is None else slice(32 * half, 32 * half + 32)


def half_blocks(half):
    return slice(None) if half is None else slice(2 * half, 2 * half + 2)


def matmul(a, b, dims=((1,), (0,)), precision=None):
    return lax.dot_general(a, b, (dims, ((), ())), precision=precision, preferred_element_type=F32)


def silu(value):
    half = 0.5 * value
    return half + half * jnp.tanh(half)


def kernel(
    bias_in,
    rate_in,
    tokens_in,
    gain_in,
    xw_in,
    zw_in,
    bw_in,
    cw_in,
    dw_in,
    xt_in,
    bt_in,
    ct_in,
    og_in,
    ow_in,
    out_hbm,
    bias_ref,
    rate_ref,
    tokens_ref,
    gain_ref,
    dw_ref,
    taps_ref,
    og_ref,
    out_ref,
    T,
    WA,
    WB,
    OYZ,
    O,
    E,
    Z,
    DT,
    CUM,
    XS,
    BS,
    CS,
    Y,
    U,
    SS,
    RS,
    SR,
    RR,
    GT,
    G,
    ring_send,
    ring_recv,
    pair_send,
    pair_recv,
    halo_send,
    halo_recv,
    state_send,
    state_recv,
    back_send,
    back_recv,
    mix_send,
    mix_recv,
    local_sem,
    load_sem,
    out_sem,
):
    z, y = lax.axis_index("sp_0"), lax.axis_index("sp_1")
    x, c = lax.axis_index("tp_0"), lax.axis_index("tp_1")
    place = (z, y, x, c)
    sp, tp = z * 4 + y, x * 2 + c
    other = 1 - c
    partner = (z, y, x, other)

    def sp_device(i):
        return (i // 4, lax.rem(i, 4), x, c)

    def tp_device(i):
        return (z, y, i // 2, lax.rem(i, 2))

    barrier = pltpu.get_barrier_semaphore()
    for step in (1, 2, 3):
        for axis in range(3):
            near = tuple(lax.rem(p + step, 4) if k == axis else p for k, p in enumerate(place))
            pl.semaphore_signal(barrier, inc=1, device_id=near, device_id_type=MESH)
    pl.semaphore_signal(barrier, inc=1, device_id=partner, device_id_type=MESH)

    loads = (
        (xw_in, WA.at[z, y, :, 0:128]),
        (bw_in, WA.at[z, y, :, 128:256]),
        (cw_in, WB.at[z, y, :, 0:128]),
        (zw_in, WB.at[z, y, :, 128:256]),
        (dw_in, dw_ref),
        (ow_in, OYZ.at[z, y]),
        (gain_in, gain_ref),
        *((tokens_in.at[s], tokens_ref.at[s]) for s in range(SEQS)),
        (xt_in, taps_ref.at[0]),
        (bt_in, taps_ref.at[1]),
        (ct_in, taps_ref.at[2]),
        (og_in, og_ref),
        (bias_in, bias_ref),
        (rate_in, rate_ref),
    )
    loads = [pltpu.make_async_copy(*pair, load_sem.at[k]) for k, pair in enumerate(loads)]
    for load in loads:
        load.start()

    lane = lax.broadcasted_iota(jnp.int32, (1, LANES), 1)
    low = lane < 64

    head_at = lax.broadcasted_iota(jnp.int32, (2, LANES), 0)
    lane_at = lax.broadcasted_iota(jnp.int32, (2, LANES), 1)
    spread = (lane_at // 64 == head_at).astype(BF16)
    for load in loads[0:7]:
        load.wait()
    WB[z, y, :, 256:384] = matmul(dw_ref[...], spread, ((0,), (0,))).astype(BF16)

    def normed(s):
        loads[7 + s].wait()
        source = tokens_ref[s].astype(F32)
        scale = lax.rsqrt(jnp.mean(source * source, axis=-1, keepdims=True) + epsilon)
        T[s, pl.ds(pl.multiple_of(tp * ROWS, ROWS), ROWS), :] = (
            source * scale * gain_ref[...]
        ).astype(BF16)

    own_columns = pl.multiple_of((c * 4 + x) * LANES, LANES)
    pl.semaphore_wait(barrier, 10)

    def token_block(s):
        def block(i, half):
            start = (i * 2 + c) * ROWS + (0 if half is None else 32 * half)
            rows = ROWS if half is None else 32
            return T.at[s, pl.ds(pl.multiple_of(start, 32), rows), :]

        return block

    ring = lambda axis, block, number, direct=False: Ring(
        place, axis, block, ring_send, ring_recv, number, direct
    )
    tokens = [ring(2, token_block(s), s) for s in range(SEQS)]
    wa1 = ring(1, lambda i, h: WA.at[z, i, half_rows(h)], 4, True)
    wb1 = ring(0, lambda i, h: WB.at[i, y, half_rows(h)], 5, True)
    shifted = lambda i, k: lax.rem(i + k, 4)
    wa2 = [ring(0, lambda i, h, k=k: WA.at[i, shifted(y, k), half_rows(h)], 6 + k) for k in range(4)]
    wb2 = [ring(1, lambda i, h, k=k: WB.at[shifted(z, k), i, half_rows(h)], 10 + k) for k in range(4)]
    oy = ring(1, lambda i, h: OYZ.at[z, i], 14, True)
    oz = ring(0, lambda i, h: OYZ.at[i, half_blocks(h)], 15)

    def out_rows(core, i, half):
        rows = LANES if half is None else 64
        start = i * LANES + (0 if half is None else 64 * half)
        return O.at[core, pl.ds(pl.multiple_of(start, 64), rows), :]

    ox = ring(2, lambda i, h: out_rows(c, i, h), 16)

    def pair_copy(s, k, core):
        i, half = (
            (x, None),
            (tokens[s].left, None),
            (tokens[s].right, None),
            (tokens[s].far, 0),
            (tokens[s].far, 1),
        )[k]
        start = (i * 2 + core) * ROWS + (0 if half is None else 32 * half)
        rows = ROWS if half is None else 32
        ref = T.at[s, pl.ds(pl.multiple_of(start, 32), rows), :]
        return remote(ref, ref, pair_send.at[s, k], pair_recv.at[s, k], partner)

    def out_pair(k, core):
        i, half = ((x, None), (ox.left, None), (ox.right, None), (ox.far, 0), (ox.far, 1))[k]
        ref = out_rows(core, i, half)
        return remote(ref, ref, pair_send.at[SEQS, k], pair_recv.at[SEQS, k], partner)

    def out_own():
        block = OYZ[...].reshape(WIDTH, LANES).astype(F32).T.astype(BF16)
        O[c, pl.ds(pl.multiple_of(x * LANES, LANES), LANES), :] = block
        ox.own()
        out_pair(0, c).start()

    def out_near():
        ox.near()
        out_pair(1, c).start()
        out_pair(2, c).start()

    def out_last():
        ox.last()
        out_pair(3, c).start()
        out_pair(4, c).start()

    def out_pairs():
        for k in range(5):
            out_pair(k, other).wait_recv()

    def token_own(s):
        tokens[s].own()
        pair_copy(s, 0, c).start()

    def token_near(s):
        tokens[s].near()
        pair_copy(s, 1, c).start()
        pair_copy(s, 2, c).start()

    def token_last(s):
        tokens[s].last()
        pair_copy(s, 3, c).start()
        pair_copy(s, 4, c).start()

    wa1.own()
    wb1.own()
    wa2[0].own()
    wb2[0].own()
    normed(0)
    token_own(0)
    normed(1)
    token_own(1)
    normed(2)
    normed(3)
    wa1.near()
    wa2[1].own()
    wa2[3].own()
    wb1.near()
    wb2[1].own()
    wb2[3].own()
    wa1.last()
    wa2[2].own()
    wb1.last()
    wb2[2].own()
    wa2[0].near()
    wb2[0].near()
    token_near(0)
    token_own(2)
    wa2[1].near()
    wa2[3].near()
    wb2[1].near()
    wb2[3].near()
    oy.own()
    token_near(1)
    token_own(3)
    wa2[2].near()
    wb2[2].near()
    token_last(0)
    wa2[0].last()
    wa2[1].last()
    wa2[3].last()
    wb2[0].last()
    wb2[1].last()
    wb2[3].last()
    oy.near()
    oy.last()
    oz.own()
    token_near(2)
    token_last(1)
    wa2[2].last()
    wb2[2].last()

    for load in loads[11:]:
        load.wait()
    bias = jnp.where(low, bias_ref[0], bias_ref[1])
    rate = jnp.where(low, rate_ref[0], rate_ref[1])
    row_at = lax.broadcasted_iota(jnp.int32, (CHUNK, CHUNK), 0)
    column_at = lax.broadcasted_iota(jnp.int32, (CHUNK, CHUNK), 1)
    lower = row_at >= column_at
    ones_below = lower.astype(BF16)
    tiles = [slice(k * ROWS, (k + 1) * ROWS) for k in range(SPAN // ROWS)]
    following = sp_device(lax.rem(sp + 1, 16))

    def halo(s):
        return remote(
            E.at[s, :, SPAN : SPAN + 8, :],
            E.at[s, :, 0:8, :],
            halo_send.at[s],
            halo_recv.at[s],
            following,
        )

    def token_pair(s, first, last):
        for k in range(first, last):
            pair_copy(s, k, other).wait_recv()

    def halo_in(s):
        halo(s).wait_recv()

    def state_in(s):
        remote(
            SS.at[s, 0:15], RS.at[s, 0:15], state_send.at[s], state_recv.at[s], partner
        ).wait_recv()

    def back_in(s):
        remote(
            SR.at[s, 0:15], RR.at[s, 0:15], back_send.at[s], back_recv.at[s], partner
        ).wait_recv()

    def project(s):
        product = matmul(T[s], WA[...].reshape(WIDTH, 256))
        E[s, 0, 8 : SPAN + 8, :] = product[:, 0:128]
        E[s, 1, 8 : SPAN + 8, :] = product[:, 128:256]
        product = matmul(T[s], WB[...].reshape(WIDTH, 384))
        E[s, 2, 8 : SPAN + 8, :] = product[:, 0:128]
        Z[s] = product[:, 128:256]
        DT[s] = product[:, 256:384]
        halo(s).start()
        for rows in tiles:
            Z[s, rows, :] = silu(Z[s, rows, :])
            step = DT[s, rows, :] + bias
            step = jnp.maximum(step, 0.0) + jnp.log1p(jnp.exp(-jnp.abs(step)))
            DT[s, rows, :] = step
            XS[s, rows, :] = (-(step * rate) / LENGTH).astype(BF16)
        for k in range(2):
            rows = slice(k * CHUNK, (k + 1) * CHUNK)
            CUM[s, rows, :] = matmul(ones_below, XS[s, rows, :])

    def convolve(s):
        for k in range(3):
            E[s, k, 0:8, :] = jnp.where(sp == 0, 0.0, E[s, k, 0:8, :])
        for k in range(3):
            taps = [taps_ref[k, offset : offset + 1, :] for offset in range(CONV)]
            for rows in tiles:
                start = rows.start + 5
                running = taps[0] * E[s, k, start : start + ROWS, :]
                for offset in range(1, CONV):
                    first = start + offset
                    running = running + taps[offset] * E[s, k, first : first + ROWS, :]
                running = silu(running)
                if k == 0:
                    decayed = DT[s, rows, :] * jnp.exp(-CUM[s, rows, :])
                    XS[s, rows, :] = (running * decayed).astype(BF16)
                elif k == 1:
                    BS[s, rows, :] = running.astype(BF16)
                else:
                    CS[s, rows, :] = running.astype(BF16)

    def states(s):
        for k in range(2):
            rows = slice(k * CHUNK, (k + 1) * CHUNK)
            U[s, k] = matmul(BS[s, rows, :], XS[s, rows, :], ((0,), (0,)))
        first, second = CUM[s, CHUNK - 1 : CHUNK, :], CUM[s, SPAN - 1 : SPAN, :]
        final = jnp.exp(second) * (jnp.exp(first) * U[s, 0] + U[s, 1])
        total = jnp.broadcast_to((first + second).reshape(1, 1, LANES), (16, 8, LANES))
        SS[s] = jnp.concatenate([final.reshape(16, 8, LANES), total], axis=1).astype(BF16)

        def send(k, _):
            i = lax.rem(sp + k, 16)
            remote(
                SS.at[s, i], RS.at[s, sp], state_send.at[s], state_recv.at[s], sp_device(i)
            ).start()
            return 0

        lax.fori_loop(1, 16, send, 0)
        RS[s, sp] = SS[s, sp]

    def inside(s):
        for k in range(2):
            rows = slice(k * CHUNK, (k + 1) * CHUNK)
            scores = matmul(CS[s, rows, :], BS[s, rows, :], ((1,), (1,)))
            scores = jnp.where(lower, scores, 0.0).astype(BF16)
            Y[s, rows, :] = matmul(scores, XS[s, rows, :])

    def scan(s):
        entering = jnp.zeros((8, LANES), F32)
        for i in range(16):
            SR[s, i] = entering
            piece = RS[s, i].astype(F32)
            entering = jnp.exp(piece[8:16]) * entering + piece[0:8]

        def send(k, _):
            i = lax.rem(sp + k, 16)
            remote(
                SR.at[s, i], RR.at[s, sp], back_send.at[s], back_recv.at[s], sp_device(i)
            ).start()
            return 0

        lax.fori_loop(1, 16, send, 0)
        RR[s, sp] = SR[s, sp]

    def finish(s):
        entering = RR[s].reshape(LANES, LANES)
        for k in range(2):
            rows = slice(k * CHUNK, (k + 1) * CHUNK)
            Y[s, rows, :] += matmul(CS[s, rows, :], entering.astype(BF16))
            if k == 0:
                grown = jnp.exp(CUM[s, CHUNK - 1 : CHUNK, :])
                entering = grown * (entering + U[s, 0])
        for rows in tiles:
            gated = Y[s, rows, :] * jnp.exp(CUM[s, rows, :]) * Z[s, rows, :]
            scale = lax.rsqrt(jnp.mean(gated * gated, axis=-1, keepdims=True) + epsilon)
            GT[s, rows, :] = (gated * scale * og_ref[...]).astype(BF16)

        def send(k, _):
            i = lax.rem(tp + k, 8)
            remote(
                GT.at[s, pl.ds(pl.multiple_of(i * ROWS, ROWS), ROWS), :],
                G.at[s, :, pl.ds(own_columns, LANES)],
                mix_send.at[s],
                mix_recv.at[s],
                tp_device(i),
            ).start()
            return 0

        lax.fori_loop(1, 8, send, 0)
        own(s).start()

    def own(s):
        return pltpu.make_async_copy(
            GT.at[s, pl.ds(pl.multiple_of(tp * ROWS, ROWS), ROWS), :],
            G.at[s, :, pl.ds(own_columns, LANES)],
            local_sem.at[s],
        )

    def mixed_in(s):
        remote(
            G.at[s, :, 0:896], G.at[s, :, 0:896], mix_send.at[s], mix_recv.at[s], partner
        ).wait_recv()
        own(s).wait()

    def put_out(first, last):
        return pltpu.make_async_copy(
            out_ref.at[first:last], out_hbm.at[first:last], out_sem.at[first]
        )

    def multiply(first, last):
        gathered = G[first:last].reshape((last - first) * ROWS, WIDTH)
        result = matmul(gathered, O[...].reshape(WIDTH, WIDTH))
        out_ref[first:last] = result.astype(BF16).reshape(last - first, ROWS, WIDTH)
        put_out(first, last).start()

    token_pair(0, 0, 5)
    project(0)
    token_near(3)
    token_pair(1, 0, 5)
    project(1)
    oz.near()
    token_last(2)
    halo_in(0)
    convolve(0)
    states(0)
    token_pair(2, 0, 5)
    project(2)
    oz.last()
    out_own()
    halo_in(1)
    convolve(1)
    states(1)
    token_last(3)
    state_in(0)
    scan(0)
    token_pair(3, 0, 5)
    project(3)
    halo_in(2)
    convolve(2)
    states(2)
    inside(0)
    state_in(1)
    scan(1)
    out_near()
    halo_in(3)
    convolve(3)
    states(3)
    back_in(0)
    finish(0)
    inside(1)
    state_in(2)
    scan(2)
    back_in(1)
    finish(1)
    inside(2)
    inside(3)
    out_last()
    state_in(3)
    scan(3)
    back_in(2)
    finish(2)
    back_in(3)
    finish(3)
    out_pairs()
    mixed_in(0)
    mixed_in(1)
    mixed_in(2)
    multiply(0, 3)
    mixed_in(3)
    multiply(3, 4)

    for each in (*tokens, wa1, wb1, *wa2, *wb2, oy, oz, ox):
        each.drain()
    for k in range(5):
        out_pair(k, c).wait_send()
    put_out(0, 3).wait()
    put_out(3, 4).wait()
    for s in range(SEQS):
        for k in range(5):
            pair_copy(s, k, c).wait_send()
        halo(s).wait_send()
        remote(
            SS.at[s, 0:15], RS.at[s, 0:15], state_send.at[s], state_recv.at[s], partner
        ).wait_send()
        remote(
            SR.at[s, 0:15], RR.at[s, 0:15], back_send.at[s], back_recv.at[s], partner
        ).wait_send()
        remote(
            G.at[s, :, 0:896], G.at[s, :, 0:896], mix_send.at[s], mix_recv.at[s], partner
        ).wait_send()


def local(
    tokens,
    norm_gain,
    x_weight,
    z_weight,
    b_weight,
    c_weight,
    dt_weight,
    x_conv,
    b_conv,
    c_conv,
    dt_bias,
    decay_rate,
    out_gain,
    out_weight,
):
    hbm = pl.BlockSpec(memory_space=pltpu.HBM)
    dma = pltpu.SemaphoreType.DMA
    return pl.pallas_call(
        kernel,
        out_shape=jax.ShapeDtypeStruct(tokens.shape, BF16),
        in_specs=[hbm] * 14,
        out_specs=hbm,
        scratch_shapes=[
            pltpu.SMEM((2,), F32),
            pltpu.SMEM((2,), F32),
            pltpu.VMEM((SEQS, ROWS, WIDTH), BF16),
            pltpu.VMEM((1, WIDTH), F32),
            pltpu.VMEM((2, ROWS), BF16),
            pltpu.VMEM((3, CONV, LANES), F32),
            pltpu.VMEM((1, LANES), F32),
            pltpu.VMEM((SEQS, ROWS, WIDTH), BF16),
            pltpu.VMEM((SEQS, SPAN, WIDTH), BF16),
            pltpu.VMEM((4, 4, ROWS, 256), BF16),
            pltpu.VMEM((4, 4, ROWS, 384), BF16),
            pltpu.VMEM((4, 4, ROWS, LANES), BF16),
            pltpu.VMEM((2, 512, WIDTH), BF16),
            pltpu.VMEM((SEQS, 3, SPAN + 8, LANES), F32),
            pltpu.VMEM((SEQS, SPAN, LANES), F32),
            pltpu.VMEM((SEQS, SPAN, LANES), F32),
            pltpu.VMEM((SEQS, SPAN, LANES), F32),
            pltpu.VMEM((SEQS, SPAN, LANES), BF16),
            pltpu.VMEM((SEQS, SPAN, LANES), BF16),
            pltpu.VMEM((SEQS, SPAN, LANES), BF16),
            pltpu.VMEM((SEQS, SPAN, LANES), F32),
            pltpu.VMEM((SEQS, 2, LANES, LANES), F32),
            pltpu.VMEM((SEQS, 16, 16, LANES), BF16),
            pltpu.VMEM((SEQS, 16, 16, LANES), BF16),
            pltpu.VMEM((SEQS, 16, 8, LANES), F32),
            pltpu.VMEM((SEQS, 16, 8, LANES), F32),
            pltpu.VMEM((SEQS, SPAN, LANES), BF16),
            pltpu.VMEM((SEQS, ROWS, WIDTH), BF16),
            dma((17, 4)),
            dma((17, 4)),
            dma((SEQS + 1, 5)),
            dma((SEQS + 1, 5)),
            dma((SEQS,)),
            dma((SEQS,)),
            dma((SEQS,)),
            dma((SEQS,)),
            dma((SEQS,)),
            dma((SEQS,)),
            dma((SEQS,)),
            dma((SEQS,)),
            dma((SEQS,)),
            dma((17,)),
            dma((SEQS,)),
        ],
        compiler_params=pltpu.CompilerParams(
            collective_id=0, has_side_effects=True, vmem_limit_bytes=56 * 1024 * 1024
        ),
        name="mixer",
    )(
        dt_bias,
        decay_rate,
        tokens,
        norm_gain.reshape(1, -1),
        x_weight,
        z_weight,
        b_weight,
        c_weight,
        dt_weight.T,
        x_conv,
        b_conv,
        c_conv,
        out_gain.reshape(1, -1),
        out_weight.T,
    )


def solution(mesh):
    torus = Mesh(mesh.devices.reshape(4, 4, 4, 2), SP_TP)
    return jax.shard_map(
        local,
        mesh=torus,
        in_specs=(
            P(None, SP_TP, None),
            P(),
            P(SP, TP),
            P(SP, TP),
            P(SP, TP),
            P(SP, TP),
            P(SP, TP),
            P(None, TP),
            P(None, TP),
            P(None, TP),
            P(TP),
            P(TP),
            P(TP),
            P(TP, SP),
        ),
        out_specs=P(None, SP_TP, None),
        check_vma=False,
    )
```

```python
import functools

import jax
import jax.numpy as jnp
from jax import lax
from jax.experimental import pallas as pl
from jax.experimental.pallas import tpu as pltpu
from jax.sharding import Mesh
from jax.sharding import PartitionSpec as P

CONV = 4
SP = ("sp_0", "sp_1")
TP = ("tp_0", "tp_1")
SP_TP = ("sp_0", "sp_1", "tp_0", "tp_1")
LENGTH = 8192
SEQS = 4
SPAN = 512
ROWS = 64
WIDTH = 1024
CHUNK = 256
LANES = 128
epsilon = 1e-05
MESH = pl.DeviceIdType.MESH
F32 = jnp.float32
BF16 = jnp.bfloat16


def remote(src, dst, send, recv, device):
    return pltpu.make_async_remote_copy(
        src_ref=src,
        dst_ref=dst,
        send_sem=send,
        recv_sem=recv,
        device_id=device,
        device_id_type=MESH,
    )


class Ring:
    def __init__(self, place, axis, block, sends, recvs, number, direct=False):
        self.block, self.sends, self.recvs, self.number = block, sends, recvs, number
        self.direct = direct
        self.me = place[axis]
        self.right, self.left = lax.rem(self.me + 1, 4), lax.rem(self.me + 3, 4)
        self.far = lax.rem(self.me + 2, 4)
        to = lambda i: tuple(i if k == axis else p for k, p in enumerate(place))
        self.to_right, self.to_left, self.to_far = to(self.right), to(self.left), to(self.far)

    def copy(self, ref, lane, device):
        return remote(
            ref, ref, self.sends.at[self.number, lane], self.recvs.at[self.number, lane], device
        )

    def own(self):
        self.copy(self.block(self.me, None), 0, self.to_right).start()
        self.copy(self.block(self.me, None), 1, self.to_left).start()
        if self.direct:
            self.copy(self.block(self.me, None), 2, self.to_far).start()

    def near(self):
        self.copy(self.block(self.left, None), 0, self.to_right).wait_recv()
        if not self.direct:
            self.copy(self.block(self.left, 0), 2, self.to_right).start()
        self.copy(self.block(self.right, None), 1, self.to_left).wait_recv()
        if not self.direct:
            self.copy(self.block(self.right, 1), 3, self.to_left).start()

    def last(self):
        if self.direct:
            self.copy(self.block(self.far, None), 2, self.to_far).wait_recv()
        else:
            self.copy(self.block(self.far, 0), 2, self.to_right).wait_recv()
            self.copy(self.block(self.far, 1), 3, self.to_left).wait_recv()

    def drain(self):
        self.copy(self.block(self.me, None), 0, self.to_right).wait_send()
        self.copy(self.block(self.me, None), 1, self.to_left).wait_send()
        if self.direct:
            self.copy(self.block(self.me, None), 2, self.to_far).wait_send()
        else:
            self.copy(self.block(self.left, 0), 2, self.to_right).wait_send()
            self.copy(self.block(self.right, 1), 3, self.to_left).wait_send()


def half_rows(half):
    return slice(None) if half is None else slice(32 * half, 32 * half + 32)


def half_blocks(half):
    return slice(None) if half is None else slice(2 * half, 2 * half + 2)


def matmul(a, b, dims=((1,), (0,)), precision=None):
    return lax.dot_general(a, b, (dims, ((), ())), precision=precision, preferred_element_type=F32)


def silu(value):
    half = 0.5 * value
    return half + half * jnp.tanh(half)


def kernel(
    bias_in,
    rate_in,
    tokens_in,
    gain_in,
    xw_in,
    zw_in,
    bw_in,
    cw_in,
    dw_in,
    xt_in,
    bt_in,
    ct_in,
    og_in,
    ow_in,
    out_ref,
    bias_ref,
    rate_ref,
    tokens_ref,
    gain_ref,
    dw_ref,
    taps_ref,
    og_ref,
    T,
    WA,
    WB,
    OYZ,
    O,
    E,
    Z,
    DT,
    CUM,
    XS,
    BS,
    CS,
    Y,
    U,
    SS,
    RS,
    SR,
    RR,
    ROW,
    GT,
    G,
    ring_send,
    ring_recv,
    pair_send,
    pair_recv,
    halo_send,
    halo_recv,
    state_send,
    state_recv,
    back_send,
    back_recv,
    mix_send,
    mix_recv,
    local_sem,
    load_sem,
):
    z, y = lax.axis_index("sp_0"), lax.axis_index("sp_1")
    x, c = lax.axis_index("tp_0"), lax.axis_index("tp_1")
    place = (z, y, x, c)
    sp, tp = z * 4 + y, x * 2 + c
    other = 1 - c
    partner = (z, y, x, other)

    def sp_device(i):
        return (i // 4, lax.rem(i, 4), x, c)

    def tp_device(i):
        return (z, y, i // 2, lax.rem(i, 2))

    barrier = pltpu.get_barrier_semaphore()
    for step in (1, 2, 3):
        for axis in range(3):
            near = tuple(lax.rem(p + step, 4) if k == axis else p for k, p in enumerate(place))
            pl.semaphore_signal(barrier, inc=1, device_id=near, device_id_type=MESH)
    pl.semaphore_signal(barrier, inc=1, device_id=partner, device_id_type=MESH)

    loads = (
        (xw_in, WA.at[z, y, :, 0:128]),
        (bw_in, WA.at[z, y, :, 128:256]),
        (cw_in, WB.at[z, y, :, 0:128]),
        (zw_in, WB.at[z, y, :, 128:256]),
        (dw_in, dw_ref),
        (ow_in, OYZ.at[z, y]),
        (gain_in, gain_ref),
        *((tokens_in.at[s], tokens_ref.at[s]) for s in range(SEQS)),
        (xt_in, taps_ref.at[0]),
        (bt_in, taps_ref.at[1]),
        (ct_in, taps_ref.at[2]),
        (og_in, og_ref),
        (bias_in, bias_ref),
        (rate_in, rate_ref),
    )
    loads = [pltpu.make_async_copy(*pair, load_sem.at[k]) for k, pair in enumerate(loads)]
    for load in loads:
        load.start()

    lane = lax.broadcasted_iota(jnp.int32, (1, LANES), 1)
    low = lane < 64

    head_at = lax.broadcasted_iota(jnp.int32, (2, LANES), 0)
    lane_at = lax.broadcasted_iota(jnp.int32, (2, LANES), 1)
    spread = (lane_at // 64 == head_at).astype(BF16)
    for load in loads[0:7]:
        load.wait()
    WB[z, y, :, 256:384] = matmul(dw_ref[...], spread, ((0,), (0,))).astype(BF16)

    def normed(s):
        loads[7 + s].wait()
        source = tokens_ref[s].astype(F32)
        scale = lax.rsqrt(jnp.mean(source * source, axis=-1, keepdims=True) + epsilon)
        T[s, pl.ds(pl.multiple_of(tp * ROWS, ROWS), ROWS), :] = (
            source * scale * gain_ref[...]
        ).astype(BF16)

    own_columns = pl.multiple_of((c * 4 + x) * LANES, LANES)
    pl.semaphore_wait(barrier, 10)

    def token_block(s):
        def block(i, half):
            start = (i * 2 + c) * ROWS + (0 if half is None else 32 * half)
            rows = ROWS if half is None else 32
            return T.at[s, pl.ds(pl.multiple_of(start, 32), rows), :]

        return block

    ring = lambda axis, block, number, direct=False: Ring(
        place, axis, block, ring_send, ring_recv, number, direct
    )
    tokens = [ring(2, token_block(s), s) for s in range(SEQS)]
    wa1 = ring(1, lambda i, h: WA.at[z, i, half_rows(h)], 4, True)
    wb1 = ring(0, lambda i, h: WB.at[i, y, half_rows(h)], 5, True)
    shifted = lambda i, k: lax.rem(i + k, 4)
    wa2 = [ring(0, lambda i, h, k=k: WA.at[i, shifted(y, k), half_rows(h)], 6 + k) for k in range(4)]
    wb2 = [ring(1, lambda i, h, k=k: WB.at[shifted(z, k), i, half_rows(h)], 10 + k) for k in range(4)]
    oy = ring(1, lambda i, h: OYZ.at[z, i], 14, True)
    oz = ring(0, lambda i, h: OYZ.at[i], 15, True)

    def out_rows(core, i, half):
        rows = LANES if half is None else 64
        start = i * LANES + (0 if half is None else 64 * half)
        return O.at[core, pl.ds(pl.multiple_of(start, 64), rows), :]

    ox = ring(2, lambda i, h: out_rows(c, i, h), 16)

    def pair_copy(s, k, core):
        i, half = (
            (x, None),
            (tokens[s].left, None),
            (tokens[s].right, None),
            (tokens[s].far, 0),
            (tokens[s].far, 1),
        )[k]
        start = (i * 2 + core) * ROWS + (0 if half is None else 32 * half)
        rows = ROWS if half is None else 32
        ref = T.at[s, pl.ds(pl.multiple_of(start, 32), rows), :]
        return remote(ref, ref, pair_send.at[s, k], pair_recv.at[s, k], partner)

    def out_pair(k, core):
        i, half = ((x, None), (ox.left, None), (ox.right, None), (ox.far, 0), (ox.far, 1))[k]
        ref = out_rows(core, i, half)
        return remote(ref, ref, pair_send.at[SEQS, k], pair_recv.at[SEQS, k], partner)

    def out_own():
        block = OYZ[...].reshape(WIDTH, LANES).astype(F32).T.astype(BF16)
        O[c, pl.ds(pl.multiple_of(x * LANES, LANES), LANES), :] = block
        ox.own()
        out_pair(0, c).start()

    def out_near():
        ox.near()
        out_pair(1, c).start()
        out_pair(2, c).start()

    def out_last():
        ox.last()
        out_pair(3, c).start()
        out_pair(4, c).start()

    def out_pairs():
        for k in range(5):
            out_pair(k, other).wait_recv()

    def token_own(s):
        tokens[s].own()
        pair_copy(s, 0, c).start()

    def token_near(s):
        tokens[s].near()
        pair_copy(s, 1, c).start()
        pair_copy(s, 2, c).start()

    def token_last(s):
        tokens[s].last()
        pair_copy(s, 3, c).start()
        pair_copy(s, 4, c).start()

    wa1.own()
    wb1.own()
    wa2[0].own()
    wb2[0].own()
    oy.own()
    normed(0)
    token_own(0)
    normed(1)
    token_own(1)
    normed(2)
    normed(3)
    wa1.near()
    wa2[1].own()
    wa2[3].own()
    wb1.near()
    wb2[1].own()
    wb2[3].own()
    wa1.last()
    wa2[2].own()
    wb1.last()
    wb2[2].own()
    wa2[0].near()
    wb2[0].near()
    token_near(0)
    token_own(2)
    token_own(3)
    wa2[1].near()
    wa2[3].near()
    wb2[1].near()
    wb2[3].near()
    token_near(1)
    oy.near()
    oy.last()
    oz.own()
    wa2[2].near()
    wb2[2].near()
    token_last(0)
    wa2[0].last()
    wa2[1].last()
    wa2[3].last()
    wb2[0].last()
    wb2[1].last()
    wb2[3].last()
    token_near(2)
    wa2[2].last()
    wb2[2].last()

    for load in loads[11:]:
        load.wait()
    bias = jnp.where(low, bias_ref[0], bias_ref[1])
    rate = jnp.where(low, rate_ref[0], rate_ref[1])
    row_at = lax.broadcasted_iota(jnp.int32, (CHUNK, CHUNK), 0)
    column_at = lax.broadcasted_iota(jnp.int32, (CHUNK, CHUNK), 1)
    lower = row_at >= column_at
    ones_below = lower.astype(BF16)
    tiles = [slice(k * ROWS, (k + 1) * ROWS) for k in range(SPAN // ROWS)]
    following = sp_device(lax.rem(sp + 1, 16))

    def packed(state, log):
        log = jnp.broadcast_to(log, (16, LANES))
        return jnp.concatenate([state, log], axis=0).astype(BF16)

    def share(source, slots, axis, send, recv):
        for k in (1, 3, 2):
            there = tuple(lax.rem(p + k, 4) if j == axis else p for j, p in enumerate(place))
            remote(source, slots.at[place[axis]], send, recv, there).start()
        slots[place[axis]] = source[...]

    def halo(s):
        return remote(
            E.at[s, :, SPAN : SPAN + 8, :],
            E.at[s, :, 0:8, :],
            halo_send.at[s],
            halo_recv.at[s],
            following,
        )

    def token_pair(s, first, last):
        for k in range(first, last):
            pair_copy(s, k, other).wait_recv()

    def halo_in(s):
        halo(s).wait_recv()

    def state_in(s):
        remote(
            RS.at[s, 0:3], RS.at[s, 0:3], state_send.at[s], state_recv.at[s], partner
        ).wait_recv()

    def back_in(s):
        remote(
            RR.at[s, 0:3], RR.at[s, 0:3], back_send.at[s], back_recv.at[s], partner
        ).wait_recv()

    def project(s):
        product = matmul(T[s], WA[...].reshape(WIDTH, 256))
        E[s, 0, 8 : SPAN + 8, :] = product[:, 0:128]
        E[s, 1, 8 : SPAN + 8, :] = product[:, 128:256]
        product = matmul(T[s], WB[...].reshape(WIDTH, 384))
        E[s, 2, 8 : SPAN + 8, :] = product[:, 0:128]
        Z[s] = product[:, 128:256]
        DT[s] = product[:, 256:384]
        halo(s).start()

    def gate(s):
        for rows in tiles:
            Z[s, rows, :] = silu(Z[s, rows, :])

    def steps(s):
        for rows in tiles:
            step = DT[s, rows, :] + bias
            step = jnp.maximum(step, 0.0) + jnp.log1p(jnp.exp(-jnp.abs(step)))
            DT[s, rows, :] = step
            XS[s, rows, :] = (-(step * rate) / LENGTH).astype(BF16)
        for k in range(2):
            rows = slice(k * CHUNK, (k + 1) * CHUNK)
            CUM[s, rows, :] = matmul(ones_below, XS[s, rows, :])

    def conv_tail(s):
        convolve(s, tiles[1:])
        gains(s, 1)

    def conv_head(s):
        for k in range(3):
            E[s, k, 0:8, :] = jnp.where(sp == 0, 0.0, E[s, k, 0:8, :])
        convolve(s, tiles[:1])

    def convolve(s, some):
        for k in range(3):
            taps = [taps_ref[k, offset : offset + 1, :] for offset in range(CONV)]
            for rows in some:
                start = rows.start + 5
                running = taps[0] * E[s, k, start : start + ROWS, :]
                for offset in range(1, CONV):
                    first = start + offset
                    running = running + taps[offset] * E[s, k, first : first + ROWS, :]
                running = silu(running)
                if k == 0:
                    decayed = DT[s, rows, :] * jnp.exp(-CUM[s, rows, :])
                    XS[s, rows, :] = (running * decayed).astype(BF16)
                elif k == 1:
                    BS[s, rows, :] = running.astype(BF16)
                else:
                    CS[s, rows, :] = running.astype(BF16)

    def gains(s, k):
        rows = slice(k * CHUNK, (k + 1) * CHUNK)
        U[s, k] = matmul(BS[s, rows, :], XS[s, rows, :], ((0,), (0,)))

    def states(s):
        gains(s, 0)
        first, second = CUM[s, CHUNK - 1 : CHUNK, :], CUM[s, SPAN - 1 : SPAN, :]
        final = jnp.exp(second) * (jnp.exp(first) * U[s, 0] + U[s, 1])
        SS[s] = packed(final, first + second)
        share(SS.at[s], RS.at[s], 1, state_send.at[s], state_recv.at[s])

    def inside(s):
        for k in range(2):
            rows = slice(k * CHUNK, (k + 1) * CHUNK)
            scores = matmul(CS[s, rows, :], BS[s, rows, :], ((1,), (1,)))
            scores = jnp.where(lower, scores, 0.0).astype(BF16)
            Y[s, rows, :] = matmul(scores, XS[s, rows, :])

    def scan(s):
        before, before_log = jnp.zeros((LANES, LANES), F32), jnp.zeros((1, LANES), F32)
        total, total_log = before, before_log
        for i in range(4):
            piece = RS[s, i].astype(F32)
            log = piece[LANES : LANES + 1]
            total = jnp.exp(log) * total + piece[0:LANES]
            total_log = total_log + log
            if i < 3:
                before = jnp.where(i + 1 == y, total, before)
                before_log = jnp.where(i + 1 == y, total_log, before_log)
        ROW[s, 0:LANES] = before
        ROW[s, LANES : LANES + 1] = jnp.exp(before_log)
        SR[s] = packed(total, total_log)
        share(SR.at[s], RR.at[s], 0, back_send.at[s], back_recv.at[s])

    def finish(s):
        total = jnp.zeros((LANES, LANES), F32)
        entering = total
        for i in range(3):
            piece = RR[s, i].astype(F32)
            total = jnp.exp(piece[LANES : LANES + 1]) * total + piece[0:LANES]
            entering = jnp.where(i + 1 == z, total, entering)
        entering = ROW[s, LANES : LANES + 1] * entering + ROW[s, 0:LANES]
        for k in range(2):
            rows = slice(k * CHUNK, (k + 1) * CHUNK)
            Y[s, rows, :] += matmul(CS[s, rows, :], entering.astype(BF16))
            if k == 0:
                grown = jnp.exp(CUM[s, CHUNK - 1 : CHUNK, :])
                entering = grown * (entering + U[s, 0])
        for rows in tiles:
            gated = Y[s, rows, :] * jnp.exp(CUM[s, rows, :]) * Z[s, rows, :]
            scale = lax.rsqrt(jnp.mean(gated * gated, axis=-1, keepdims=True) + epsilon)
            GT[s, rows, :] = (gated * scale * og_ref[...]).astype(BF16)

        def send(k, _):
            i = lax.rem(tp + k, 8)
            remote(
                GT.at[s, pl.ds(pl.multiple_of(i * ROWS, ROWS), ROWS), :],
                G.at[s, :, pl.ds(own_columns, LANES)],
                mix_send.at[s],
                mix_recv.at[s],
                tp_device(i),
            ).start()
            return 0

        lax.fori_loop(1, 8, send, 0)
        own(s).start()

    def own(s):
        return pltpu.make_async_copy(
            GT.at[s, pl.ds(pl.multiple_of(tp * ROWS, ROWS), ROWS), :],
            G.at[s, :, pl.ds(own_columns, LANES)],
            local_sem.at[s],
        )

    def mixed_in(s):
        remote(
            G.at[s, :, 0:896], G.at[s, :, 0:896], mix_send.at[s], mix_recv.at[s], partner
        ).wait_recv()
        own(s).wait()

    def multiply(first, last):
        gathered = G[first:last].reshape((last - first) * ROWS, WIDTH)
        result = matmul(gathered, O[...].reshape(WIDTH, WIDTH))
        out_ref[first:last] = result.astype(BF16).reshape(last - first, ROWS, WIDTH)

    token_pair(0, 0, 5)
    project(0)
    steps(0)
    conv_tail(0)
    token_near(3)
    oz.near()
    oz.last()
    out_own()
    token_last(1)
    halo_in(0)
    conv_head(0)
    states(0)
    token_last(2)
    inside(0)
    gate(0)
    token_pair(1, 0, 5)
    project(1)
    token_last(3)
    token_pair(2, 0, 5)
    project(2)
    steps(1)
    conv_tail(1)
    halo_in(1)
    conv_head(1)
    states(1)
    token_pair(3, 0, 5)
    project(3)
    state_in(0)
    scan(0)
    steps(2)
    conv_tail(2)
    halo_in(2)
    conv_head(2)
    states(2)
    steps(3)
    conv_tail(3)
    halo_in(3)
    conv_head(3)
    states(3)
    out_near()
    state_in(1)
    scan(1)
    back_in(0)
    finish(0)
    gate(1)
    inside(1)
    state_in(2)
    scan(2)
    gate(2)
    inside(2)
    gate(3)
    inside(3)
    state_in(3)
    scan(3)
    back_in(1)
    finish(1)
    out_last()
    back_in(2)
    finish(2)
    back_in(3)
    finish(3)
    out_pairs()
    mixed_in(0)
    mixed_in(1)
    mixed_in(2)
    multiply(0, 3)
    mixed_in(3)
    multiply(3, 4)

    for each in (*tokens, wa1, wb1, *wa2, *wb2, oy, oz, ox):
        each.drain()
    for k in range(5):
        out_pair(k, c).wait_send()
    for s in range(SEQS):
        for k in range(5):
            pair_copy(s, k, c).wait_send()
        halo(s).wait_send()
        remote(
            RS.at[s, 0:3], RS.at[s, 0:3], state_send.at[s], state_recv.at[s], partner
        ).wait_send()
        remote(
            RR.at[s, 0:3], RR.at[s, 0:3], back_send.at[s], back_recv.at[s], partner
        ).wait_send()
        remote(
            G.at[s, :, 0:896], G.at[s, :, 0:896], mix_send.at[s], mix_recv.at[s], partner
        ).wait_send()


def local(
    tokens,
    norm_gain,
    x_weight,
    z_weight,
    b_weight,
    c_weight,
    dt_weight,
    x_conv,
    b_conv,
    c_conv,
    dt_bias,
    decay_rate,
    out_gain,
    out_weight,
):
    hbm = pl.BlockSpec(memory_space=pltpu.HBM)
    dma = pltpu.SemaphoreType.DMA
    return pl.pallas_call(
        kernel,
        out_shape=pltpu.VMEM(tokens.shape, BF16),
        in_specs=[hbm] * 14,
        out_specs=pl.BlockSpec(memory_space=pltpu.VMEM),
        scratch_shapes=[
            pltpu.SMEM((2,), F32),
            pltpu.SMEM((2,), F32),
            pltpu.VMEM((SEQS, ROWS, WIDTH), BF16),
            pltpu.VMEM((1, WIDTH), F32),
            pltpu.VMEM((2, ROWS), BF16),
            pltpu.VMEM((3, CONV, LANES), F32),
            pltpu.VMEM((1, LANES), F32),
            pltpu.VMEM((SEQS, SPAN, WIDTH), BF16),
            pltpu.VMEM((4, 4, ROWS, 256), BF16),
            pltpu.VMEM((4, 4, ROWS, 384), BF16),
            pltpu.VMEM((4, 4, ROWS, LANES), BF16),
            pltpu.VMEM((2, 512, WIDTH), BF16),
            pltpu.VMEM((SEQS, 3, SPAN + 8, LANES), F32),
            pltpu.VMEM((SEQS, SPAN, LANES), F32),
            pltpu.VMEM((SEQS, SPAN, LANES), F32),
            pltpu.VMEM((SEQS, SPAN, LANES), F32),
            pltpu.VMEM((SEQS, SPAN, LANES), BF16),
            pltpu.VMEM((SEQS, SPAN, LANES), BF16),
            pltpu.VMEM((SEQS, SPAN, LANES), BF16),
            pltpu.VMEM((SEQS, SPAN, LANES), F32),
            pltpu.VMEM((SEQS, 2, LANES, LANES), F32),
            pltpu.VMEM((SEQS, LANES + 16, LANES), BF16),
            pltpu.VMEM((SEQS, 4, LANES + 16, LANES), BF16),
            pltpu.VMEM((SEQS, LANES + 16, LANES), BF16),
            pltpu.VMEM((SEQS, 4, LANES + 16, LANES), BF16),
            pltpu.VMEM((SEQS, LANES + 8, LANES), F32),
            pltpu.VMEM((SEQS, SPAN, LANES), BF16),
            pltpu.VMEM((SEQS, ROWS, WIDTH), BF16),
            dma((17, 4)),
            dma((17, 4)),
            dma((SEQS + 1, 5)),
            dma((SEQS + 1, 5)),
            dma((SEQS,)),
            dma((SEQS,)),
            dma((SEQS,)),
            dma((SEQS,)),
            dma((SEQS,)),
            dma((SEQS,)),
            dma((SEQS,)),
            dma((SEQS,)),
            dma((SEQS,)),
            dma((17,)),
        ],
        compiler_params=pltpu.CompilerParams(
            collective_id=0, has_side_effects=True, vmem_limit_bytes=60 * 1024 * 1024
        ),
        name="mixer",
    )(
        dt_bias,
        decay_rate,
        tokens,
        norm_gain.reshape(1, -1),
        x_weight,
        z_weight,
        b_weight,
        c_weight,
        dt_weight.T,
        x_conv,
        b_conv,
        c_conv,
        out_gain.reshape(1, -1),
        out_weight.T,
    )


def solution(mesh):
    torus = Mesh(mesh.devices.reshape(4, 4, 4, 2), SP_TP)
    return jax.shard_map(
        local,
        mesh=torus,
        in_specs=(
            P(None, SP_TP, None),
            P(),
            P(SP, TP),
            P(SP, TP),
            P(SP, TP),
            P(SP, TP),
            P(SP, TP),
            P(None, TP),
            P(None, TP),
            P(None, TP),
            P(TP),
            P(TP),
            P(TP),
            P(TP, SP),
        ),
        out_specs=P(None, SP_TP, None),
        check_vma=False,
    )
```

```python
import functools

import jax
import jax.numpy as jnp
from jax import lax
from jax.experimental import pallas as pl
from jax.experimental.pallas import tpu as pltpu
from jax.sharding import Mesh
from jax.sharding import PartitionSpec as P

CONV = 4
SP = ("sp_0", "sp_1")
TP = ("tp_0", "tp_1")
SP_TP = ("sp_0", "sp_1", "tp_0", "tp_1")
LENGTH = 8192
SEQS = 4
SPAN = 512
ROWS = 64
WIDTH = 1024
CHUNK = 256
LANES = 128
epsilon = 1e-05
MESH = pl.DeviceIdType.MESH
F32 = jnp.float32
BF16 = jnp.bfloat16


def remote(src, dst, send, recv, device):
    return pltpu.make_async_remote_copy(
        src_ref=src,
        dst_ref=dst,
        send_sem=send,
        recv_sem=recv,
        device_id=device,
        device_id_type=MESH,
    )


class Ring:
    def __init__(self, place, axis, block, sends, recvs, number, direct=False):
        self.block, self.sends, self.recvs, self.number = block, sends, recvs, number
        self.direct = direct
        self.me = place[axis]
        self.right, self.left = lax.rem(self.me + 1, 4), lax.rem(self.me + 3, 4)
        self.far = lax.rem(self.me + 2, 4)
        to = lambda i: tuple(i if k == axis else p for k, p in enumerate(place))
        self.to_right, self.to_left, self.to_far = to(self.right), to(self.left), to(self.far)

    def copy(self, ref, lane, device):
        return remote(
            ref, ref, self.sends.at[self.number, lane], self.recvs.at[self.number, lane], device
        )

    def own(self):
        self.copy(self.block(self.me, None), 0, self.to_right).start()
        self.copy(self.block(self.me, None), 1, self.to_left).start()
        if self.direct:
            self.copy(self.block(self.me, None), 2, self.to_far).start()

    def near(self):
        self.copy(self.block(self.left, None), 0, self.to_right).wait_recv()
        if not self.direct:
            self.copy(self.block(self.left, 0), 2, self.to_right).start()
        self.copy(self.block(self.right, None), 1, self.to_left).wait_recv()
        if not self.direct:
            self.copy(self.block(self.right, 1), 3, self.to_left).start()

    def last(self):
        if self.direct:
            self.copy(self.block(self.far, None), 2, self.to_far).wait_recv()
        else:
            self.copy(self.block(self.far, 0), 2, self.to_right).wait_recv()
            self.copy(self.block(self.far, 1), 3, self.to_left).wait_recv()

    def drain(self):
        self.copy(self.block(self.me, None), 0, self.to_right).wait_send()
        self.copy(self.block(self.me, None), 1, self.to_left).wait_send()
        if self.direct:
            self.copy(self.block(self.me, None), 2, self.to_far).wait_send()
        else:
            self.copy(self.block(self.left, 0), 2, self.to_right).wait_send()
            self.copy(self.block(self.right, 1), 3, self.to_left).wait_send()


def half_rows(half):
    return slice(None) if half is None else slice(32 * half, 32 * half + 32)


def half_blocks(half):
    return slice(None) if half is None else slice(2 * half, 2 * half + 2)


def matmul(a, b, dims=((1,), (0,)), precision=None):
    return lax.dot_general(a, b, (dims, ((), ())), precision=precision, preferred_element_type=F32)


def silu(value):
    half = 0.5 * value
    return half + half * jnp.tanh(half)


def kernel(
    bias_in,
    rate_in,
    tokens_in,
    gain_in,
    xw_in,
    zw_in,
    bw_in,
    cw_in,
    dw_in,
    xt_in,
    bt_in,
    ct_in,
    og_in,
    ow_in,
    out_ref,
    bias_ref,
    rate_ref,
    tokens_ref,
    gain_ref,
    dw_ref,
    taps_ref,
    og_ref,
    T,
    WA,
    WB,
    OYZ,
    O,
    E,
    Z,
    DT,
    CUM,
    XS,
    BS,
    CS,
    Y,
    U,
    SS,
    RS,
    SR,
    RR,
    ROW,
    GT,
    G,
    ring_send,
    ring_recv,
    pair_send,
    pair_recv,
    halo_send,
    halo_recv,
    state_send,
    state_recv,
    back_send,
    back_recv,
    mix_send,
    mix_recv,
    local_sem,
    load_sem,
    ready_sem,
):
    z, y = lax.axis_index("sp_0"), lax.axis_index("sp_1")
    x, c = lax.axis_index("tp_0"), lax.axis_index("tp_1")
    place = (z, y, x, c)
    sp, tp = z * 4 + y, x * 2 + c
    other = 1 - c
    partner = (z, y, x, other)

    def sp_device(i):
        return (i // 4, lax.rem(i, 4), x, c)

    def tp_device(i):
        return (z, y, i // 2, lax.rem(i, 2))

    barrier = pltpu.get_barrier_semaphore()

    def greet(semaphore, there):
        pl.semaphore_signal(semaphore, inc=1, device_id=there, device_id_type=MESH)

    for step in (1, 3):
        greet(barrier, (z, y, lax.rem(x + step, 4), c))
    greet(barrier, partner)
    for step in (1, 2, 3):
        pl.when(y + step < 4)(lambda step=step: greet(barrier, (z, y + step, x, c)))
        pl.when(z + step < 4)(lambda step=step: greet(barrier, (z + step, y, x, c)))

    loads = (
        (xw_in, WA.at[z, y, :, 0:128]),
        (bw_in, WA.at[z, y, :, 128:256]),
        (cw_in, WB.at[z, y, :, 0:128]),
        (zw_in, WB.at[z, y, :, 128:256]),
        (dw_in, dw_ref),
        (ow_in, OYZ.at[z, y]),
        (gain_in, gain_ref),
        *((tokens_in.at[s], tokens_ref.at[s]) for s in range(SEQS)),
        (xt_in, taps_ref.at[0]),
        (bt_in, taps_ref.at[1]),
        (ct_in, taps_ref.at[2]),
        (og_in, og_ref),
        (bias_in, bias_ref),
        (rate_in, rate_ref),
    )
    loads = [pltpu.make_async_copy(*pair, load_sem.at[k]) for k, pair in enumerate(loads)]
    for load in loads:
        load.start()

    lane = lax.broadcasted_iota(jnp.int32, (1, LANES), 1)
    low = lane < 64

    head_at = lax.broadcasted_iota(jnp.int32, (2, LANES), 0)
    lane_at = lax.broadcasted_iota(jnp.int32, (2, LANES), 1)
    spread = (lane_at // 64 == head_at).astype(BF16)
    for load in loads[0:7]:
        load.wait()
    WB[z, y, :, 256:384] = matmul(dw_ref[...], spread, ((0,), (0,))).astype(BF16)

    def normed(s):
        loads[7 + s].wait()
        source = tokens_ref[s].astype(F32)
        scale = lax.rsqrt(jnp.mean(source * source, axis=-1, keepdims=True) + epsilon)
        T[s, pl.ds(pl.multiple_of(tp * ROWS, ROWS), ROWS), :] = (
            source * scale * gain_ref[...]
        ).astype(BF16)

    own_columns = pl.multiple_of((c * 4 + x) * LANES, LANES)
    pl.semaphore_wait(barrier, 3 + y + z)
    for step in (1, 2, 3):
        pl.when(y >= step)(lambda step=step: greet(ready_sem, (z, y - step, x, c)))
        pl.when(z >= step)(lambda step=step: greet(ready_sem, (z - step, y, x, c)))

    def token_block(s):
        def block(i, half):
            start = (i * 2 + c) * ROWS + (0 if half is None else 32 * half)
            rows = ROWS if half is None else 32
            return T.at[s, pl.ds(pl.multiple_of(start, 32), rows), :]

        return block

    ring = lambda axis, block, number, direct=False: Ring(
        place, axis, block, ring_send, ring_recv, number, direct
    )
    tokens = [ring(2, token_block(s), s) for s in range(SEQS)]
    wa1 = ring(1, lambda i, h: WA.at[z, i, half_rows(h)], 4, True)
    wb1 = ring(0, lambda i, h: WB.at[i, y, half_rows(h)], 5, True)
    shifted = lambda i, k: lax.rem(i + k, 4)
    wa2 = [ring(0, lambda i, h, k=k: WA.at[i, shifted(y, k), half_rows(h)], 6 + k) for k in range(4)]
    wb2 = [ring(1, lambda i, h, k=k: WB.at[shifted(z, k), i, half_rows(h)], 10 + k) for k in range(4)]
    oy = ring(1, lambda i, h: OYZ.at[z, i], 14, True)
    oz = ring(0, lambda i, h: OYZ.at[i], 15, True)

    def out_rows(core, i, half):
        rows = LANES if half is None else 64
        start = i * LANES + (0 if half is None else 64 * half)
        return O.at[core, pl.ds(pl.multiple_of(start, 64), rows), :]

    ox = ring(2, lambda i, h: out_rows(c, i, h), 16)

    def pair_copy(s, k, core):
        i, half = (
            (x, None),
            (tokens[s].left, None),
            (tokens[s].right, None),
            (tokens[s].far, 0),
            (tokens[s].far, 1),
        )[k]
        start = (i * 2 + core) * ROWS + (0 if half is None else 32 * half)
        rows = ROWS if half is None else 32
        ref = T.at[s, pl.ds(pl.multiple_of(start, 32), rows), :]
        return remote(ref, ref, pair_send.at[s, k], pair_recv.at[s, k], partner)

    def out_pair(k, core):
        i, half = ((x, None), (ox.left, None), (ox.right, None), (ox.far, 0), (ox.far, 1))[k]
        ref = out_rows(core, i, half)
        return remote(ref, ref, pair_send.at[SEQS, k], pair_recv.at[SEQS, k], partner)

    def out_own():
        block = OYZ[...].reshape(WIDTH, LANES).astype(F32).T.astype(BF16)
        O[c, pl.ds(pl.multiple_of(x * LANES, LANES), LANES), :] = block
        ox.own()
        out_pair(0, c).start()

    def out_near():
        ox.near()
        out_pair(1, c).start()
        out_pair(2, c).start()

    def out_last():
        ox.last()
        out_pair(3, c).start()
        out_pair(4, c).start()

    def out_pairs():
        for k in range(5):
            out_pair(k, other).wait_recv()

    def token_own(s):
        tokens[s].own()
        pair_copy(s, 0, c).start()

    def token_near(s):
        tokens[s].near()
        pair_copy(s, 1, c).start()
        pair_copy(s, 2, c).start()

    def token_last(s):
        tokens[s].last()
        pair_copy(s, 3, c).start()
        pair_copy(s, 4, c).start()

    normed(0)
    token_own(0)
    pl.when(y + z < 6)(lambda: pl.semaphore_wait(ready_sem, 6 - y - z))
    wa1.own()
    wb1.own()
    wa2[0].own()
    wb2[0].own()
    oy.own()
    normed(1)
    token_own(1)
    normed(2)
    normed(3)
    wa1.near()
    wa2[1].own()
    wa2[3].own()
    wb1.near()
    wb2[1].own()
    wb2[3].own()
    wa1.last()
    wa2[2].own()
    wb1.last()
    wb2[2].own()
    wa2[0].near()
    wb2[0].near()
    token_near(0)
    token_own(2)
    token_own(3)
    wa2[1].near()
    wa2[3].near()
    wb2[1].near()
    wb2[3].near()
    token_near(1)
    oy.near()
    oy.last()
    oz.own()
    wa2[2].near()
    wb2[2].near()
    token_last(0)
    wa2[0].last()
    wa2[1].last()
    wa2[3].last()
    wb2[0].last()
    wb2[1].last()
    wb2[3].last()
    token_near(2)
    wa2[2].last()
    wb2[2].last()

    for load in loads[11:]:
        load.wait()
    bias = jnp.where(low, bias_ref[0], bias_ref[1])
    rate = jnp.where(low, rate_ref[0], rate_ref[1])
    row_at = lax.broadcasted_iota(jnp.int32, (CHUNK, CHUNK), 0)
    column_at = lax.broadcasted_iota(jnp.int32, (CHUNK, CHUNK), 1)
    lower = row_at >= column_at
    ones_below = lower.astype(BF16)
    tiles = [slice(k * ROWS, (k + 1) * ROWS) for k in range(SPAN // ROWS)]
    following = sp_device(lax.rem(sp + 1, 16))

    def packed(state, log):
        log = jnp.broadcast_to(log, (16, LANES))
        return jnp.concatenate([state, log], axis=0).astype(BF16)

    def share_row(s):
        for k in (1, 3, 2):
            there = (z, lax.rem(y + k, 4), x, c)
            copy = remote(SS.at[s], RS.at[s, y], state_send.at[s, k], state_recv.at[s, y], there)
            pl.when((y + k < 4) | (z < 3))(copy.start)
        RS[s, y] = SS[s]

    def share_up(s):
        for k in (1, 2, 3):
            there = (lax.rem(z + k, 4), y, x, c)
            copy = remote(SR.at[s], RR.at[s, z], back_send.at[s, k], back_recv.at[s, z], there)
            pl.when(z + k < 4)(copy.start)

    def states_out(s):
        for k in (1, 3, 2):
            copy = remote(
                SS.at[s], RS.at[s, y], state_send.at[s, k], state_recv.at[s, y], partner
            )
            pl.when((y + k < 4) | (z < 3))(copy.wait_send)
            copy = remote(SR.at[s], RR.at[s, z], back_send.at[s, k], back_recv.at[s, z], partner)
            pl.when(z + k < 4)(copy.wait_send)

    def halo(s):
        return remote(
            E.at[s, :, SPAN : SPAN + 8, :],
            E.at[s, :, 0:8, :],
            halo_send.at[s],
            halo_recv.at[s],
            following,
        )

    def token_pair(s, first, last):
        for k in range(first, last):
            pair_copy(s, k, other).wait_recv()

    def halo_in(s):
        pl.when(sp > 0)(halo(s).wait_recv)

    def state_in(s):
        for k in (1, 3, 2):
            i = lax.rem(y + k, 4)
            copy = remote(
                SS.at[s], RS.at[s, i], state_send.at[s, k], state_recv.at[s, i], partner
            )
            pl.when((i < y) | (z < 3))(copy.wait_recv)

    def back_in(s):
        for i in range(3):
            copy = remote(SR.at[s], RR.at[s, i], back_send.at[s, 0], back_recv.at[s, i], partner)
            pl.when(i < z)(copy.wait_recv)

    def project(s):
        product = matmul(T[s], WA[...].reshape(WIDTH, 256))
        E[s, 0, 8 : SPAN + 8, :] = product[:, 0:128]
        E[s, 1, 8 : SPAN + 8, :] = product[:, 128:256]
        product = matmul(T[s], WB[...].reshape(WIDTH, 384))
        E[s, 2, 8 : SPAN + 8, :] = product[:, 0:128]
        Z[s] = product[:, 128:256]
        DT[s] = product[:, 256:384]
        pl.when(sp < 15)(halo(s).start)

    def gate(s):
        for rows in tiles:
            Z[s, rows, :] = silu(Z[s, rows, :])

    def steps(s):
        for rows in tiles:
            step = DT[s, rows, :] + bias
            step = jnp.maximum(step, 0.0) + jnp.log1p(jnp.exp(-jnp.abs(step)))
            DT[s, rows, :] = step
            XS[s, rows, :] = (-(step * rate) / LENGTH).astype(BF16)
        for k in range(2):
            rows = slice(k * CHUNK, (k + 1) * CHUNK)
            CUM[s, rows, :] = matmul(ones_below, XS[s, rows, :])

    def conv_tail(s):
        convolve(s, tiles[1:])
        gains(s, 1)

    def conv_head(s):
        for k in range(3):
            E[s, k, 0:8, :] = jnp.where(sp == 0, 0.0, E[s, k, 0:8, :])
        convolve(s, tiles[:1])

    def convolve(s, some):
        for k in range(3):
            taps = [taps_ref[k, offset : offset + 1, :] for offset in range(CONV)]
            for rows in some:
                start = rows.start + 5
                running = taps[0] * E[s, k, start : start + ROWS, :]
                for offset in range(1, CONV):
                    first = start + offset
                    running = running + taps[offset] * E[s, k, first : first + ROWS, :]
                running = silu(running)
                if k == 0:
                    decayed = DT[s, rows, :] * jnp.exp(-CUM[s, rows, :])
                    XS[s, rows, :] = (running * decayed).astype(BF16)
                elif k == 1:
                    BS[s, rows, :] = running.astype(BF16)
                else:
                    CS[s, rows, :] = running.astype(BF16)

    def gains(s, k):
        rows = slice(k * CHUNK, (k + 1) * CHUNK)
        U[s, k] = matmul(BS[s, rows, :], XS[s, rows, :], ((0,), (0,)))

    def states(s):
        gains(s, 0)
        first, second = CUM[s, CHUNK - 1 : CHUNK, :], CUM[s, SPAN - 1 : SPAN, :]
        final = jnp.exp(second) * (jnp.exp(first) * U[s, 0] + U[s, 1])
        SS[s] = packed(final, first + second)
        share_row(s)

    def inside(s):
        for k in range(2):
            rows = slice(k * CHUNK, (k + 1) * CHUNK)
            scores = matmul(CS[s, rows, :], BS[s, rows, :], ((1,), (1,)))
            scores = jnp.where(lower, scores, 0.0).astype(BF16)
            Y[s, rows, :] = matmul(scores, XS[s, rows, :])

    def scan(s):
        before, before_log = jnp.zeros((LANES, LANES), F32), jnp.zeros((1, LANES), F32)
        total, total_log = before, before_log
        for i in range(4):
            piece = RS[s, i].astype(F32)
            log = piece[LANES : LANES + 1]
            total = jnp.exp(log) * total + piece[0:LANES]
            total_log = total_log + log
            if i < 3:
                before = jnp.where(i + 1 == y, total, before)
                before_log = jnp.where(i + 1 == y, total_log, before_log)
        ROW[s, 0:LANES] = before
        ROW[s, LANES : LANES + 1] = jnp.exp(before_log)
        SR[s] = packed(total, total_log)
        share_up(s)

    def finish(s):
        total = jnp.zeros((LANES, LANES), F32)
        entering = total
        for i in range(3):
            piece = RR[s, i].astype(F32)
            total = jnp.exp(piece[LANES : LANES + 1]) * total + piece[0:LANES]
            entering = jnp.where(i + 1 == z, total, entering)
        entering = ROW[s, LANES : LANES + 1] * entering + ROW[s, 0:LANES]
        for k in range(2):
            rows = slice(k * CHUNK, (k + 1) * CHUNK)
            Y[s, rows, :] += matmul(CS[s, rows, :], entering.astype(BF16))
            if k == 0:
                grown = jnp.exp(CUM[s, CHUNK - 1 : CHUNK, :])
                entering = grown * (entering + U[s, 0])
        for rows in tiles:
            gated = Y[s, rows, :] * jnp.exp(CUM[s, rows, :]) * Z[s, rows, :]
            scale = lax.rsqrt(jnp.mean(gated * gated, axis=-1, keepdims=True) + epsilon)
            GT[s, rows, :] = (gated * scale * og_ref[...]).astype(BF16)

        def send(k, _):
            i = lax.rem(tp + k, 8)
            remote(
                GT.at[s, pl.ds(pl.multiple_of(i * ROWS, ROWS), ROWS), :],
                G.at[s, :, pl.ds(own_columns, LANES)],
                mix_send.at[s],
                mix_recv.at[s],
                tp_device(i),
            ).start()
            return 0

        lax.fori_loop(1, 8, send, 0)
        own(s).start()

    def own(s):
        return pltpu.make_async_copy(
            GT.at[s, pl.ds(pl.multiple_of(tp * ROWS, ROWS), ROWS), :],
            G.at[s, :, pl.ds(own_columns, LANES)],
            local_sem.at[s],
        )

    def mixed_in(s):
        remote(
            G.at[s, :, 0:896], G.at[s, :, 0:896], mix_send.at[s], mix_recv.at[s], partner
        ).wait_recv()
        own(s).wait()

    def multiply(first, last):
        gathered = G[first:last].reshape((last - first) * ROWS, WIDTH)
        result = matmul(gathered, O[...].reshape(WIDTH, WIDTH))
        out_ref[first:last] = result.astype(BF16).reshape(last - first, ROWS, WIDTH)

    token_pair(0, 0, 5)
    project(0)
    steps(0)
    conv_tail(0)
    token_near(3)
    oz.near()
    oz.last()
    out_own()
    token_last(1)
    halo_in(0)
    conv_head(0)
    states(0)
    token_last(2)
    inside(0)
    gate(0)
    token_pair(1, 0, 5)
    project(1)
    token_last(3)
    token_pair(2, 0, 5)
    project(2)
    steps(1)
    conv_tail(1)
    halo_in(1)
    conv_head(1)
    states(1)
    token_pair(3, 0, 5)
    project(3)
    state_in(0)
    scan(0)
    steps(2)
    conv_tail(2)
    halo_in(2)
    conv_head(2)
    states(2)
    steps(3)
    conv_tail(3)
    halo_in(3)
    conv_head(3)
    states(3)
    out_near()
    state_in(1)
    scan(1)
    back_in(0)
    finish(0)
    gate(1)
    inside(1)
    state_in(2)
    scan(2)
    gate(2)
    inside(2)
    gate(3)
    inside(3)
    state_in(3)
    scan(3)
    back_in(1)
    finish(1)
    out_last()
    back_in(2)
    finish(2)
    back_in(3)
    finish(3)
    out_pairs()
    mixed_in(0)
    mixed_in(1)
    mixed_in(2)
    multiply(0, 3)
    mixed_in(3)
    multiply(3, 4)

    for each in (*tokens, wa1, wb1, *wa2, *wb2, oy, oz, ox):
        each.drain()
    for k in range(5):
        out_pair(k, c).wait_send()
    for s in range(SEQS):
        for k in range(5):
            pair_copy(s, k, c).wait_send()
        pl.when(sp < 15)(halo(s).wait_send)
        states_out(s)
        remote(
            G.at[s, :, 0:896], G.at[s, :, 0:896], mix_send.at[s], mix_recv.at[s], partner
        ).wait_send()


def local(
    tokens,
    norm_gain,
    x_weight,
    z_weight,
    b_weight,
    c_weight,
    dt_weight,
    x_conv,
    b_conv,
    c_conv,
    dt_bias,
    decay_rate,
    out_gain,
    out_weight,
):
    hbm = pl.BlockSpec(memory_space=pltpu.HBM)
    dma = pltpu.SemaphoreType.DMA
    return pl.pallas_call(
        kernel,
        out_shape=pltpu.VMEM(tokens.shape, BF16),
        in_specs=[hbm] * 14,
        out_specs=pl.BlockSpec(memory_space=pltpu.VMEM),
        scratch_shapes=[
            pltpu.SMEM((2,), F32),
            pltpu.SMEM((2,), F32),
            pltpu.VMEM((SEQS, ROWS, WIDTH), BF16),
            pltpu.VMEM((1, WIDTH), F32),
            pltpu.VMEM((2, ROWS), BF16),
            pltpu.VMEM((3, CONV, LANES), F32),
            pltpu.VMEM((1, LANES), F32),
            pltpu.VMEM((SEQS, SPAN, WIDTH), BF16),
            pltpu.VMEM((4, 4, ROWS, 256), BF16),
            pltpu.VMEM((4, 4, ROWS, 384), BF16),
            pltpu.VMEM((4, 4, ROWS, LANES), BF16),
            pltpu.VMEM((2, 512, WIDTH), BF16),
            pltpu.VMEM((SEQS, 3, SPAN + 8, LANES), F32),
            pltpu.VMEM((SEQS, SPAN, LANES), F32),
            pltpu.VMEM((SEQS, SPAN, LANES), F32),
            pltpu.VMEM((SEQS, SPAN, LANES), F32),
            pltpu.VMEM((SEQS, SPAN, LANES), BF16),
            pltpu.VMEM((SEQS, SPAN, LANES), BF16),
            pltpu.VMEM((SEQS, SPAN, LANES), BF16),
            pltpu.VMEM((SEQS, SPAN, LANES), F32),
            pltpu.VMEM((SEQS, 2, LANES, LANES), F32),
            pltpu.VMEM((SEQS, LANES + 16, LANES), BF16),
            pltpu.VMEM((SEQS, 4, LANES + 16, LANES), BF16),
            pltpu.VMEM((SEQS, LANES + 16, LANES), BF16),
            pltpu.VMEM((SEQS, 4, LANES + 16, LANES), BF16),
            pltpu.VMEM((SEQS, LANES + 8, LANES), F32),
            pltpu.VMEM((SEQS, SPAN, LANES), BF16),
            pltpu.VMEM((SEQS, ROWS, WIDTH), BF16),
            dma((17, 4)),
            dma((17, 4)),
            dma((SEQS + 1, 5)),
            dma((SEQS + 1, 5)),
            dma((SEQS,)),
            dma((SEQS,)),
            dma((SEQS, 4)),
            dma((SEQS, 4)),
            dma((SEQS, 4)),
            dma((SEQS, 4)),
            dma((SEQS,)),
            dma((SEQS,)),
            dma((SEQS,)),
            dma((17,)),
            pltpu.SemaphoreType.REGULAR,
        ],
        compiler_params=pltpu.CompilerParams(
            collective_id=0, has_side_effects=True, vmem_limit_bytes=60 * 1024 * 1024
        ),
        name="mixer",
    )(
        dt_bias,
        decay_rate,
        tokens,
        norm_gain.reshape(1, -1),
        x_weight,
        z_weight,
        b_weight,
        c_weight,
        dt_weight.T,
        x_conv,
        b_conv,
        c_conv,
        out_gain.reshape(1, -1),
        out_weight.T,
    )


def solution(mesh):
    torus = Mesh(mesh.devices.reshape(4, 4, 4, 2), SP_TP)
    return jax.shard_map(
        local,
        mesh=torus,
        in_specs=(
            P(None, SP_TP, None),
            P(),
            P(SP, TP),
            P(SP, TP),
            P(SP, TP),
            P(SP, TP),
            P(SP, TP),
            P(None, TP),
            P(None, TP),
            P(None, TP),
            P(TP),
            P(TP),
            P(TP),
            P(TP, SP),
        ),
        out_specs=P(None, SP_TP, None),
        check_vma=False,
    )
```

```python
import functools

import jax
import jax.numpy as jnp
from jax import lax
from jax.experimental import pallas as pl
from jax.experimental.pallas import tpu as pltpu
from jax.sharding import Mesh
from jax.sharding import PartitionSpec as P

CONV = 4
SP = ("sp_0", "sp_1")
TP = ("tp_0", "tp_1")
SP_TP = ("sp_0", "sp_1", "tp_0", "tp_1")
LENGTH = 8192
SEQS = 4
SPAN = 512
ROWS = 64
WIDTH = 1024
CHUNK = 256
LANES = 128
epsilon = 1e-05
MESH = pl.DeviceIdType.MESH
F32 = jnp.float32
BF16 = jnp.bfloat16


def remote(src, dst, send, recv, device):
    return pltpu.make_async_remote_copy(
        src_ref=src,
        dst_ref=dst,
        send_sem=send,
        recv_sem=recv,
        device_id=device,
        device_id_type=MESH,
    )


class Ring:
    def __init__(self, place, axis, block, sends, recvs, number, direct=False):
        self.block, self.sends, self.recvs, self.number = block, sends, recvs, number
        self.direct = direct
        self.me = place[axis]
        self.right, self.left = lax.rem(self.me + 1, 4), lax.rem(self.me + 3, 4)
        self.far = lax.rem(self.me + 2, 4)
        to = lambda i: tuple(i if k == axis else p for k, p in enumerate(place))
        self.to_right, self.to_left, self.to_far = to(self.right), to(self.left), to(self.far)

    def copy(self, ref, lane, device):
        return remote(
            ref, ref, self.sends.at[self.number, lane], self.recvs.at[self.number, lane], device
        )

    def own(self):
        self.copy(self.block(self.me, None), 0, self.to_right).start()
        self.copy(self.block(self.me, None), 1, self.to_left).start()
        if self.direct:
            self.copy(self.block(self.me, None), 2, self.to_far).start()

    def near(self):
        self.copy(self.block(self.left, None), 0, self.to_right).wait_recv()
        if not self.direct:
            self.copy(self.block(self.left, 0), 2, self.to_right).start()
        self.copy(self.block(self.right, None), 1, self.to_left).wait_recv()
        if not self.direct:
            self.copy(self.block(self.right, 1), 3, self.to_left).start()

    def last(self):
        if self.direct:
            self.copy(self.block(self.far, None), 2, self.to_far).wait_recv()
        else:
            self.copy(self.block(self.far, 0), 2, self.to_right).wait_recv()
            self.copy(self.block(self.far, 1), 3, self.to_left).wait_recv()

    def drain(self):
        self.copy(self.block(self.me, None), 0, self.to_right).wait_send()
        self.copy(self.block(self.me, None), 1, self.to_left).wait_send()
        if self.direct:
            self.copy(self.block(self.me, None), 2, self.to_far).wait_send()
        else:
            self.copy(self.block(self.left, 0), 2, self.to_right).wait_send()
            self.copy(self.block(self.right, 1), 3, self.to_left).wait_send()


def half_rows(half):
    return slice(None) if half is None else slice(32 * half, 32 * half + 32)


def half_blocks(half):
    return slice(None) if half is None else slice(2 * half, 2 * half + 2)


def matmul(a, b, dims=((1,), (0,)), precision=None):
    return lax.dot_general(a, b, (dims, ((), ())), precision=precision, preferred_element_type=F32)


def silu(value):
    half = 0.5 * value
    return half + half * jnp.tanh(half)


def kernel(
    bias_in,
    rate_in,
    tokens_in,
    gain_in,
    xw_in,
    zw_in,
    bw_in,
    cw_in,
    dw_in,
    xt_in,
    bt_in,
    ct_in,
    og_in,
    ow_in,
    out_ref,
    bias_ref,
    rate_ref,
    tokens_ref,
    gain_ref,
    dw_ref,
    taps_ref,
    og_ref,
    T,
    WA,
    WB,
    OYZ,
    O,
    E,
    Z,
    DT,
    CUM,
    XS,
    BS,
    CS,
    Y,
    U,
    SS,
    RS,
    SR,
    RR,
    ROW,
    GT,
    G,
    ring_send,
    ring_recv,
    pair_send,
    pair_recv,
    halo_send,
    halo_recv,
    state_send,
    state_recv,
    back_send,
    back_recv,
    mix_send,
    mix_recv,
    local_sem,
    load_sem,
):
    z, y = lax.axis_index("sp_0"), lax.axis_index("sp_1")
    x, c = lax.axis_index("tp_0"), lax.axis_index("tp_1")
    place = (z, y, x, c)
    sp, tp = z * 4 + y, x * 2 + c
    other = 1 - c
    partner = (z, y, x, other)

    def sp_device(i):
        return (i // 4, lax.rem(i, 4), x, c)

    def tp_device(i):
        return (z, y, i // 2, lax.rem(i, 2))

    barrier = pltpu.get_barrier_semaphore()

    def greet(semaphore, there):
        pl.semaphore_signal(semaphore, inc=1, device_id=there, device_id_type=MESH)

    for step in (1, 3):
        greet(barrier, (z, y, lax.rem(x + step, 4), c))
    greet(barrier, partner)
    for step in (1, 2, 3):
        greet(barrier, (z, lax.rem(y + step, 4), x, c))
        greet(barrier, (lax.rem(z + step, 4), y, x, c))

    loads = (
        (xw_in, WA.at[z, y, :, 0:128]),
        (bw_in, WA.at[z, y, :, 128:256]),
        (cw_in, WB.at[z, y, :, 0:128]),
        (zw_in, WB.at[z, y, :, 128:256]),
        (dw_in, dw_ref),
        (ow_in, OYZ.at[z, y]),
        (gain_in, gain_ref),
        *((tokens_in.at[s], tokens_ref.at[s]) for s in range(SEQS)),
        (xt_in, taps_ref.at[0]),
        (bt_in, taps_ref.at[1]),
        (ct_in, taps_ref.at[2]),
        (og_in, og_ref),
        (bias_in, bias_ref),
        (rate_in, rate_ref),
    )
    loads = [pltpu.make_async_copy(*pair, load_sem.at[k]) for k, pair in enumerate(loads)]
    for load in loads:
        load.start()

    lane = lax.broadcasted_iota(jnp.int32, (1, LANES), 1)
    low = lane < 64

    head_at = lax.broadcasted_iota(jnp.int32, (2, LANES), 0)
    lane_at = lax.broadcasted_iota(jnp.int32, (2, LANES), 1)
    spread = (lane_at // 64 == head_at).astype(BF16)
    for load in loads[0:7]:
        load.wait()
    WB[z, y, :, 256:384] = matmul(dw_ref[...], spread, ((0,), (0,))).astype(BF16)

    def normed(s):
        loads[7 + s].wait()
        source = tokens_ref[s].astype(F32)
        scale = lax.rsqrt(jnp.mean(source * source, axis=-1, keepdims=True) + epsilon)
        T[s, pl.ds(pl.multiple_of(tp * ROWS, ROWS), ROWS), :] = (
            source * scale * gain_ref[...]
        ).astype(BF16)

    own_columns = pl.multiple_of((c * 4 + x) * LANES, LANES)
    pl.semaphore_wait(barrier, 9)

    def token_block(s):
        def block(i, half):
            start = (i * 2 + c) * ROWS + (0 if half is None else 32 * half)
            rows = ROWS if half is None else 32
            return T.at[s, pl.ds(pl.multiple_of(start, 32), rows), :]

        return block

    ring = lambda axis, block, number, direct=False: Ring(
        place, axis, block, ring_send, ring_recv, number, direct
    )
    tokens = [ring(2, token_block(s), s) for s in range(SEQS)]
    wa1 = ring(1, lambda i, h: WA.at[z, i, half_rows(h)], 4, True)
    wb1 = ring(0, lambda i, h: WB.at[i, y, half_rows(h)], 5, True)
    shifted = lambda i, k: lax.rem(i + k, 4)
    wa2 = [ring(0, lambda i, h, k=k: WA.at[i, shifted(y, k), half_rows(h)], 6 + k) for k in range(4)]
    wb2 = [ring(1, lambda i, h, k=k: WB.at[shifted(z, k), i, half_rows(h)], 10 + k) for k in range(4)]
    oy = ring(1, lambda i, h: OYZ.at[z, i], 14, True)
    oz = ring(0, lambda i, h: OYZ.at[i], 15, True)

    def out_rows(core, i, half):
        rows = LANES if half is None else 64
        start = i * LANES + (0 if half is None else 64 * half)
        return O.at[core, pl.ds(pl.multiple_of(start, 64), rows), :]

    ox = ring(2, lambda i, h: out_rows(c, i, h), 16)

    def pair_copy(s, k, core):
        i, half = (
            (x, None),
            (tokens[s].left, None),
            (tokens[s].right, None),
            (tokens[s].far, 0),
            (tokens[s].far, 1),
        )[k]
        start = (i * 2 + core) * ROWS + (0 if half is None else 32 * half)
        rows = ROWS if half is None else 32
        ref = T.at[s, pl.ds(pl.multiple_of(start, 32), rows), :]
        return remote(ref, ref, pair_send.at[s, k], pair_recv.at[s, k], partner)

    def out_pair(k, core):
        i, half = ((x, None), (ox.left, None), (ox.right, None), (ox.far, 0), (ox.far, 1))[k]
        ref = out_rows(core, i, half)
        return remote(ref, ref, pair_send.at[SEQS, k], pair_recv.at[SEQS, k], partner)

    def out_own():
        block = OYZ[...].reshape(WIDTH, LANES).astype(F32).T.astype(BF16)
        O[c, pl.ds(pl.multiple_of(x * LANES, LANES), LANES), :] = block
        ox.own()
        out_pair(0, c).start()

    def out_near():
        ox.near()
        out_pair(1, c).start()
        out_pair(2, c).start()

    def out_last():
        ox.last()
        out_pair(3, c).start()
        out_pair(4, c).start()

    def out_pairs():
        for k in range(5):
            out_pair(k, other).wait_recv()

    def token_own(s):
        tokens[s].own()
        pair_copy(s, 0, c).start()

    def token_near(s):
        tokens[s].near()
        pair_copy(s, 1, c).start()
        pair_copy(s, 2, c).start()

    def token_last(s):
        tokens[s].last()
        pair_copy(s, 3, c).start()
        pair_copy(s, 4, c).start()

    wa1.own()
    wb1.own()
    wa2[0].own()
    wb2[0].own()
    normed(0)
    token_own(0)
    normed(1)
    token_own(1)
    normed(2)
    normed(3)
    wa1.near()
    wa2[1].own()
    wa2[3].own()
    wb1.near()
    wb2[1].own()
    wb2[3].own()
    wa1.last()
    wa2[2].own()
    wb1.last()
    wb2[2].own()
    oy.own()
    wa2[0].near()
    wb2[0].near()
    token_near(0)
    token_own(2)
    wa2[1].near()
    wa2[3].near()
    wb2[1].near()
    wb2[3].near()
    token_near(1)
    token_own(3)
    wa2[2].near()
    wb2[2].near()
    oy.near()
    oy.last()
    oz.own()
    token_last(0)
    wa2[0].last()
    wa2[1].last()
    wa2[3].last()
    wb2[0].last()
    wb2[1].last()
    wb2[3].last()
    token_near(2)
    wa2[2].last()
    wb2[2].last()

    for load in loads[11:]:
        load.wait()
    bias = jnp.where(low, bias_ref[0], bias_ref[1])
    rate = jnp.where(low, rate_ref[0], rate_ref[1])
    row_at = lax.broadcasted_iota(jnp.int32, (CHUNK, CHUNK), 0)
    column_at = lax.broadcasted_iota(jnp.int32, (CHUNK, CHUNK), 1)
    lower = row_at >= column_at
    ones_below = lower.astype(BF16)
    tiles = [slice(k * ROWS, (k + 1) * ROWS) for k in range(SPAN // ROWS)]
    following = sp_device(lax.rem(sp + 1, 16))

    def packed(state, log):
        log = jnp.broadcast_to(log, (16, LANES))
        return jnp.concatenate([state, log], axis=0).astype(BF16)

    def share_row(s):
        for k in (1, 3, 2):
            there = (z, lax.rem(y + k, 4), x, c)
            copy = remote(SS.at[s], RS.at[s, y], state_send.at[s, k], state_recv.at[s, y], there)
            pl.when((y + k < 4) | (z < 3))(copy.start)
        RS[s, y] = SS[s]

    def share_up(s):
        for k in (1, 2, 3):
            there = (lax.rem(z + k, 4), y, x, c)
            copy = remote(SR.at[s], RR.at[s, z], back_send.at[s, k], back_recv.at[s, z], there)
            pl.when(z + k < 4)(copy.start)

    def states_out(s):
        for k in (1, 3, 2):
            copy = remote(
                SS.at[s], RS.at[s, y], state_send.at[s, k], state_recv.at[s, y], partner
            )
            pl.when((y + k < 4) | (z < 3))(copy.wait_send)
            copy = remote(SR.at[s], RR.at[s, z], back_send.at[s, k], back_recv.at[s, z], partner)
            pl.when(z + k < 4)(copy.wait_send)

    def halo(s):
        return remote(
            E.at[s, :, SPAN : SPAN + 8, :],
            E.at[s, :, 0:8, :],
            halo_send.at[s],
            halo_recv.at[s],
            following,
        )

    def token_pair(s, first, last):
        for k in range(first, last):
            pair_copy(s, k, other).wait_recv()

    def halo_in(s):
        pl.when(sp > 0)(halo(s).wait_recv)

    def state_in(s):
        for k in (1, 3, 2):
            i = lax.rem(y + k, 4)
            copy = remote(
                SS.at[s], RS.at[s, i], state_send.at[s, k], state_recv.at[s, i], partner
            )
            pl.when((i < y) | (z < 3))(copy.wait_recv)

    def back_in(s):
        for i in range(3):
            copy = remote(SR.at[s], RR.at[s, i], back_send.at[s, 0], back_recv.at[s, i], partner)
            pl.when(i < z)(copy.wait_recv)

    def project(s):
        product = matmul(T[s], WA[...].reshape(WIDTH, 256))
        E[s, 0, 8 : SPAN + 8, :] = product[:, 0:128]
        E[s, 1, 8 : SPAN + 8, :] = product[:, 128:256]
        product = matmul(T[s], WB[...].reshape(WIDTH, 384))
        E[s, 2, 8 : SPAN + 8, :] = product[:, 0:128]
        Z[s] = product[:, 128:256]
        DT[s] = product[:, 256:384]
        pl.when(sp < 15)(halo(s).start)

    def gate(s):
        for rows in tiles:
            Z[s, rows, :] = silu(Z[s, rows, :])

    def steps(s):
        for rows in tiles:
            step = DT[s, rows, :] + bias
            step = jnp.maximum(step, 0.0) + jnp.log1p(jnp.exp(-jnp.abs(step)))
            DT[s, rows, :] = step
            XS[s, rows, :] = (-(step * rate) / LENGTH).astype(BF16)
        for k in range(2):
            rows = slice(k * CHUNK, (k + 1) * CHUNK)
            CUM[s, rows, :] = matmul(ones_below, XS[s, rows, :])

    def conv_tail(s):
        convolve(s, tiles[1:])
        gains(s, 1)

    def conv_head(s):
        for k in range(3):
            E[s, k, 0:8, :] = jnp.where(sp == 0, 0.0, E[s, k, 0:8, :])
        convolve(s, tiles[:1])

    def convolve(s, some):
        for k in range(3):
            taps = [taps_ref[k, offset : offset + 1, :] for offset in range(CONV)]
            for rows in some:
                start = rows.start + 5
                running = taps[0] * E[s, k, start : start + ROWS, :]
                for offset in range(1, CONV):
                    first = start + offset
                    running = running + taps[offset] * E[s, k, first : first + ROWS, :]
                running = silu(running)
                if k == 0:
                    decayed = DT[s, rows, :] * jnp.exp(-CUM[s, rows, :])
                    XS[s, rows, :] = (running * decayed).astype(BF16)
                elif k == 1:
                    BS[s, rows, :] = running.astype(BF16)
                else:
                    CS[s, rows, :] = running.astype(BF16)

    def gains(s, k):
        rows = slice(k * CHUNK, (k + 1) * CHUNK)
        U[s, k] = matmul(BS[s, rows, :], XS[s, rows, :], ((0,), (0,)))

    def states(s):
        gains(s, 0)
        first, second = CUM[s, CHUNK - 1 : CHUNK, :], CUM[s, SPAN - 1 : SPAN, :]
        final = jnp.exp(second) * (jnp.exp(first) * U[s, 0] + U[s, 1])
        SS[s] = packed(final, first + second)
        share_row(s)

    def inside(s):
        for k in range(2):
            rows = slice(k * CHUNK, (k + 1) * CHUNK)
            scores = matmul(CS[s, rows, :], BS[s, rows, :], ((1,), (1,)))
            scores = jnp.where(lower, scores, 0.0).astype(BF16)
            Y[s, rows, :] = matmul(scores, XS[s, rows, :])

    def scan(s):
        before, before_log = jnp.zeros((LANES, LANES), F32), jnp.zeros((1, LANES), F32)
        total, total_log = before, before_log
        for i in range(4):
            piece = RS[s, i].astype(F32)
            log = piece[LANES : LANES + 1]
            total = jnp.exp(log) * total + piece[0:LANES]
            total_log = total_log + log
            if i < 3:
                before = jnp.where(i + 1 == y, total, before)
                before_log = jnp.where(i + 1 == y, total_log, before_log)
        ROW[s, 0:LANES] = before
        ROW[s, LANES : LANES + 1] = jnp.exp(before_log)
        SR[s] = packed(total, total_log)
        share_up(s)

    def finish(s):
        total = jnp.zeros((LANES, LANES), F32)
        entering = total
        for i in range(3):
            piece = RR[s, i].astype(F32)
            total = jnp.exp(piece[LANES : LANES + 1]) * total + piece[0:LANES]
            entering = jnp.where(i + 1 == z, total, entering)
        entering = ROW[s, LANES : LANES + 1] * entering + ROW[s, 0:LANES]
        for k in range(2):
            rows = slice(k * CHUNK, (k + 1) * CHUNK)
            Y[s, rows, :] += matmul(CS[s, rows, :], entering.astype(BF16))
            if k == 0:
                grown = jnp.exp(CUM[s, CHUNK - 1 : CHUNK, :])
                entering = grown * (entering + U[s, 0])
        for rows in tiles:
            gated = Y[s, rows, :] * jnp.exp(CUM[s, rows, :]) * Z[s, rows, :]
            scale = lax.rsqrt(jnp.mean(gated * gated, axis=-1, keepdims=True) + epsilon)
            GT[s, rows, :] = (gated * scale * og_ref[...]).astype(BF16)

        def send(k, _):
            i = lax.rem(tp + k, 8)
            remote(
                GT.at[s, pl.ds(pl.multiple_of(i * ROWS, ROWS), ROWS), :],
                G.at[s, :, pl.ds(own_columns, LANES)],
                mix_send.at[s],
                mix_recv.at[s],
                tp_device(i),
            ).start()
            return 0

        lax.fori_loop(1, 8, send, 0)
        own(s).start()

    def own(s):
        return pltpu.make_async_copy(
            GT.at[s, pl.ds(pl.multiple_of(tp * ROWS, ROWS), ROWS), :],
            G.at[s, :, pl.ds(own_columns, LANES)],
            local_sem.at[s],
        )

    def mixed_in(s):
        remote(
            G.at[s, :, 0:896], G.at[s, :, 0:896], mix_send.at[s], mix_recv.at[s], partner
        ).wait_recv()
        own(s).wait()

    def multiply(first, last):
        gathered = G[first:last].reshape((last - first) * ROWS, WIDTH)
        result = matmul(gathered, O[...].reshape(WIDTH, WIDTH))
        out_ref[first:last] = result.astype(BF16).reshape(last - first, ROWS, WIDTH)

    token_pair(0, 0, 5)
    project(0)
    token_last(1)
    steps(0)
    conv_tail(0)
    token_near(3)
    oz.near()
    oz.last()
    out_own()
    token_pair(1, 0, 5)
    project(1)
    halo_in(0)
    conv_head(0)
    states(0)
    token_last(2)
    steps(1)
    conv_tail(1)
    token_last(3)
    halo_in(1)
    conv_head(1)
    states(1)
    token_pair(2, 0, 5)
    project(2)
    steps(2)
    conv_tail(2)
    token_pair(3, 0, 5)
    project(3)
    halo_in(2)
    conv_head(2)
    states(2)
    out_near()
    state_in(0)
    scan(0)
    steps(3)
    conv_tail(3)
    halo_in(3)
    conv_head(3)
    states(3)
    state_in(1)
    scan(1)
    gate(0)
    inside(0)
    gate(1)
    inside(1)
    back_in(0)
    finish(0)
    gate(2)
    inside(2)
    state_in(2)
    scan(2)
    gate(3)
    inside(3)
    back_in(1)
    finish(1)
    state_in(3)
    scan(3)
    back_in(2)
    finish(2)
    back_in(3)
    finish(3)
    out_last()
    mixed_in(0)
    mixed_in(1)
    out_pairs()
    mixed_in(2)
    multiply(0, 3)
    mixed_in(3)
    multiply(3, 4)

    for each in (*tokens, wa1, wb1, *wa2, *wb2, oy, oz, ox):
        each.drain()
    for k in range(5):
        out_pair(k, c).wait_send()
    for s in range(SEQS):
        for k in range(5):
            pair_copy(s, k, c).wait_send()
        pl.when(sp < 15)(halo(s).wait_send)
        states_out(s)
        remote(
            G.at[s, :, 0:896], G.at[s, :, 0:896], mix_send.at[s], mix_recv.at[s], partner
        ).wait_send()


def local(
    tokens,
    norm_gain,
    x_weight,
    z_weight,
    b_weight,
    c_weight,
    dt_weight,
    x_conv,
    b_conv,
    c_conv,
    dt_bias,
    decay_rate,
    out_gain,
    out_weight,
):
    hbm = pl.BlockSpec(memory_space=pltpu.HBM)
    dma = pltpu.SemaphoreType.DMA
    return pl.pallas_call(
        kernel,
        out_shape=pltpu.VMEM(tokens.shape, BF16),
        in_specs=[hbm] * 14,
        out_specs=pl.BlockSpec(memory_space=pltpu.VMEM),
        scratch_shapes=[
            pltpu.SMEM((2,), F32),
            pltpu.SMEM((2,), F32),
            pltpu.VMEM((SEQS, ROWS, WIDTH), BF16),
            pltpu.VMEM((1, WIDTH), F32),
            pltpu.VMEM((2, ROWS), BF16),
            pltpu.VMEM((3, CONV, LANES), F32),
            pltpu.VMEM((1, LANES), F32),
            pltpu.VMEM((SEQS, SPAN, WIDTH), BF16),
            pltpu.VMEM((4, 4, ROWS, 256), BF16),
            pltpu.VMEM((4, 4, ROWS, 384), BF16),
            pltpu.VMEM((4, 4, ROWS, LANES), BF16),
            pltpu.VMEM((2, 512, WIDTH), BF16),
            pltpu.VMEM((SEQS, 3, SPAN + 8, LANES), F32),
            pltpu.VMEM((SEQS, SPAN, LANES), F32),
            pltpu.VMEM((SEQS, SPAN, LANES), F32),
            pltpu.VMEM((SEQS, SPAN, LANES), F32),
            pltpu.VMEM((SEQS, SPAN, LANES), BF16),
            pltpu.VMEM((SEQS, SPAN, LANES), BF16),
            pltpu.VMEM((SEQS, SPAN, LANES), BF16),
            pltpu.VMEM((SEQS, SPAN, LANES), F32),
            pltpu.VMEM((SEQS, 2, LANES, LANES), F32),
            pltpu.VMEM((SEQS, LANES + 16, LANES), BF16),
            pltpu.VMEM((SEQS, 4, LANES + 16, LANES), BF16),
            pltpu.VMEM((SEQS, LANES + 16, LANES), BF16),
            pltpu.VMEM((SEQS, 4, LANES + 16, LANES), BF16),
            pltpu.VMEM((SEQS, LANES + 8, LANES), F32),
            pltpu.VMEM((SEQS, SPAN, LANES), BF16),
            pltpu.VMEM((SEQS, ROWS, WIDTH), BF16),
            dma((17, 4)),
            dma((17, 4)),
            dma((SEQS + 1, 5)),
            dma((SEQS + 1, 5)),
            dma((SEQS,)),
            dma((SEQS,)),
            dma((SEQS, 4)),
            dma((SEQS, 4)),
            dma((SEQS, 4)),
            dma((SEQS, 4)),
            dma((SEQS,)),
            dma((SEQS,)),
            dma((SEQS,)),
            dma((17,)),
        ],
        compiler_params=pltpu.CompilerParams(
            collective_id=0, has_side_effects=True, vmem_limit_bytes=60 * 1024 * 1024
        ),
        name="mixer",
    )(
        dt_bias,
        decay_rate,
        tokens,
        norm_gain.reshape(1, -1),
        x_weight,
        z_weight,
        b_weight,
        c_weight,
        dt_weight.T,
        x_conv,
        b_conv,
        c_conv,
        out_gain.reshape(1, -1),
        out_weight.T,
    )


def solution(mesh):
    torus = Mesh(mesh.devices.reshape(4, 4, 4, 2), SP_TP)
    return jax.shard_map(
        local,
        mesh=torus,
        in_specs=(
            P(None, SP_TP, None),
            P(),
            P(SP, TP),
            P(SP, TP),
            P(SP, TP),
            P(SP, TP),
            P(SP, TP),
            P(None, TP),
            P(None, TP),
            P(None, TP),
            P(TP),
            P(TP),
            P(TP),
            P(TP, SP),
        ),
        out_specs=P(None, SP_TP, None),
        check_vma=False,
    )
```

```python
import functools

import jax
import jax.numpy as jnp
from jax import lax
from jax.experimental import pallas as pl
from jax.experimental.pallas import tpu as pltpu
from jax.sharding import Mesh
from jax.sharding import PartitionSpec as P

CONV = 4
SP = ("sp_0", "sp_1")
TP = ("tp_0", "tp_1")
SP_TP = ("sp_0", "sp_1", "tp_0", "tp_1")
LENGTH = 8192
SEQS = 4
SPAN = 512
ROWS = 64
WIDTH = 1024
CHUNK = 256
LANES = 128
epsilon = 1e-05
MESH = pl.DeviceIdType.MESH
F32 = jnp.float32
BF16 = jnp.bfloat16


def remote(src, dst, send, recv, device):
    return pltpu.make_async_remote_copy(
        src_ref=src,
        dst_ref=dst,
        send_sem=send,
        recv_sem=recv,
        device_id=device,
        device_id_type=MESH,
    )


class Ring:
    def __init__(self, place, axis, block, send, recvs, both, direct=False):
        self.block, self.send, self.recvs, self.both = block, send, recvs, both
        self.direct = direct
        self.me = place[axis]
        self.right, self.left = lax.rem(self.me + 1, 4), lax.rem(self.me + 3, 4)
        self.far = lax.rem(self.me + 2, 4)
        to = lambda i: tuple(i if k == axis else p for k, p in enumerate(place))
        self.to_right, self.to_left, self.to_far = to(self.right), to(self.left), to(self.far)

    def copy(self, ref, lane, device):
        return remote(ref, ref, self.send, self.recvs.at[lane], device)

    def own(self):
        self.copy(self.block(self.me, None), 0, self.to_right).start()
        self.copy(self.block(self.me, None), 0, self.to_left).start()
        if self.direct:
            self.copy(self.block(self.me, None), 1, self.to_far).start()

    def near(self):
        self.copy(self.both, 0, self.to_right).wait_recv()
        if not self.direct:
            self.copy(self.block(self.left, 0), 1, self.to_right).start()
            self.copy(self.block(self.right, 1), 1, self.to_left).start()

    def last(self):
        self.copy(self.block(self.far, None), 1, self.to_right).wait_recv()


def half_rows(half):
    return slice(None) if half is None else slice(32 * half, 32 * half + 32)


def half_blocks(half):
    return slice(None) if half is None else slice(2 * half, 2 * half + 2)


def matmul(a, b, dims=((1,), (0,)), precision=None):
    return lax.dot_general(a, b, (dims, ((), ())), precision=precision, preferred_element_type=F32)


def silu(value):
    half = 0.5 * value
    return half + half * jnp.tanh(half)


def kernel(
    bias_in,
    rate_in,
    tokens_in,
    gain_in,
    xw_in,
    zw_in,
    bw_in,
    cw_in,
    dw_in,
    xt_in,
    bt_in,
    ct_in,
    og_in,
    ow_in,
    out_ref,
    bias_ref,
    rate_ref,
    tokens_ref,
    gain_ref,
    dw_ref,
    taps_ref,
    og_ref,
    T,
    WA,
    WB,
    OYZ,
    O,
    E,
    Z,
    DT,
    CUM,
    XS,
    BS,
    CS,
    Y,
    U,
    SS,
    RS,
    SR,
    RR,
    ROW,
    GT,
    G,
    sends,
    ring_recv,
    pair_recv,
    halo_recv,
    state_recv,
    back_recv,
    mix_recv,
    local_sem,
    load_sem,
):
    z, y = lax.axis_index("sp_0"), lax.axis_index("sp_1")
    x, c = lax.axis_index("tp_0"), lax.axis_index("tp_1")
    place = (z, y, x, c)
    sp, tp = z * 4 + y, x * 2 + c
    other = 1 - c
    partner = (z, y, x, other)

    def sp_device(i):
        return (i // 4, lax.rem(i, 4), x, c)

    def tp_device(i):
        return (z, y, i // 2, lax.rem(i, 2))

    barrier = pltpu.get_barrier_semaphore()

    def greet(semaphore, there):
        pl.semaphore_signal(semaphore, inc=1, device_id=there, device_id_type=MESH)

    for step in (1, 3):
        greet(barrier, (z, y, lax.rem(x + step, 4), c))
    greet(barrier, partner)
    for step in (1, 2, 3):
        greet(barrier, (z, lax.rem(y + step, 4), x, c))
        greet(barrier, (lax.rem(z + step, 4), y, x, c))

    group = lambda k, *pairs: [pltpu.make_async_copy(*pair, load_sem.at[k]) for pair in pairs]
    weights_in = group(
        0,
        (xw_in, WA.at[z, y, :, 0:128]),
        (bw_in, WA.at[z, y, :, 128:256]),
        (cw_in, WB.at[z, y, :, 0:128]),
        (zw_in, WB.at[z, y, :, 128:256]),
        (ow_in, OYZ.at[z, y]),
    )
    (dt_in,) = group(1, (dw_in, dw_ref))
    (gain_copy,) = group(2, (gain_in, gain_ref))
    token_copies = [group(3 + s, (tokens_in.at[s], tokens_ref.at[s]))[0] for s in range(SEQS)]
    taps_in = group(
        7, *((ref, taps_ref.at[k]) for k, ref in enumerate((xt_in, bt_in, ct_in)))
    )
    small_in = [
        *group(8, (og_in, og_ref)),
        *group(9, (bias_in, bias_ref)),
        *group(10, (rate_in, rate_ref)),
    ]
    for load in (*weights_in, dt_in, gain_copy, *token_copies, *taps_in, *small_in):
        load.start()

    lane = lax.broadcasted_iota(jnp.int32, (1, LANES), 1)
    low = lane < 64

    head_at = lax.broadcasted_iota(jnp.int32, (2, LANES), 0)
    lane_at = lax.broadcasted_iota(jnp.int32, (2, LANES), 1)
    spread = (lane_at // 64 == head_at).astype(BF16)
    five = T.at[0, 0:80, 0:512]
    pltpu.make_async_copy(five, five, load_sem.at[0]).wait()
    dt_in.wait()
    gain_copy.wait()
    WB[z, y, :, 256:384] = matmul(dw_ref[...], spread, ((0,), (0,))).astype(BF16)

    def normed(s):
        token_copies[s].wait()
        source = tokens_ref[s].astype(F32)
        scale = lax.rsqrt(jnp.mean(source * source, axis=-1, keepdims=True) + epsilon)
        T[s, pl.ds(pl.multiple_of(tp * ROWS, ROWS), ROWS), :] = (
            source * scale * gain_ref[...]
        ).astype(BF16)

    own_columns = pl.multiple_of((c * 4 + x) * LANES, LANES)
    pl.semaphore_wait(barrier, 9)

    def token_block(s):
        def block(i, half):
            start = (i * 2 + c) * ROWS + (0 if half is None else 32 * half)
            rows = ROWS if half is None else 32
            return T.at[s, pl.ds(pl.multiple_of(start, 32), rows), :]

        return block

    def ring(axis, block, number, rows, direct=False):
        group = 0 if number < SEQS else 1 if number < 16 else 2
        both = T.at[0, 0:rows, :]
        send = sends.at[group]
        return Ring(place, axis, block, send, ring_recv.at[number], both, direct)

    tokens = [ring(2, token_block(s), s, 2 * ROWS) for s in range(SEQS)]
    wa1 = ring(1, lambda i, h: WA.at[z, i, half_rows(h)], 4, 32, True)
    wb1 = ring(0, lambda i, h: WB.at[i, y, half_rows(h)], 5, 48, True)
    shifted = lambda i, k: lax.rem(i + k, 4)
    wa2 = [ring(0, lambda i, h, k=k: WA.at[i, shifted(y, k), half_rows(h)], 6 + k, 32) for k in range(4)]
    wb2 = [ring(1, lambda i, h, k=k: WB.at[shifted(z, k), i, half_rows(h)], 10 + k, 48) for k in range(4)]
    oy = ring(1, lambda i, h: OYZ.at[z, i], 14, 16, True)
    oz = ring(0, lambda i, h: OYZ.at[i], 15, ROWS, True)

    def out_rows(core, i, half):
        rows = LANES if half is None else 64
        start = i * LANES + (0 if half is None else 64 * half)
        return O.at[core, pl.ds(pl.multiple_of(start, 64), rows), :]

    ox = ring(2, lambda i, h: out_rows(c, i, h), 16, 256)

    def pair_copy(s, k, core):
        i, half = (
            (x, None),
            (tokens[s].left, None),
            (tokens[s].right, None),
            (tokens[s].far, 0),
            (tokens[s].far, 1),
        )[k]
        start = (i * 2 + core) * ROWS + (0 if half is None else 32 * half)
        rows = ROWS if half is None else 32
        ref = T.at[s, pl.ds(pl.multiple_of(start, 32), rows), :]
        return remote(ref, ref, sends.at[0], pair_recv.at[s], partner)

    def out_pair(k, core):
        i, half = ((x, None), (ox.left, None), (ox.right, None), (ox.far, 0), (ox.far, 1))[k]
        ref = out_rows(core, i, half)
        return remote(ref, ref, sends.at[2], pair_recv.at[SEQS], partner)

    def out_own():
        block = OYZ[...].reshape(WIDTH, LANES).astype(F32).T.astype(BF16)
        O[c, pl.ds(pl.multiple_of(x * LANES, LANES), LANES), :] = block
        ox.own()
        out_pair(0, c).start()

    def out_near():
        ox.near()
        out_pair(1, c).start()
        out_pair(2, c).start()

    def out_last():
        ox.last()
        out_pair(3, c).start()
        out_pair(4, c).start()

    def out_pairs():
        remote(T.at[0], T.at[0], sends.at[2], pair_recv.at[SEQS], partner).wait_recv()

    def token_own(s):
        tokens[s].own()
        pair_copy(s, 0, c).start()

    def token_near(s):
        tokens[s].near()
        pair_copy(s, 1, c).start()
        pair_copy(s, 2, c).start()

    def token_last(s):
        tokens[s].last()
        pair_copy(s, 3, c).start()
        pair_copy(s, 4, c).start()

    wa1.own()
    wb1.own()
    wa2[0].own()
    wb2[0].own()
    normed(0)
    token_own(0)
    normed(1)
    token_own(1)
    normed(2)
    normed(3)
    wa1.near()
    wa2[1].own()
    wa2[3].own()
    wb1.near()
    wb2[1].own()
    wb2[3].own()
    wa1.last()
    wa2[2].own()
    wb1.last()
    wb2[2].own()
    oy.own()
    wa2[0].near()
    wb2[0].near()
    token_near(0)
    token_own(2)
    wa2[1].near()
    wa2[3].near()
    wb2[1].near()
    wb2[3].near()
    token_near(1)
    token_own(3)
    wa2[2].near()
    wb2[2].near()
    oy.near()
    oy.last()
    oz.own()
    token_last(0)
    wa2[0].last()
    wa2[1].last()
    wa2[3].last()
    wb2[0].last()
    wb2[1].last()
    wb2[3].last()
    token_near(2)
    wa2[2].last()
    wb2[2].last()

    pltpu.make_async_copy(taps_ref, taps_ref, load_sem.at[7]).wait()
    for load in small_in:
        load.wait()
    bias = jnp.where(low, bias_ref[0], bias_ref[1])
    rate = jnp.where(low, rate_ref[0], rate_ref[1])
    row_at = lax.broadcasted_iota(jnp.int32, (CHUNK, CHUNK), 0)
    column_at = lax.broadcasted_iota(jnp.int32, (CHUNK, CHUNK), 1)
    lower = row_at >= column_at
    ones_below = lower.astype(BF16)
    tiles = [slice(k * ROWS, (k + 1) * ROWS) for k in range(SPAN // ROWS)]
    following = sp_device(lax.rem(sp + 1, 16))

    def packed(state, log):
        log = jnp.broadcast_to(log, (16, LANES))
        return jnp.concatenate([state, log], axis=0).astype(BF16)

    def share_row(s):
        for k in (1, 3, 2):
            there = (z, lax.rem(y + k, 4), x, c)
            copy = remote(SS.at[s], RS.at[s, y], sends.at[4], state_recv.at[s], there)
            pl.when((y + k < 4) | (z < 3))(copy.start)
        RS[s, y] = SS[s]

    def share_up(s):
        for k in (1, 2, 3):
            there = (lax.rem(z + k, 4), y, x, c)
            copy = remote(SR.at[s], RR.at[s, z], sends.at[5], back_recv.at[s], there)
            pl.when(z + k < 4)(copy.start)

    def states_out():
        for n in (1, 2, 3):
            ref = RS.at[:, 0:n]
            copy = remote(ref, ref, sends.at[4], state_recv.at[0], partner)
            pl.when(jnp.where(z < 3, 3, 3 - y) == n)(copy.wait_send)
            copy = remote(ref, ref, sends.at[5], back_recv.at[0], partner)
            pl.when(3 - z == n)(copy.wait_send)

    def halo(s):
        return remote(
            E.at[s, :, SPAN : SPAN + 8, :],
            E.at[s, :, 0:8, :],
            sends.at[3],
            halo_recv.at[s],
            following,
        )

    def token_pair(s):
        half = T.at[s, 0:256, :]
        remote(half, half, sends.at[0], pair_recv.at[s], partner).wait_recv()

    def halo_in(s):
        pl.when(sp > 0)(halo(s).wait_recv)

    def state_in(s):
        for n in (1, 2, 3):
            ref = RS.at[s, 0:n]
            copy = remote(ref, ref, sends.at[4], state_recv.at[s], partner)
            pl.when(jnp.where(z < 3, 3, y) == n)(copy.wait_recv)

    def back_in(s):
        for n in (1, 2, 3):
            ref = RR.at[s, 0:n]
            copy = remote(ref, ref, sends.at[5], back_recv.at[s], partner)
            pl.when(z == n)(copy.wait_recv)

    def project(s):
        product = matmul(T[s], WA[...].reshape(WIDTH, 256))
        E[s, 0, 8 : SPAN + 8, :] = product[:, 0:128]
        E[s, 1, 8 : SPAN + 8, :] = product[:, 128:256]
        product = matmul(T[s], WB[...].reshape(WIDTH, 384))
        E[s, 2, 8 : SPAN + 8, :] = product[:, 0:128]
        Z[s] = product[:, 128:256]
        DT[s] = product[:, 256:384]
        pl.when(sp < 15)(halo(s).start)

    def gate(s):
        for rows in tiles:
            Z[s, rows, :] = silu(Z[s, rows, :])

    def steps(s):
        for rows in tiles:
            step = DT[s, rows, :] + bias
            step = jnp.maximum(step, 0.0) + jnp.log1p(jnp.exp(-jnp.abs(step)))
            DT[s, rows, :] = step
            XS[s, rows, :] = (-(step * rate) / LENGTH).astype(BF16)
        for k in range(2):
            rows = slice(k * CHUNK, (k + 1) * CHUNK)
            CUM[s, rows, :] = matmul(ones_below, XS[s, rows, :])

    def conv_tail(s):
        convolve(s, tiles[1:])
        gains(s, 1)

    def conv_head(s):
        for k in range(3):
            E[s, k, 0:8, :] = jnp.where(sp == 0, 0.0, E[s, k, 0:8, :])
        convolve(s, tiles[:1])

    def convolve(s, some):
        for k in range(3):
            taps = [taps_ref[k, offset : offset + 1, :] for offset in range(CONV)]
            for rows in some:
                start = rows.start + 5
                running = taps[0] * E[s, k, start : start + ROWS, :]
                for offset in range(1, CONV):
                    first = start + offset
                    running = running + taps[offset] * E[s, k, first : first + ROWS, :]
                running = silu(running)
                if k == 0:
                    decayed = DT[s, rows, :] * jnp.exp(-CUM[s, rows, :])
                    XS[s, rows, :] = (running * decayed).astype(BF16)
                elif k == 1:
                    BS[s, rows, :] = running.astype(BF16)
                else:
                    CS[s, rows, :] = running.astype(BF16)

    def gains(s, k):
        rows = slice(k * CHUNK, (k + 1) * CHUNK)
        U[s, k] = matmul(BS[s, rows, :], XS[s, rows, :], ((0,), (0,)))

    def states(s):
        gains(s, 0)
        first, second = CUM[s, CHUNK - 1 : CHUNK, :], CUM[s, SPAN - 1 : SPAN, :]
        final = jnp.exp(second) * (jnp.exp(first) * U[s, 0] + U[s, 1])
        SS[s] = packed(final, first + second)
        share_row(s)

    def inside(s):
        for k in range(2):
            rows = slice(k * CHUNK, (k + 1) * CHUNK)
            scores = matmul(CS[s, rows, :], BS[s, rows, :], ((1,), (1,)))
            scores = jnp.where(lower, scores, 0.0).astype(BF16)
            Y[s, rows, :] = matmul(scores, XS[s, rows, :])

    def scan(s):
        before, before_log = jnp.zeros((LANES, LANES), F32), jnp.zeros((1, LANES), F32)
        total, total_log = before, before_log
        for i in range(4):
            piece = RS[s, i].astype(F32)
            log = piece[LANES : LANES + 1]
            total = jnp.exp(log) * total + piece[0:LANES]
            total_log = total_log + log
            if i < 3:
                before = jnp.where(i + 1 == y, total, before)
                before_log = jnp.where(i + 1 == y, total_log, before_log)
        ROW[s, 0:LANES] = before
        ROW[s, LANES : LANES + 1] = jnp.exp(before_log)
        SR[s] = packed(total, total_log)
        share_up(s)

    def finish(s):
        total = jnp.zeros((LANES, LANES), F32)
        entering = total
        for i in range(3):
            piece = RR[s, i].astype(F32)
            total = jnp.exp(piece[LANES : LANES + 1]) * total + piece[0:LANES]
            entering = jnp.where(i + 1 == z, total, entering)
        entering = ROW[s, LANES : LANES + 1] * entering + ROW[s, 0:LANES]
        for k in range(2):
            rows = slice(k * CHUNK, (k + 1) * CHUNK)
            Y[s, rows, :] += matmul(CS[s, rows, :], entering.astype(BF16))
            if k == 0:
                grown = jnp.exp(CUM[s, CHUNK - 1 : CHUNK, :])
                entering = grown * (entering + U[s, 0])
        for i in range(8):
            rows = tiles[i]
            gated = Y[s, rows, :] * jnp.exp(CUM[s, rows, :]) * Z[s, rows, :]
            scale = lax.rsqrt(jnp.mean(gated * gated, axis=-1, keepdims=True) + epsilon)
            GT[s, rows, :] = (gated * scale * og_ref[...]).astype(BF16)
            if i % 4 == 3:
                for j in range(i - 3, i + 1):
                    pl.when(tp != j)(mix_copy(s, j).start)
        own(s).start()

    def mix_copy(s, i):
        return remote(
            GT.at[s, i * ROWS : (i + 1) * ROWS, :],
            G.at[s, :, pl.ds(own_columns, LANES)],
            sends.at[6],
            mix_recv.at[s],
            (z, y, i // 2, i % 2),
        )

    def own(s):
        return pltpu.make_async_copy(
            GT.at[s, pl.ds(pl.multiple_of(tp * ROWS, ROWS), ROWS), :],
            G.at[s, :, pl.ds(own_columns, LANES)],
            local_sem.at[s],
        )

    def mixed_in(s):
        remote(
            G.at[s, :, 0:896], G.at[s, :, 0:896], sends.at[6], mix_recv.at[s], partner
        ).wait_recv()
        own(s).wait()

    def multiply(first, last):
        gathered = G[first:last].reshape((last - first) * ROWS, WIDTH)
        result = matmul(gathered, O[...].reshape(WIDTH, WIDTH))
        out_ref[first:last] = result.astype(BF16).reshape(last - first, ROWS, WIDTH)

    def sent(ref, group):
        return remote(ref, ref, sends.at[group], pair_recv.at[0], partner)

    def drain():
        sent(T.at[:, 0:448, :], 0).wait_send()
        sent(T.at[0:3, 0:240, :], 1).wait_send()
        pl.when(sp < 15)(sent(E.at[:, :, 0:8, :], 3).wait_send)
        states_out()

    def ox_drain():
        sent(T.at[0:2, 0:448, :], 2).wait_send()

    def out_drain():
        sent(G.at[:, :, 0:896], 6).wait_send()

    token_pair(0)
    project(0)
    token_last(1)
    steps(0)
    conv_tail(0)
    token_near(3)
    oz.near()
    oz.last()
    out_own()
    token_pair(1)
    project(1)
    token_last(2)
    halo_in(0)
    conv_head(0)
    states(0)
    steps(1)
    conv_tail(1)
    halo_in(1)
    conv_head(1)
    states(1)
    token_last(3)
    token_pair(2)
    project(2)
    steps(2)
    conv_tail(2)
    token_pair(3)
    project(3)
    halo_in(2)
    conv_head(2)
    states(2)
    out_near()
    state_in(0)
    scan(0)
    steps(3)
    conv_tail(3)
    halo_in(3)
    conv_head(3)
    states(3)
    state_in(1)
    scan(1)
    gate(0)
    inside(0)
    gate(1)
    inside(1)
    back_in(0)
    finish(0)
    gate(2)
    inside(2)
    state_in(2)
    scan(2)
    gate(3)
    inside(3)
    back_in(1)
    finish(1)
    state_in(3)
    scan(3)
    back_in(2)
    finish(2)
    back_in(3)
    finish(3)
    out_last()
    drain()
    mixed_in(0)
    mixed_in(1)
    out_pairs()
    ox_drain()
    multiply(0, 2)
    mixed_in(2)
    mixed_in(3)
    multiply(2, 4)

    out_drain()


def local(
    tokens,
    norm_gain,
    x_weight,
    z_weight,
    b_weight,
    c_weight,
    dt_weight,
    x_conv,
    b_conv,
    c_conv,
    dt_bias,
    decay_rate,
    out_gain,
    out_weight,
):
    hbm = pl.BlockSpec(memory_space=pltpu.HBM)
    dma = pltpu.SemaphoreType.DMA
    return pl.pallas_call(
        kernel,
        out_shape=pltpu.VMEM(tokens.shape, BF16),
        in_specs=[hbm] * 14,
        out_specs=pl.BlockSpec(memory_space=pltpu.VMEM),
        scratch_shapes=[
            pltpu.SMEM((2,), F32),
            pltpu.SMEM((2,), F32),
            pltpu.VMEM((SEQS, ROWS, WIDTH), BF16),
            pltpu.VMEM((1, WIDTH), F32),
            pltpu.VMEM((2, ROWS), BF16),
            pltpu.VMEM((3, CONV, LANES), F32),
            pltpu.VMEM((1, LANES), F32),
            pltpu.VMEM((SEQS, SPAN, WIDTH), BF16),
            pltpu.VMEM((4, 4, ROWS, 256), BF16),
            pltpu.VMEM((4, 4, ROWS, 384), BF16),
            pltpu.VMEM((4, 4, ROWS, LANES), BF16),
            pltpu.VMEM((2, 512, WIDTH), BF16),
            pltpu.VMEM((SEQS, 3, SPAN + 8, LANES), F32),
            pltpu.VMEM((SEQS, SPAN, LANES), F32),
            pltpu.VMEM((SEQS, SPAN, LANES), F32),
            pltpu.VMEM((SEQS, SPAN, LANES), F32),
            pltpu.VMEM((SEQS, SPAN, LANES), BF16),
            pltpu.VMEM((SEQS, SPAN, LANES), BF16),
            pltpu.VMEM((SEQS, SPAN, LANES), BF16),
            pltpu.VMEM((SEQS, SPAN, LANES), F32),
            pltpu.VMEM((SEQS, 2, LANES, LANES), F32),
            pltpu.VMEM((SEQS, LANES + 16, LANES), BF16),
            pltpu.VMEM((SEQS, 4, LANES + 16, LANES), BF16),
            pltpu.VMEM((SEQS, LANES + 16, LANES), BF16),
            pltpu.VMEM((SEQS, 4, LANES + 16, LANES), BF16),
            pltpu.VMEM((SEQS, LANES + 8, LANES), F32),
            pltpu.VMEM((SEQS, SPAN, LANES), BF16),
            pltpu.VMEM((SEQS, ROWS, WIDTH), BF16),
            dma((7,)),
            dma((17, 2)),
            dma((SEQS + 1,)),
            dma((SEQS,)),
            dma((SEQS,)),
            dma((SEQS,)),
            dma((SEQS,)),
            dma((SEQS,)),
            dma((11,)),
        ],
        compiler_params=pltpu.CompilerParams(
            collective_id=0, has_side_effects=True, vmem_limit_bytes=60 * 1024 * 1024
        ),
        name="mixer",
    )(
        dt_bias,
        decay_rate,
        tokens,
        norm_gain.reshape(1, -1),
        x_weight,
        z_weight,
        b_weight,
        c_weight,
        dt_weight.T,
        x_conv,
        b_conv,
        c_conv,
        out_gain.reshape(1, -1),
        out_weight.T,
    )


def solution(mesh):
    torus = Mesh(mesh.devices.reshape(4, 4, 4, 2), SP_TP)
    return jax.shard_map(
        local,
        mesh=torus,
        in_specs=(
            P(None, SP_TP, None),
            P(),
            P(SP, TP),
            P(SP, TP),
            P(SP, TP),
            P(SP, TP),
            P(SP, TP),
            P(None, TP),
            P(None, TP),
            P(None, TP),
            P(TP),
            P(TP),
            P(TP),
            P(TP, SP),
        ),
        out_specs=P(None, SP_TP, None),
        check_vma=False,
    )
```

```python
import functools

import jax
import jax.numpy as jnp
from jax import lax
from jax.experimental import pallas as pl
from jax.experimental.pallas import tpu as pltpu
from jax.sharding import Mesh
from jax.sharding import PartitionSpec as P

CONV = 4
SP = ("sp_0", "sp_1")
TP = ("tp_0", "tp_1")
SP_TP = ("sp_0", "sp_1", "tp_0", "tp_1")
LENGTH = 8192
SEQS = 4
SPAN = 512
ROWS = 64
WIDTH = 1024
CHUNK = 256
LANES = 128
epsilon = 1e-05
MESH = pl.DeviceIdType.MESH
F32 = jnp.float32
BF16 = jnp.bfloat16


def remote(src, dst, send, recv, device):
    return pltpu.make_async_remote_copy(
        src_ref=src,
        dst_ref=dst,
        send_sem=send,
        recv_sem=recv,
        device_id=device,
        device_id_type=MESH,
    )


class Ring:
    def __init__(self, place, axis, block, send, recvs, both, direct=False):
        self.block, self.send, self.recvs, self.both = block, send, recvs, both
        self.direct = direct
        self.me = place[axis]
        self.right, self.left = lax.rem(self.me + 1, 4), lax.rem(self.me + 3, 4)
        self.far = lax.rem(self.me + 2, 4)
        to = lambda i: tuple(i if k == axis else p for k, p in enumerate(place))
        self.to_right, self.to_left, self.to_far = to(self.right), to(self.left), to(self.far)

    def copy(self, ref, lane, device):
        return remote(ref, ref, self.send, self.recvs[lane], device)

    def own(self):
        self.copy(self.block(self.me, None), 0, self.to_right).start()
        self.copy(self.block(self.me, None), 0, self.to_left).start()
        if self.direct:
            self.copy(self.block(self.me, None), 1, self.to_far).start()

    def near(self):
        self.copy(self.both, 0, self.to_right).wait_recv()
        if not self.direct:
            self.copy(self.block(self.left, 0), 1, self.to_right).start()
            self.copy(self.block(self.right, 1), 1, self.to_left).start()

    def last(self):
        self.copy(self.block(self.far, None), 1, self.to_right).wait_recv()


def half_rows(half):
    return slice(None) if half is None else slice(32 * half, 32 * half + 32)


def half_blocks(half):
    return slice(None) if half is None else slice(2 * half, 2 * half + 2)


def matmul(a, b, dims=((1,), (0,)), precision=None):
    return lax.dot_general(a, b, (dims, ((), ())), precision=precision, preferred_element_type=F32)


def silu(value):
    half = 0.5 * value
    return half + half * jnp.tanh(half)


def kernel(
    bias_in,
    rate_in,
    tokens_in,
    gain_in,
    xw_in,
    zw_in,
    bw_in,
    cw_in,
    dw_in,
    xt_in,
    bt_in,
    ct_in,
    og_in,
    ow_in,
    out_ref,
    bias_ref,
    rate_ref,
    tokens_ref,
    gain_ref,
    dw_ref,
    taps_ref,
    og_ref,
    T,
    WA,
    WB,
    OYZ,
    O,
    E,
    Z,
    DT,
    CUM,
    XS,
    BS,
    CS,
    Y,
    U,
    SS,
    RS,
    SR,
    RR,
    ROW,
    GT,
    G,
    sends,
    ring_recv,
    pair_recv,
    halo_recv,
    state_recv,
    back_recv,
    mix_recv,
    local_sem,
    load_sem,
):
    z, y = lax.axis_index("sp_0"), lax.axis_index("sp_1")
    x, c = lax.axis_index("tp_0"), lax.axis_index("tp_1")
    place = (z, y, x, c)
    sp, tp = z * 4 + y, x * 2 + c
    other = 1 - c
    partner = (z, y, x, other)

    def sp_device(i):
        return (i // 4, lax.rem(i, 4), x, c)

    def tp_device(i):
        return (z, y, i // 2, lax.rem(i, 2))

    barrier = pltpu.get_barrier_semaphore()

    def greet(semaphore, there):
        pl.semaphore_signal(semaphore, inc=1, device_id=there, device_id_type=MESH)

    for step in (1, 3):
        greet(barrier, (z, y, lax.rem(x + step, 4), c))
    greet(barrier, partner)
    for step in (1, 2, 3):
        greet(barrier, (z, lax.rem(y + step, 4), x, c))
        greet(barrier, (lax.rem(z + step, 4), y, x, c))

    group = lambda k, *pairs: [pltpu.make_async_copy(*pair, load_sem.at[k]) for pair in pairs]
    weights_in = group(
        0,
        (xw_in, WA.at[z, y, :, 0:128]),
        (bw_in, WA.at[z, y, :, 128:256]),
        (cw_in, WB.at[z, y, :, 0:128]),
        (zw_in, WB.at[z, y, :, 128:256]),
        (ow_in, OYZ.at[z, y]),
    )
    (dt_in,) = group(1, (dw_in, dw_ref))
    (gain_copy,) = group(2, (gain_in, gain_ref))
    token_copies = [group(3 + s, (tokens_in.at[s], tokens_ref.at[s]))[0] for s in range(SEQS)]
    taps_in = group(
        7, *((ref, taps_ref.at[k]) for k, ref in enumerate((xt_in, bt_in, ct_in)))
    )
    small_in = [
        *group(8, (og_in, og_ref)),
        *group(9, (bias_in, bias_ref)),
        *group(10, (rate_in, rate_ref)),
    ]
    for load in (*weights_in, dt_in, gain_copy, *token_copies, *taps_in, *small_in):
        load.start()

    lane = lax.broadcasted_iota(jnp.int32, (1, LANES), 1)
    low = lane < 64

    head_at = lax.broadcasted_iota(jnp.int32, (2, LANES), 0)
    lane_at = lax.broadcasted_iota(jnp.int32, (2, LANES), 1)
    spread = (lane_at // 64 == head_at).astype(BF16)
    five = T.at[0, 0:80, 0:512]
    pltpu.make_async_copy(five, five, load_sem.at[0]).wait()
    dt_in.wait()
    gain_copy.wait()
    WB[z, y, :, 256:384] = matmul(dw_ref[...], spread, ((0,), (0,))).astype(BF16)

    def normed(s):
        token_copies[s].wait()
        source = tokens_ref[s].astype(F32)
        scale = lax.rsqrt(jnp.mean(source * source, axis=-1, keepdims=True) + epsilon)
        T[s, pl.ds(pl.multiple_of(tp * ROWS, ROWS), ROWS), :] = (
            source * scale * gain_ref[...]
        ).astype(BF16)

    own_columns = pl.multiple_of((c * 4 + x) * LANES, LANES)
    normed(0)
    pl.semaphore_wait(barrier, 9)

    def token_block(s):
        def block(i, half):
            start = (i * 2 + c) * ROWS + (0 if half is None else 32 * half)
            rows = ROWS if half is None else 32
            return T.at[s, pl.ds(pl.multiple_of(start, 32), rows), :]

        return block

    def ring(axis, block, number, rows, direct=False):
        group = 0 if number < SEQS else 1 if number < 16 else 2
        both = T.at[0, 0:rows, :]
        send = sends.at[group]
        last = number if number < 6 else max(6, number - 7)
        recvs = (ring_recv.at[number], ring_recv.at[17 + last])
        return Ring(place, axis, block, send, recvs, both, direct)

    tokens = [ring(2, token_block(s), s, 2 * ROWS) for s in range(SEQS)]
    wa1 = ring(1, lambda i, h: WA.at[z, i, half_rows(h)], 4, 32, True)
    wb1 = ring(0, lambda i, h: WB.at[i, y, half_rows(h)], 5, 48, True)
    shifted = lambda i, k: lax.rem(i + k, 4)
    wa2 = [ring(0, lambda i, h, k=k: WA.at[i, shifted(y, k), half_rows(h)], 6 + k, 32, k in (2,)) for k in range(4)]
    wb2 = [ring(1, lambda i, h, k=k: WB.at[shifted(z, k), i, half_rows(h)], 10 + k, 48, k in (2,)) for k in range(4)]
    oy = ring(1, lambda i, h: OYZ.at[z, i], 14, 16, True)
    oz = ring(0, lambda i, h: OYZ.at[i], 15, ROWS, True)

    def out_rows(core, i, half):
        rows = LANES if half is None else 64
        start = i * LANES + (0 if half is None else 64 * half)
        return O.at[core, pl.ds(pl.multiple_of(start, 64), rows), :]

    ox = ring(2, lambda i, h: out_rows(c, i, h), 16, 256)

    def pair_copy(s, k, core):
        i, half = (
            (x, None),
            (tokens[s].left, None),
            (tokens[s].right, None),
            (tokens[s].far, 0),
            (tokens[s].far, 1),
        )[k]
        start = (i * 2 + core) * ROWS + (0 if half is None else 32 * half)
        rows = ROWS if half is None else 32
        ref = T.at[s, pl.ds(pl.multiple_of(start, 32), rows), :]
        return remote(ref, ref, sends.at[0], pair_recv.at[s], partner)

    def out_pair(k, core):
        i, half = ((x, None), (ox.left, None), (ox.right, None), (ox.far, 0), (ox.far, 1))[k]
        ref = out_rows(core, i, half)
        return remote(ref, ref, sends.at[2], pair_recv.at[SEQS], partner)

    def out_own():
        block = OYZ[...].reshape(WIDTH, LANES).astype(F32).T.astype(BF16)
        O[c, pl.ds(pl.multiple_of(x * LANES, LANES), LANES), :] = block
        ox.own()
        out_pair(0, c).start()

    def out_near():
        ox.near()
        out_pair(1, c).start()
        out_pair(2, c).start()

    def out_last():
        ox.last()
        out_pair(3, c).start()
        out_pair(4, c).start()

    def out_pairs():
        remote(T.at[0], T.at[0], sends.at[2], pair_recv.at[SEQS], partner).wait_recv()

    def token_own(s):
        tokens[s].own()
        pair_copy(s, 0, c).start()

    def token_near(s):
        tokens[s].near()
        pair_copy(s, 1, c).start()
        pair_copy(s, 2, c).start()

    def token_last(s):
        tokens[s].last()
        pair_copy(s, 3, c).start()
        pair_copy(s, 4, c).start()

    wa1.own()
    wb1.own()
    wa2[0].own()
    wb2[0].own()
    token_own(0)
    normed(1)
    token_own(1)
    normed(2)
    normed(3)
    wa1.near()
    wa2[1].own()
    wa2[3].own()
    wb1.near()
    wb2[1].own()
    wb2[3].own()
    wa1.last()
    wa2[2].own()
    wb1.last()
    wb2[2].own()
    oy.own()
    wa2[0].near()
    wb2[0].near()
    token_near(0)
    token_own(2)
    wa2[1].near()
    wa2[3].near()
    wb2[1].near()
    wb2[3].near()
    token_near(1)
    token_own(3)
    wa2[2].near()
    wb2[2].near()
    oy.near()
    oy.last()
    oz.own()
    token_last(0)
    token_near(2)
    weights = T.at[0, 0:160, :]
    remote(weights, weights, sends.at[1], ring_recv.at[23], partner).wait_recv()

    pltpu.make_async_copy(taps_ref, taps_ref, load_sem.at[7]).wait()
    for load in small_in:
        load.wait()
    bias = jnp.where(low, bias_ref[0], bias_ref[1])
    rate = jnp.where(low, rate_ref[0], rate_ref[1])
    row_at = lax.broadcasted_iota(jnp.int32, (CHUNK, CHUNK), 0)
    column_at = lax.broadcasted_iota(jnp.int32, (CHUNK, CHUNK), 1)
    lower = row_at >= column_at
    ones_below = lower.astype(BF16)
    tiles = [slice(k * ROWS, (k + 1) * ROWS) for k in range(SPAN // ROWS)]
    following = sp_device(lax.rem(sp + 1, 16))

    def packed(state, log):
        log = jnp.broadcast_to(log, (16, LANES))
        return jnp.concatenate([state, log], axis=0).astype(BF16)

    def share_row(s):
        for k in (1, 3, 2):
            there = (z, lax.rem(y + k, 4), x, c)
            copy = remote(SS.at[s], RS.at[s, y], sends.at[4], state_recv.at[s], there)
            pl.when((y + k < 4) | (z < 3))(copy.start)
        RS[s, y] = SS[s]

    def share_up(s):
        for k in (1, 2, 3):
            there = (lax.rem(z + k, 4), y, x, c)
            copy = remote(SR.at[s], RR.at[s, z], sends.at[5], back_recv.at[s], there)
            pl.when(z + k < 4)(copy.start)

    def states_out():
        for n in (1, 2, 3):
            ref = RS.at[:, 0:n]
            copy = remote(ref, ref, sends.at[4], state_recv.at[0], partner)
            pl.when(jnp.where(z < 3, 3, 3 - y) == n)(copy.wait_send)
            copy = remote(ref, ref, sends.at[5], back_recv.at[0], partner)
            pl.when(3 - z == n)(copy.wait_send)

    def halo(s):
        return remote(
            E.at[s, :, SPAN : SPAN + 8, :],
            E.at[s, :, 0:8, :],
            sends.at[3],
            halo_recv.at[s],
            following,
        )

    def token_pair(s):
        half = T.at[s, 0:256, :]
        remote(half, half, sends.at[0], pair_recv.at[s], partner).wait_recv()

    def halo_in(s):
        pl.when(sp > 0)(halo(s).wait_recv)

    def state_in(s):
        for n in (1, 2, 3):
            ref = RS.at[s, 0:n]
            copy = remote(ref, ref, sends.at[4], state_recv.at[s], partner)
            pl.when(jnp.where(z < 3, 3, y) == n)(copy.wait_recv)

    def back_in(s):
        for n in (1, 2, 3):
            ref = RR.at[s, 0:n]
            copy = remote(ref, ref, sends.at[5], back_recv.at[s], partner)
            pl.when(z == n)(copy.wait_recv)

    def project(s):
        product = matmul(T[s], WA[...].reshape(WIDTH, 256))
        E[s, 0, 8 : SPAN + 8, :] = product[:, 0:128]
        E[s, 1, 8 : SPAN + 8, :] = product[:, 128:256]
        product = matmul(T[s], WB[...].reshape(WIDTH, 384))
        E[s, 2, 8 : SPAN + 8, :] = product[:, 0:128]
        Z[s] = product[:, 128:256]
        DT[s] = product[:, 256:384]
        pl.when(sp < 15)(halo(s).start)

    def gate(s):
        for rows in tiles:
            Z[s, rows, :] = silu(Z[s, rows, :]) * jnp.exp(CUM[s, rows, :])

    def steps(s):
        for rows in tiles:
            step = DT[s, rows, :] + bias
            step = jnp.maximum(step, 0.0) + jnp.log1p(jnp.exp(-jnp.abs(step)))
            DT[s, rows, :] = step
            XS[s, rows, :] = (-(step * rate) / LENGTH).astype(BF16)
        for k in range(2):
            rows = slice(k * CHUNK, (k + 1) * CHUNK)
            CUM[s, rows, :] = matmul(ones_below, XS[s, rows, :])

    def conv_tail(s):
        convolve(s, tiles[1:])
        gains(s, 1)

    def conv_head(s):
        for k in range(3):
            E[s, k, 0:8, :] = jnp.where(sp == 0, 0.0, E[s, k, 0:8, :])
        convolve(s, tiles[:1])

    def convolve(s, some):
        for k in range(3):
            taps = [taps_ref[k, offset : offset + 1, :] for offset in range(CONV)]
            for rows in some:
                start = rows.start + 5
                running = taps[0] * E[s, k, start : start + ROWS, :]
                for offset in range(1, CONV):
                    first = start + offset
                    running = running + taps[offset] * E[s, k, first : first + ROWS, :]
                running = silu(running)
                if k == 0:
                    decayed = DT[s, rows, :] * jnp.exp(-CUM[s, rows, :])
                    XS[s, rows, :] = (running * decayed).astype(BF16)
                elif k == 1:
                    BS[s, rows, :] = running.astype(BF16)
                else:
                    CS[s, rows, :] = running.astype(BF16)

    def gains(s, k):
        rows = slice(k * CHUNK, (k + 1) * CHUNK)
        U[s, k] = matmul(BS[s, rows, :], XS[s, rows, :], ((0,), (0,)))

    def states(s):
        gains(s, 0)
        first, second = CUM[s, CHUNK - 1 : CHUNK, :], CUM[s, SPAN - 1 : SPAN, :]
        final = jnp.exp(second) * (jnp.exp(first) * U[s, 0] + U[s, 1])
        SS[s] = packed(final, first + second)
        share_row(s)

    def inside(s):
        for k in range(2):
            rows = slice(k * CHUNK, (k + 1) * CHUNK)
            scores = matmul(CS[s, rows, :], BS[s, rows, :], ((1,), (1,)))
            scores = jnp.where(lower, scores, 0.0).astype(BF16)
            part = matmul(scores, XS[s, rows, :])
            if k:
                grown = jnp.exp(CUM[s, CHUNK - 1 : CHUNK, :])
                part = part + grown * matmul(CS[s, rows, :], U[s, 0].astype(BF16))
            Y[s, rows, :] = part

    def scan(s):
        before, before_log = jnp.zeros((LANES, LANES), F32), jnp.zeros((1, LANES), F32)
        total, total_log = before, before_log
        for i in range(4):
            piece = RS[s, i].astype(F32)
            log = piece[LANES : LANES + 1]
            total = jnp.exp(log) * total + piece[0:LANES]
            total_log = total_log + log
            if i < 3:
                before = jnp.where(i + 1 == y, total, before)
                before_log = jnp.where(i + 1 == y, total_log, before_log)
        ROW[s, 0:LANES] = before
        ROW[s, LANES : LANES + 1] = jnp.exp(before_log)
        SR[s] = packed(total, total_log)
        share_up(s)

    def finish(s):
        total = jnp.zeros((LANES, LANES), F32)
        entering = total
        for i in range(3):
            piece = RR[s, i].astype(F32)
            total = jnp.exp(piece[LANES : LANES + 1]) * total + piece[0:LANES]
            entering = jnp.where(i + 1 == z, total, entering)
        entering = ROW[s, LANES : LANES + 1] * entering + ROW[s, 0:LANES]
        carried = matmul(CS[s], entering.astype(BF16))
        grown = jnp.exp(CUM[s, CHUNK - 1 : CHUNK, :])
        for i in range(8):
            rows = tiles[i]
            part = carried[rows] if i < 4 else grown * carried[rows]
            gated = (Y[s, rows, :] + part) * Z[s, rows, :]
            scale = lax.rsqrt(jnp.mean(gated * gated, axis=-1, keepdims=True) + epsilon)
            GT[s, rows, :] = (gated * scale * og_ref[...]).astype(BF16)
            if i % 4 == 3:
                for j in range(i - 3, i + 1):
                    pl.when(tp != j)(mix_copy(s, j).start)
        own(s).start()

    def mix_copy(s, i):
        return remote(
            GT.at[s, i * ROWS : (i + 1) * ROWS, :],
            G.at[s, :, pl.ds(own_columns, LANES)],
            sends.at[6],
            mix_recv.at[s // 2],
            (z, y, i // 2, i % 2),
        )

    def own(s):
        return pltpu.make_async_copy(
            GT.at[s, pl.ds(pl.multiple_of(tp * ROWS, ROWS), ROWS), :],
            G.at[s, :, pl.ds(own_columns, LANES)],
            local_sem.at[0],
        )

    def mixed_in(pair):
        ref = G.at[2 * pair : 2 * pair + 2, :, 0:896]
        remote(ref, ref, sends.at[6], mix_recv.at[pair], partner).wait_recv()

    def owns_in():
        ref = G.at[:, :, 0:LANES]
        pltpu.make_async_copy(ref, ref, local_sem.at[0]).wait()

    def multiply(first, last):
        gathered = G[first:last].reshape((last - first) * ROWS, WIDTH)
        result = matmul(gathered, O[...].reshape(WIDTH, WIDTH))
        out_ref[first:last] = result.astype(BF16).reshape(last - first, ROWS, WIDTH)

    def sent(ref, group):
        return remote(ref, ref, sends.at[group], pair_recv.at[0], partner)

    def drain():
        sent(T.at[:, 0:448, :], 0).wait_send()
        sent(T.at[0:3, 0:240, :], 1).wait_send()
        pl.when(sp < 15)(sent(E.at[:, :, 0:8, :], 3).wait_send)
        states_out()

    def ox_drain():
        sent(T.at[0:2, 0:448, :], 2).wait_send()

    def out_drain():
        sent(G.at[:, :, 0:896], 6).wait_send()

    token_pair(0)
    project(0)
    token_last(1)
    steps(0)
    conv_tail(0)
    token_near(3)
    oz.near()
    oz.last()
    out_own()
    token_pair(1)
    project(1)
    token_last(2)
    halo_in(0)
    conv_head(0)
    states(0)
    steps(1)
    conv_tail(1)
    halo_in(1)
    conv_head(1)
    states(1)
    token_last(3)
    token_pair(2)
    project(2)
    steps(2)
    conv_tail(2)
    token_pair(3)
    project(3)
    halo_in(2)
    conv_head(2)
    states(2)
    out_near()
    state_in(0)
    scan(0)
    steps(3)
    conv_tail(3)
    halo_in(3)
    conv_head(3)
    states(3)
    state_in(1)
    scan(1)
    gate(0)
    inside(0)
    gate(1)
    inside(1)
    back_in(0)
    finish(0)
    gate(2)
    inside(2)
    state_in(2)
    scan(2)
    gate(3)
    inside(3)
    back_in(1)
    finish(1)
    state_in(3)
    scan(3)
    back_in(2)
    finish(2)
    back_in(3)
    finish(3)
    out_last()
    drain()
    owns_in()
    mixed_in(0)
    out_pairs()
    ox_drain()
    multiply(0, 2)
    mixed_in(1)
    multiply(2, 4)

    out_drain()


def local(
    tokens,
    norm_gain,
    x_weight,
    z_weight,
    b_weight,
    c_weight,
    dt_weight,
    x_conv,
    b_conv,
    c_conv,
    dt_bias,
    decay_rate,
    out_gain,
    out_weight,
):
    hbm = pl.BlockSpec(memory_space=pltpu.HBM)
    dma = pltpu.SemaphoreType.DMA
    return pl.pallas_call(
        kernel,
        out_shape=pltpu.VMEM(tokens.shape, BF16),
        in_specs=[hbm] * 14,
        out_specs=pl.BlockSpec(memory_space=pltpu.VMEM),
        scratch_shapes=[
            pltpu.SMEM((2,), F32),
            pltpu.SMEM((2,), F32),
            pltpu.VMEM((SEQS, ROWS, WIDTH), BF16),
            pltpu.VMEM((1, WIDTH), F32),
            pltpu.VMEM((2, ROWS), BF16),
            pltpu.VMEM((3, CONV, LANES), F32),
            pltpu.VMEM((1, LANES), F32),
            pltpu.VMEM((SEQS, SPAN, WIDTH), BF16),
            pltpu.VMEM((4, 4, ROWS, 256), BF16),
            pltpu.VMEM((4, 4, ROWS, 384), BF16),
            pltpu.VMEM((4, 4, ROWS, LANES), BF16),
            pltpu.VMEM((2, 512, WIDTH), BF16),
            pltpu.VMEM((SEQS, 3, SPAN + 8, LANES), F32),
            pltpu.VMEM((SEQS, SPAN, LANES), F32),
            pltpu.VMEM((SEQS, SPAN, LANES), F32),
            pltpu.VMEM((SEQS, SPAN, LANES), F32),
            pltpu.VMEM((SEQS, SPAN, LANES), BF16),
            pltpu.VMEM((SEQS, SPAN, LANES), BF16),
            pltpu.VMEM((SEQS, SPAN, LANES), BF16),
            pltpu.VMEM((SEQS, SPAN, LANES), F32),
            pltpu.VMEM((SEQS, 2, LANES, LANES), F32),
            pltpu.VMEM((SEQS, LANES + 16, LANES), BF16),
            pltpu.VMEM((SEQS, 4, LANES + 16, LANES), BF16),
            pltpu.VMEM((SEQS, LANES + 16, LANES), BF16),
            pltpu.VMEM((SEQS, 4, LANES + 16, LANES), BF16),
            pltpu.VMEM((SEQS, LANES + 8, LANES), F32),
            pltpu.VMEM((SEQS, SPAN, LANES), BF16),
            pltpu.VMEM((SEQS, ROWS, WIDTH), BF16),
            dma((7,)),
            dma((27,)),
            dma((SEQS + 1,)),
            dma((SEQS,)),
            dma((SEQS,)),
            dma((SEQS,)),
            dma((2,)),
            dma((1,)),
            dma((11,)),
        ],
        compiler_params=pltpu.CompilerParams(
            collective_id=0, has_side_effects=True, vmem_limit_bytes=60 * 1024 * 1024
        ),
        name="mixer",
    )(
        dt_bias,
        decay_rate,
        tokens,
        norm_gain.reshape(1, -1),
        x_weight,
        z_weight,
        b_weight,
        c_weight,
        dt_weight.T,
        x_conv,
        b_conv,
        c_conv,
        out_gain.reshape(1, -1),
        out_weight.T,
    )


def solution(mesh):
    torus = Mesh(mesh.devices.reshape(4, 4, 4, 2), SP_TP)
    return jax.shard_map(
        local,
        mesh=torus,
        in_specs=(
            P(None, SP_TP, None),
            P(),
            P(SP, TP),
            P(SP, TP),
            P(SP, TP),
            P(SP, TP),
            P(SP, TP),
            P(None, TP),
            P(None, TP),
            P(None, TP),
            P(TP),
            P(TP),
            P(TP),
            P(TP, SP),
        ),
        out_specs=P(None, SP_TP, None),
        check_vma=False,
    )
```

```python
import functools

import jax
import jax.numpy as jnp
from jax import lax
from jax.experimental import pallas as pl
from jax.experimental.pallas import tpu as pltpu
from jax.sharding import Mesh
from jax.sharding import PartitionSpec as P

CONV = 4
SP = ("sp_0", "sp_1")
TP = ("tp_0", "tp_1")
SP_TP = ("sp_0", "sp_1", "tp_0", "tp_1")
LENGTH = 8192
SEQS = 4
SPAN = 512
ROWS = 64
WIDTH = 1024
CHUNK = 256
LANES = 128
epsilon = 1e-05
MESH = pl.DeviceIdType.MESH
F32 = jnp.float32
BF16 = jnp.bfloat16


def remote(src, dst, send, recv, device):
    return pltpu.make_async_remote_copy(
        src_ref=src,
        dst_ref=dst,
        send_sem=send,
        recv_sem=recv,
        device_id=device,
        device_id_type=MESH,
    )


class Ring:
    def __init__(self, place, axis, block, send, recvs, both, direct=False):
        self.block, self.send, self.recvs, self.both = block, send, recvs, both
        self.direct = direct
        self.me = place[axis]
        self.right, self.left = lax.rem(self.me + 1, 4), lax.rem(self.me + 3, 4)
        self.far = lax.rem(self.me + 2, 4)
        to = lambda i: tuple(i if k == axis else p for k, p in enumerate(place))
        self.to_right, self.to_left, self.to_far = to(self.right), to(self.left), to(self.far)

    def copy(self, ref, lane, device):
        return remote(ref, ref, self.send, self.recvs[lane], device)

    def own(self):
        self.copy(self.block(self.me, None), 0, self.to_right).start()
        self.copy(self.block(self.me, None), 0, self.to_left).start()
        if self.direct:
            self.copy(self.block(self.me, None), 1, self.to_far).start()

    def near(self):
        self.copy(self.both, 0, self.to_right).wait_recv()
        if not self.direct:
            self.copy(self.block(self.left, 0), 1, self.to_right).start()
            self.copy(self.block(self.right, 1), 1, self.to_left).start()

    def last(self):
        self.copy(self.block(self.far, None), 1, self.to_right).wait_recv()


def half_rows(half):
    return slice(None) if half is None else slice(32 * half, 32 * half + 32)


def half_blocks(half):
    return slice(None) if half is None else slice(2 * half, 2 * half + 2)


def matmul(a, b, dims=((1,), (0,)), precision=None):
    return lax.dot_general(a, b, (dims, ((), ())), precision=precision, preferred_element_type=F32)


def silu(value):
    half = 0.5 * value
    return half + half * jnp.tanh(half)


def kernel(
    bias_in,
    rate_in,
    tokens_in,
    gain_in,
    xw_in,
    zw_in,
    bw_in,
    cw_in,
    dw_in,
    xt_in,
    bt_in,
    ct_in,
    og_in,
    ow_in,
    out_ref,
    bias_ref,
    rate_ref,
    tokens_ref,
    gain_ref,
    dw_ref,
    taps_ref,
    og_ref,
    T,
    WA,
    WB,
    OYZ,
    O,
    E,
    Z,
    DT,
    CUM,
    XS,
    BS,
    CS,
    Y,
    U,
    SS,
    RS,
    SR,
    RR,
    ROW,
    GT,
    G,
    sends,
    ring_recv,
    pair_recv,
    halo_recv,
    state_recv,
    back_recv,
    mix_recv,
    local_sem,
    load_sem,
):
    z, y = lax.axis_index("sp_0"), lax.axis_index("sp_1")
    x, c = lax.axis_index("tp_0"), lax.axis_index("tp_1")
    place = (z, y, x, c)
    sp, tp = z * 4 + y, x * 2 + c
    other = 1 - c
    partner = (z, y, x, other)

    def sp_device(i):
        return (i // 4, lax.rem(i, 4), x, c)

    def tp_device(i):
        return (z, y, i // 2, lax.rem(i, 2))

    barrier = pltpu.get_barrier_semaphore()

    def greet(semaphore, there):
        pl.semaphore_signal(semaphore, inc=1, device_id=there, device_id_type=MESH)

    for step in (1, 3):
        greet(barrier, (z, y, lax.rem(x + step, 4), c))
    greet(barrier, partner)
    for step in (1, 2, 3):
        greet(barrier, (z, lax.rem(y + step, 4), x, c))
        greet(barrier, (lax.rem(z + step, 4), y, x, c))

    group = lambda k, *pairs: [pltpu.make_async_copy(*pair, load_sem.at[k]) for pair in pairs]
    weights_in = group(
        0,
        (xw_in, WA.at[z, y, :, 0:128]),
        (bw_in, WA.at[z, y, :, 128:256]),
        (cw_in, WB.at[z, y, :, 0:128]),
        (zw_in, WB.at[z, y, :, 128:256]),
        (ow_in, OYZ.at[z, y]),
    )
    (dt_in,) = group(1, (dw_in, dw_ref))
    (gain_copy,) = group(2, (gain_in, gain_ref))
    token_copies = [group(3 + s, (tokens_in.at[s], tokens_ref.at[s]))[0] for s in range(SEQS)]
    taps_in = group(
        7, *((ref, taps_ref.at[k]) for k, ref in enumerate((xt_in, bt_in, ct_in)))
    )
    small_in = [
        *group(8, (og_in, og_ref)),
        *group(9, (bias_in, bias_ref)),
        *group(10, (rate_in, rate_ref)),
    ]
    for load in (*weights_in, dt_in, gain_copy, *token_copies, *taps_in, *small_in):
        load.start()

    lane = lax.broadcasted_iota(jnp.int32, (1, LANES), 1)
    low = lane < 64

    head_at = lax.broadcasted_iota(jnp.int32, (2, LANES), 0)
    lane_at = lax.broadcasted_iota(jnp.int32, (2, LANES), 1)
    spread = (lane_at // 64 == head_at).astype(BF16)
    five = T.at[0, 0:80, 0:512]
    pltpu.make_async_copy(five, five, load_sem.at[0]).wait()
    dt_in.wait()
    gain_copy.wait()
    WB[z, y, :, 256:384] = matmul(dw_ref[...], spread, ((0,), (0,))).astype(BF16)

    def normed(s):
        token_copies[s].wait()
        source = tokens_ref[s].astype(F32)
        scale = lax.rsqrt(jnp.mean(source * source, axis=-1, keepdims=True) + epsilon)
        T[s, pl.ds(pl.multiple_of(tp * ROWS, ROWS), ROWS), :] = (
            source * scale * gain_ref[...]
        ).astype(BF16)

    own_columns = pl.multiple_of((c * 4 + x) * LANES, LANES)
    normed(0)
    pl.semaphore_wait(barrier, 9)

    def token_block(s):
        def block(i, half):
            start = (i * 2 + c) * ROWS + (0 if half is None else 32 * half)
            rows = ROWS if half is None else 32
            return T.at[s, pl.ds(pl.multiple_of(start, 32), rows), :]

        return block

    def ring(axis, block, number, rows, direct=False):
        group = 0 if number < SEQS else 1 if number < 16 else 2
        both = T.at[0, 0:rows, :]
        send = sends.at[group]
        last = number if number < 6 else max(6, number - 7)
        recvs = (ring_recv.at[number], ring_recv.at[17 + last])
        return Ring(place, axis, block, send, recvs, both, direct)

    tokens = [ring(2, token_block(s), s, 2 * ROWS) for s in range(SEQS)]
    wa1 = ring(1, lambda i, h: WA.at[z, i, half_rows(h)], 4, 32, True)
    wb1 = ring(0, lambda i, h: WB.at[i, y, half_rows(h)], 5, 48, True)
    shifted = lambda i, k: lax.rem(i + k, 4)
    wa2 = [ring(0, lambda i, h, k=k: WA.at[i, shifted(y, k), half_rows(h)], 6 + k, 32, k in (2,)) for k in range(4)]
    wb2 = [ring(1, lambda i, h, k=k: WB.at[shifted(z, k), i, half_rows(h)], 10 + k, 48, k in (2,)) for k in range(4)]
    oy = ring(1, lambda i, h: OYZ.at[z, i], 14, 16, True)
    oz = ring(0, lambda i, h: OYZ.at[i], 15, ROWS, True)

    def out_rows(core, i, half):
        rows = LANES if half is None else 64
        start = i * LANES + (0 if half is None else 64 * half)
        return O.at[core, pl.ds(pl.multiple_of(start, 64), rows), :]

    ox = ring(2, lambda i, h: out_rows(c, i, h), 16, 256)

    def pair_copy(s, k, core):
        i, half = (
            (x, None),
            (tokens[s].left, None),
            (tokens[s].right, None),
            (tokens[s].far, 0),
            (tokens[s].far, 1),
        )[k]
        start = (i * 2 + core) * ROWS + (0 if half is None else 32 * half)
        rows = ROWS if half is None else 32
        ref = T.at[s, pl.ds(pl.multiple_of(start, 32), rows), :]
        return remote(ref, ref, sends.at[0], pair_recv.at[s], partner)

    def out_pair(k, core):
        i, half = ((x, None), (ox.left, None), (ox.right, None), (ox.far, 0), (ox.far, 1))[k]
        ref = out_rows(core, i, half)
        return remote(ref, ref, sends.at[2], pair_recv.at[SEQS], partner)

    def out_own():
        block = OYZ[...].reshape(WIDTH, LANES).astype(F32).T.astype(BF16)
        O[c, pl.ds(pl.multiple_of(x * LANES, LANES), LANES), :] = block
        ox.own()
        out_pair(0, c).start()

    def out_near():
        ox.near()
        out_pair(1, c).start()
        out_pair(2, c).start()

    def out_last():
        ox.last()
        out_pair(3, c).start()
        out_pair(4, c).start()

    def out_pairs():
        remote(T.at[0], T.at[0], sends.at[2], pair_recv.at[SEQS], partner).wait_recv()

    def token_own(s):
        tokens[s].own()
        pair_copy(s, 0, c).start()

    def token_near(s):
        tokens[s].near()
        pair_copy(s, 1, c).start()
        pair_copy(s, 2, c).start()

    def token_last(s):
        tokens[s].last()
        pair_copy(s, 3, c).start()
        pair_copy(s, 4, c).start()

    wa1.own()
    wb1.own()
    wa2[0].own()
    wb2[0].own()
    token_own(0)
    normed(1)
    token_own(1)
    normed(2)
    normed(3)
    wa1.near()
    wa2[1].own()
    wa2[3].own()
    wb1.near()
    wb2[1].own()
    wb2[3].own()
    wa1.last()
    wa2[2].own()
    wb1.last()
    wb2[2].own()
    oy.own()
    wa2[0].near()
    wb2[0].near()
    token_near(0)
    token_own(2)
    wa2[1].near()
    wa2[3].near()
    token_near(1)
    token_own(3)
    wb2[1].near()
    wb2[3].near()
    wa2[2].near()
    wb2[2].near()
    oy.near()
    oy.last()
    oz.own()
    token_last(0)
    token_near(2)
    weights = T.at[0, 0:160, :]
    remote(weights, weights, sends.at[1], ring_recv.at[23], partner).wait_recv()

    pltpu.make_async_copy(taps_ref, taps_ref, load_sem.at[7]).wait()
    for load in small_in:
        load.wait()
    bias = jnp.where(low, bias_ref[0], bias_ref[1])
    rate = jnp.where(low, rate_ref[0], rate_ref[1])
    row_at = lax.broadcasted_iota(jnp.int32, (CHUNK, CHUNK), 0)
    column_at = lax.broadcasted_iota(jnp.int32, (CHUNK, CHUNK), 1)
    lower = row_at >= column_at
    ones_below = lower.astype(BF16)
    tiles = [slice(k * ROWS, (k + 1) * ROWS) for k in range(SPAN // ROWS)]
    following = sp_device(lax.rem(sp + 1, 16))

    def packed(state, log):
        log = jnp.broadcast_to(log, (16, LANES))
        return jnp.concatenate([state, log], axis=0).astype(BF16)

    def share_row(s):
        for k in (1, 3, 2):
            there = (z, lax.rem(y + k, 4), x, c)
            copy = remote(SS.at[s], RS.at[s, y], sends.at[4], state_recv.at[s], there)
            pl.when((y + k < 4) | (z < 3))(copy.start)
        RS[s, y] = SS[s]

    def share_up(s):
        for k in (1, 2, 3):
            there = (lax.rem(z + k, 4), y, x, c)
            copy = remote(SR.at[s], RR.at[s, z], sends.at[5], back_recv.at[s], there)
            pl.when(z + k < 4)(copy.start)

    def states_out():
        for n in (1, 2, 3):
            ref = RS.at[:, 0:n]
            copy = remote(ref, ref, sends.at[4], state_recv.at[0], partner)
            pl.when(jnp.where(z < 3, 3, 3 - y) == n)(copy.wait_send)
            copy = remote(ref, ref, sends.at[5], back_recv.at[0], partner)
            pl.when(3 - z == n)(copy.wait_send)

    def halo(s):
        return remote(
            E.at[s, :, SPAN : SPAN + 8, :],
            E.at[s, :, 0:8, :],
            sends.at[3],
            halo_recv.at[s],
            following,
        )

    def token_pair(s):
        half = T.at[s, 0:256, :]
        remote(half, half, sends.at[0], pair_recv.at[s], partner).wait_recv()

    def halo_in(s):
        pl.when(sp > 0)(halo(s).wait_recv)

    def state_in(s):
        for n in (1, 2, 3):
            ref = RS.at[s, 0:n]
            copy = remote(ref, ref, sends.at[4], state_recv.at[s], partner)
            pl.when(jnp.where(z < 3, 3, y) == n)(copy.wait_recv)

    def back_in(s):
        for n in (1, 2, 3):
            ref = RR.at[s, 0:n]
            copy = remote(ref, ref, sends.at[5], back_recv.at[s], partner)
            pl.when(z == n)(copy.wait_recv)

    def project(s):
        product = matmul(T[s], WA[...].reshape(WIDTH, 256))
        E[s, 0, 8 : SPAN + 8, :] = product[:, 0:128]
        E[s, 1, 8 : SPAN + 8, :] = product[:, 128:256]
        product = matmul(T[s], WB[...].reshape(WIDTH, 384))
        E[s, 2, 8 : SPAN + 8, :] = product[:, 0:128]
        Z[s] = product[:, 128:256]
        DT[s] = product[:, 256:384]
        pl.when(sp < 15)(halo(s).start)

    def gate(s):
        for rows in tiles:
            Z[s, rows, :] = silu(Z[s, rows, :]) * jnp.exp(CUM[s, rows, :])

    def steps(s):
        for rows in tiles:
            step = DT[s, rows, :] + bias
            step = jnp.maximum(step, 0.0) + jnp.log1p(jnp.exp(-jnp.abs(step)))
            DT[s, rows, :] = step
            XS[s, rows, :] = (-(step * rate) / LENGTH).astype(BF16)
        for k in range(2):
            rows = slice(k * CHUNK, (k + 1) * CHUNK)
            CUM[s, rows, :] = matmul(ones_below, XS[s, rows, :])

    def conv_tail(s):
        convolve(s, tiles[1:])
        gains(s, 1)

    def conv_head(s):
        for k in range(3):
            E[s, k, 0:8, :] = jnp.where(sp == 0, 0.0, E[s, k, 0:8, :])
        convolve(s, tiles[:1])

    def convolve(s, some):
        for k in range(3):
            taps = [taps_ref[k, offset : offset + 1, :] for offset in range(CONV)]
            for rows in some:
                start = rows.start + 5
                running = taps[0] * E[s, k, start : start + ROWS, :]
                for offset in range(1, CONV):
                    first = start + offset
                    running = running + taps[offset] * E[s, k, first : first + ROWS, :]
                running = silu(running)
                if k == 0:
                    decayed = DT[s, rows, :] * jnp.exp(-CUM[s, rows, :])
                    XS[s, rows, :] = (running * decayed).astype(BF16)
                elif k == 1:
                    BS[s, rows, :] = running.astype(BF16)
                else:
                    CS[s, rows, :] = running.astype(BF16)

    def gains(s, k):
        rows = slice(k * CHUNK, (k + 1) * CHUNK)
        U[s, k] = matmul(BS[s, rows, :], XS[s, rows, :], ((0,), (0,)))

    def states(s):
        gains(s, 0)
        first, second = CUM[s, CHUNK - 1 : CHUNK, :], CUM[s, SPAN - 1 : SPAN, :]
        final = jnp.exp(second) * (jnp.exp(first) * U[s, 0] + U[s, 1])
        SS[s] = packed(final, first + second)
        share_row(s)

    def inside(s):
        for k in range(2):
            rows = slice(k * CHUNK, (k + 1) * CHUNK)
            scores = matmul(CS[s, rows, :], BS[s, rows, :], ((1,), (1,)))
            scores = jnp.where(lower, scores, 0.0).astype(BF16)
            part = matmul(scores, XS[s, rows, :])
            if k:
                grown = jnp.exp(CUM[s, CHUNK - 1 : CHUNK, :])
                part = part + grown * matmul(CS[s, rows, :], U[s, 0].astype(BF16))
            Y[s, rows, :] = part

    def scan(s):
        before, before_log = jnp.zeros((LANES, LANES), F32), jnp.zeros((1, LANES), F32)
        total, total_log = before, before_log
        for i in range(4):
            piece = RS[s, i].astype(F32)
            log = piece[LANES : LANES + 1]
            total = jnp.exp(log) * total + piece[0:LANES]
            total_log = total_log + log
            if i < 3:
                before = jnp.where(i + 1 == y, total, before)
                before_log = jnp.where(i + 1 == y, total_log, before_log)
        ROW[s, 0:LANES] = before
        ROW[s, LANES : LANES + 1] = jnp.exp(before_log)
        SR[s] = packed(total, total_log)
        share_up(s)

    def finish(s):
        total = jnp.zeros((LANES, LANES), F32)
        entering = total
        for i in range(3):
            piece = RR[s, i].astype(F32)
            total = jnp.exp(piece[LANES : LANES + 1]) * total + piece[0:LANES]
            entering = jnp.where(i + 1 == z, total, entering)
        entering = ROW[s, LANES : LANES + 1] * entering + ROW[s, 0:LANES]
        carried = matmul(CS[s], entering.astype(BF16))
        grown = jnp.exp(CUM[s, CHUNK - 1 : CHUNK, :])
        for i in range(8):
            rows = tiles[i]
            part = carried[rows] if i < 4 else grown * carried[rows]
            gated = (Y[s, rows, :] + part) * Z[s, rows, :]
            scale = lax.rsqrt(jnp.mean(gated * gated, axis=-1, keepdims=True) + epsilon)
            GT[s, rows, :] = (gated * scale * og_ref[...]).astype(BF16)
            if i % 4 == 3:
                for j in range(i - 3, i + 1):
                    pl.when(tp != j)(mix_copy(s, j).start)
        own(s).start()

    def mix_copy(s, i):
        return remote(
            GT.at[s, i * ROWS : (i + 1) * ROWS, :],
            G.at[s, :, pl.ds(own_columns, LANES)],
            sends.at[6],
            mix_recv.at[s // 2],
            (z, y, i // 2, i % 2),
        )

    def own(s):
        return pltpu.make_async_copy(
            GT.at[s, pl.ds(pl.multiple_of(tp * ROWS, ROWS), ROWS), :],
            G.at[s, :, pl.ds(own_columns, LANES)],
            local_sem.at[0],
        )

    def mixed_in(pair):
        ref = G.at[2 * pair : 2 * pair + 2, :, 0:896]
        remote(ref, ref, sends.at[6], mix_recv.at[pair], partner).wait_recv()

    def owns_in():
        ref = G.at[:, :, 0:LANES]
        pltpu.make_async_copy(ref, ref, local_sem.at[0]).wait()

    def multiply(first, last):
        gathered = G[first:last].reshape((last - first) * ROWS, WIDTH)
        result = matmul(gathered, O[...].reshape(WIDTH, WIDTH))
        out_ref[first:last] = result.astype(BF16).reshape(last - first, ROWS, WIDTH)

    def sent(ref, group):
        return remote(ref, ref, sends.at[group], pair_recv.at[0], partner)

    def drain():
        sent(T.at[:, 0:448, :], 0).wait_send()
        sent(T.at[0:3, 0:240, :], 1).wait_send()
        pl.when(sp < 15)(sent(E.at[:, :, 0:8, :], 3).wait_send)
        states_out()

    def ox_drain():
        sent(T.at[0:2, 0:448, :], 2).wait_send()

    def out_drain():
        sent(G.at[:, :, 0:896], 6).wait_send()

    token_pair(0)
    project(0)
    token_last(1)
    steps(0)
    conv_tail(0)
    token_near(3)
    oz.near()
    oz.last()
    out_own()
    token_pair(1)
    project(1)
    token_last(2)
    halo_in(0)
    conv_head(0)
    states(0)
    steps(1)
    conv_tail(1)
    halo_in(1)
    conv_head(1)
    states(1)
    token_last(3)
    token_pair(2)
    project(2)
    steps(2)
    conv_tail(2)
    token_pair(3)
    project(3)
    halo_in(2)
    conv_head(2)
    states(2)
    out_near()
    state_in(0)
    scan(0)
    steps(3)
    conv_tail(3)
    halo_in(3)
    conv_head(3)
    states(3)
    state_in(1)
    scan(1)
    gate(0)
    inside(0)
    gate(1)
    inside(1)
    back_in(0)
    finish(0)
    gate(2)
    inside(2)
    state_in(2)
    scan(2)
    gate(3)
    inside(3)
    back_in(1)
    finish(1)
    state_in(3)
    scan(3)
    back_in(2)
    finish(2)
    back_in(3)
    finish(3)
    out_last()
    drain()
    owns_in()
    mixed_in(0)
    out_pairs()
    ox_drain()
    multiply(0, 2)
    mixed_in(1)
    multiply(2, 4)

    out_drain()


def local(
    tokens,
    norm_gain,
    x_weight,
    z_weight,
    b_weight,
    c_weight,
    dt_weight,
    x_conv,
    b_conv,
    c_conv,
    dt_bias,
    decay_rate,
    out_gain,
    out_weight,
):
    hbm = pl.BlockSpec(memory_space=pltpu.HBM)
    dma = pltpu.SemaphoreType.DMA
    return pl.pallas_call(
        kernel,
        out_shape=pltpu.VMEM(tokens.shape, BF16),
        in_specs=[hbm] * 14,
        out_specs=pl.BlockSpec(memory_space=pltpu.VMEM),
        scratch_shapes=[
            pltpu.SMEM((2,), F32),
            pltpu.SMEM((2,), F32),
            pltpu.VMEM((SEQS, ROWS, WIDTH), BF16),
            pltpu.VMEM((1, WIDTH), F32),
            pltpu.VMEM((2, ROWS), BF16),
            pltpu.VMEM((3, CONV, LANES), F32),
            pltpu.VMEM((1, LANES), F32),
            pltpu.VMEM((SEQS, SPAN, WIDTH), BF16),
            pltpu.VMEM((4, 4, ROWS, 256), BF16),
            pltpu.VMEM((4, 4, ROWS, 384), BF16),
            pltpu.VMEM((4, 4, ROWS, LANES), BF16),
            pltpu.VMEM((2, 512, WIDTH), BF16),
            pltpu.VMEM((SEQS, 3, SPAN + 8, LANES), F32),
            pltpu.VMEM((SEQS, SPAN, LANES), F32),
            pltpu.VMEM((SEQS, SPAN, LANES), F32),
            pltpu.VMEM((SEQS, SPAN, LANES), F32),
            pltpu.VMEM((SEQS, SPAN, LANES), BF16),
            pltpu.VMEM((SEQS, SPAN, LANES), BF16),
            pltpu.VMEM((SEQS, SPAN, LANES), BF16),
            pltpu.VMEM((SEQS, SPAN, LANES), F32),
            pltpu.VMEM((SEQS, 2, LANES, LANES), F32),
            pltpu.VMEM((SEQS, LANES + 16, LANES), BF16),
            pltpu.VMEM((SEQS, 4, LANES + 16, LANES), BF16),
            pltpu.VMEM((SEQS, LANES + 16, LANES), BF16),
            pltpu.VMEM((SEQS, 4, LANES + 16, LANES), BF16),
            pltpu.VMEM((SEQS, LANES + 8, LANES), F32),
            pltpu.VMEM((SEQS, SPAN, LANES), BF16),
            pltpu.VMEM((SEQS, ROWS, WIDTH), BF16),
            dma((7,)),
            dma((27,)),
            dma((SEQS + 1,)),
            dma((SEQS,)),
            dma((SEQS,)),
            dma((SEQS,)),
            dma((2,)),
            dma((1,)),
            dma((11,)),
        ],
        compiler_params=pltpu.CompilerParams(
            collective_id=0, has_side_effects=True, vmem_limit_bytes=60 * 1024 * 1024
        ),
        name="mixer",
    )(
        dt_bias,
        decay_rate,
        tokens,
        norm_gain.reshape(1, -1),
        x_weight,
        z_weight,
        b_weight,
        c_weight,
        dt_weight.T,
        x_conv,
        b_conv,
        c_conv,
        out_gain.reshape(1, -1),
        out_weight.T,
    )


def solution(mesh):
    torus = Mesh(mesh.devices.reshape(4, 4, 4, 2), SP_TP)
    return jax.shard_map(
        local,
        mesh=torus,
        in_specs=(
            P(None, SP_TP, None),
            P(),
            P(SP, TP),
            P(SP, TP),
            P(SP, TP),
            P(SP, TP),
            P(SP, TP),
            P(None, TP),
            P(None, TP),
            P(None, TP),
            P(TP),
            P(TP),
            P(TP),
            P(TP, SP),
        ),
        out_specs=P(None, SP_TP, None),
        check_vma=False,
    )
```

```python
import functools

import jax
import jax.numpy as jnp
from jax import lax
from jax.experimental import pallas as pl
from jax.experimental.pallas import tpu as pltpu
from jax.sharding import Mesh
from jax.sharding import PartitionSpec as P

CONV = 4
SP = ("sp_0", "sp_1")
TP = ("tp_0", "tp_1")
SP_TP = ("sp_0", "sp_1", "tp_0", "tp_1")
LENGTH = 8192
SEQS = 4
SPAN = 512
ROWS = 64
WIDTH = 1024
CHUNK = 256
LANES = 128
epsilon = 1e-05
MESH = pl.DeviceIdType.MESH
F32 = jnp.float32
BF16 = jnp.bfloat16


def remote(src, dst, send, recv, device):
    return pltpu.make_async_remote_copy(
        src_ref=src,
        dst_ref=dst,
        send_sem=send,
        recv_sem=recv,
        device_id=device,
        device_id_type=MESH,
    )


class Ring:
    def __init__(self, place, axis, block, send, recvs, both, direct=False):
        self.block, self.send, self.recvs, self.both = block, send, recvs, both
        self.direct = direct
        self.me = place[axis]
        self.right, self.left = lax.rem(self.me + 1, 4), lax.rem(self.me + 3, 4)
        self.far = lax.rem(self.me + 2, 4)
        to = lambda i: tuple(i if k == axis else p for k, p in enumerate(place))
        self.to_right, self.to_left, self.to_far = to(self.right), to(self.left), to(self.far)

    def copy(self, ref, lane, device):
        return remote(ref, ref, self.send, self.recvs[lane], device)

    def own(self):
        self.copy(self.block(self.me, None), 0, self.to_right).start()
        self.copy(self.block(self.me, None), 0, self.to_left).start()
        if self.direct:
            self.copy(self.block(self.me, None), 1, self.to_far).start()

    def near(self):
        self.copy(self.both, 0, self.to_right).wait_recv()
        if not self.direct:
            self.copy(self.block(self.left, 0), 1, self.to_right).start()
            self.copy(self.block(self.right, 1), 1, self.to_left).start()

    def last(self):
        self.copy(self.block(self.far, None), 1, self.to_right).wait_recv()


def half_rows(half):
    return slice(None) if half is None else slice(32 * half, 32 * half + 32)


def half_blocks(half):
    return slice(None) if half is None else slice(2 * half, 2 * half + 2)


def matmul(a, b, dims=((1,), (0,)), precision=None):
    return lax.dot_general(a, b, (dims, ((), ())), precision=precision, preferred_element_type=F32)


def silu(value):
    half = 0.5 * value
    return half + half * jnp.tanh(half)


def kernel(
    bias_in,
    rate_in,
    tokens_in,
    gain_in,
    xw_in,
    zw_in,
    bw_in,
    cw_in,
    dw_in,
    xt_in,
    bt_in,
    ct_in,
    og_in,
    ow_in,
    out_ref,
    bias_ref,
    rate_ref,
    tokens_ref,
    gain_ref,
    dw_ref,
    taps_ref,
    og_ref,
    T,
    WA,
    WB,
    OYZ,
    O,
    E,
    Z,
    DT,
    CUM,
    XS,
    BS,
    CS,
    Y,
    U,
    SS,
    RS,
    SR,
    RR,
    ROW,
    GT,
    G,
    sends,
    ring_recv,
    pair_recv,
    halo_recv,
    state_recv,
    back_recv,
    mix_recv,
    local_sem,
    load_sem,
):
    z, y = lax.axis_index("sp_0"), lax.axis_index("sp_1")
    x, c = lax.axis_index("tp_0"), lax.axis_index("tp_1")
    place = (z, y, x, c)
    sp, tp = z * 4 + y, x * 2 + c
    other = 1 - c
    partner = (z, y, x, other)

    def sp_device(i):
        return (i // 4, lax.rem(i, 4), x, c)

    def tp_device(i):
        return (z, y, i // 2, lax.rem(i, 2))

    barrier = pltpu.get_barrier_semaphore()

    def greet(semaphore, there):
        pl.semaphore_signal(semaphore, inc=1, device_id=there, device_id_type=MESH)

    for step in (1, 3):
        greet(barrier, (z, y, lax.rem(x + step, 4), c))
    greet(barrier, partner)
    for step in (1, 2, 3):
        greet(barrier, (z, lax.rem(y + step, 4), x, c))
        greet(barrier, (lax.rem(z + step, 4), y, x, c))

    group = lambda k, *pairs: [pltpu.make_async_copy(*pair, load_sem.at[k]) for pair in pairs]
    weights_in = group(
        0,
        (xw_in, WA.at[z, y, :, 0:128]),
        (bw_in, WA.at[z, y, :, 128:256]),
        (cw_in, WB.at[z, y, :, 0:128]),
        (zw_in, WB.at[z, y, :, 128:256]),
        (ow_in, OYZ.at[z, y]),
    )
    (dt_in,) = group(1, (dw_in, dw_ref))
    (gain_copy,) = group(2, (gain_in, gain_ref))
    token_copies = group(3, (tokens_in, tokens_ref))
    taps_in = group(
        4, *((ref, taps_ref.at[k]) for k, ref in enumerate((xt_in, bt_in, ct_in)))
    )
    small_in = [
        *group(5, (og_in, og_ref)),
        *group(6, (bias_in, bias_ref)),
        *group(7, (rate_in, rate_ref)),
    ]
    for load in (*weights_in, dt_in, gain_copy, *token_copies, *taps_in, *small_in):
        load.start()

    lane = lax.broadcasted_iota(jnp.int32, (1, LANES), 1)
    low = lane < 64

    head_at = lax.broadcasted_iota(jnp.int32, (2, LANES), 0)
    lane_at = lax.broadcasted_iota(jnp.int32, (2, LANES), 1)
    spread = (lane_at // 64 == head_at).astype(BF16)
    five = T.at[0, 0:80, 0:512]
    pltpu.make_async_copy(five, five, load_sem.at[0]).wait()
    dt_in.wait()
    gain_copy.wait()
    WB[z, y, :, 256:384] = matmul(dw_ref[...], spread, ((0,), (0,))).astype(BF16)

    def normed(s):
        if s == 0:
            token_copies[0].wait()
        source = tokens_ref[s].astype(F32)
        scale = lax.rsqrt(jnp.mean(source * source, axis=-1, keepdims=True) + epsilon)
        T[s, pl.ds(pl.multiple_of(tp * ROWS, ROWS), ROWS), :] = (
            source * scale * gain_ref[...]
        ).astype(BF16)

    own_columns = pl.multiple_of((c * 4 + x) * LANES, LANES)
    normed(0)
    pl.semaphore_wait(barrier, 9)

    def token_block(s):
        def block(i, half):
            start = (i * 2 + c) * ROWS + (0 if half is None else 32 * half)
            rows = ROWS if half is None else 32
            return T.at[s, pl.ds(pl.multiple_of(start, 32), rows), :]

        return block

    def ring(axis, block, number, rows, direct=False):
        group = 0 if number < SEQS else 1 if number < 16 else 2
        both = T.at[0, 0:rows, :]
        send = sends.at[group]
        last = number if number < 6 else max(6, number - 7)
        recvs = (ring_recv.at[number], ring_recv.at[17 + last])
        return Ring(place, axis, block, send, recvs, both, direct)

    tokens = [ring(2, token_block(s), s, 2 * ROWS) for s in range(SEQS)]
    wa1 = ring(1, lambda i, h: WA.at[z, i, half_rows(h)], 4, 32, True)
    wb1 = ring(0, lambda i, h: WB.at[i, y, half_rows(h)], 5, 48, True)
    shifted = lambda i, k: lax.rem(i + k, 4)
    wa2 = [ring(0, lambda i, h, k=k: WA.at[i, shifted(y, k), half_rows(h)], 6 + k, 32, k in (2,)) for k in range(4)]
    wb2 = [ring(1, lambda i, h, k=k: WB.at[shifted(z, k), i, half_rows(h)], 10 + k, 48, k in (2,)) for k in range(4)]
    oy = ring(1, lambda i, h: OYZ.at[z, i], 14, 16, True)
    oz = ring(0, lambda i, h: OYZ.at[i], 15, ROWS, True)

    def out_rows(core, i, half):
        rows = LANES if half is None else 64
        start = i * LANES + (0 if half is None else 64 * half)
        return O.at[core, pl.ds(pl.multiple_of(start, 64), rows), :]

    ox = ring(2, lambda i, h: out_rows(c, i, h), 16, 256)

    def pair_copy(s, k, core):
        i, half = (
            (x, None),
            (tokens[s].left, None),
            (tokens[s].right, None),
            (tokens[s].far, 0),
            (tokens[s].far, 1),
        )[k]
        start = (i * 2 + core) * ROWS + (0 if half is None else 32 * half)
        rows = ROWS if half is None else 32
        ref = T.at[s, pl.ds(pl.multiple_of(start, 32), rows), :]
        return remote(ref, ref, sends.at[0], pair_recv.at[s], partner)

    def out_pair(k, core):
        i, half = ((x, None), (ox.left, None), (ox.right, None), (ox.far, 0), (ox.far, 1))[k]
        ref = out_rows(core, i, half)
        return remote(ref, ref, sends.at[2], pair_recv.at[SEQS], partner)

    def out_own():
        block = OYZ[...].reshape(WIDTH, LANES).astype(F32).T.astype(BF16)
        O[c, pl.ds(pl.multiple_of(x * LANES, LANES), LANES), :] = block
        ox.own()
        out_pair(0, c).start()

    def out_near():
        ox.near()
        out_pair(1, c).start()
        out_pair(2, c).start()

    def out_last():
        ox.last()
        out_pair(3, c).start()
        out_pair(4, c).start()

    def out_pairs():
        remote(T.at[0], T.at[0], sends.at[2], pair_recv.at[SEQS], partner).wait_recv()

    def token_own(s):
        tokens[s].own()
        pair_copy(s, 0, c).start()

    def token_near(s):
        tokens[s].near()
        pair_copy(s, 1, c).start()
        pair_copy(s, 2, c).start()

    def token_last(s):
        tokens[s].last()
        pair_copy(s, 3, c).start()
        pair_copy(s, 4, c).start()

    wa1.own()
    wb1.own()
    wa2[0].own()
    wb2[0].own()
    token_own(0)
    normed(1)
    token_own(1)
    normed(2)
    normed(3)
    wa1.near()
    wa2[1].own()
    wa2[3].own()
    wb1.near()
    wb2[1].own()
    wb2[3].own()
    wa1.last()
    wa2[2].own()
    wb1.last()
    wb2[2].own()
    oy.own()
    wa2[0].near()
    wb2[0].near()
    token_near(0)
    token_own(2)
    wa2[1].near()
    wa2[3].near()
    token_near(1)
    token_own(3)
    wb2[1].near()
    wb2[3].near()
    wa2[2].near()
    wb2[2].near()
    oy.near()
    oy.last()
    oz.own()
    token_last(0)
    token_near(2)
    weights = T.at[0, 0:160, :]
    remote(weights, weights, sends.at[1], ring_recv.at[23], partner).wait_recv()

    pltpu.make_async_copy(taps_ref, taps_ref, load_sem.at[4]).wait()
    for load in small_in:
        load.wait()
    bias = jnp.where(low, bias_ref[0], bias_ref[1])
    rate = jnp.where(low, rate_ref[0], rate_ref[1])
    row_at = lax.broadcasted_iota(jnp.int32, (CHUNK, CHUNK), 0)
    column_at = lax.broadcasted_iota(jnp.int32, (CHUNK, CHUNK), 1)
    lower = row_at >= column_at
    ones_below = lower.astype(BF16)
    tiles = [slice(k * ROWS, (k + 1) * ROWS) for k in range(SPAN // ROWS)]
    following = sp_device(lax.rem(sp + 1, 16))

    def packed(state, log):
        log = jnp.broadcast_to(log, (16, LANES))
        return jnp.concatenate([state, log], axis=0).astype(BF16)

    def share_row(s):
        for k in (1, 3, 2):
            there = (z, lax.rem(y + k, 4), x, c)
            copy = remote(SS.at[s], RS.at[s, y], sends.at[4], state_recv.at[s], there)
            pl.when((y + k < 4) | (z < 3))(copy.start)
        RS[s, y] = SS[s]

    def share_up(s):
        for k in (1, 2, 3):
            there = (lax.rem(z + k, 4), y, x, c)
            copy = remote(SR.at[s], RR.at[s, z], sends.at[5], back_recv.at[s], there)
            pl.when(z + k < 4)(copy.start)

    def states_out():
        for n in (1, 2, 3):
            ref = RS.at[:, 0:n]
            copy = remote(ref, ref, sends.at[4], state_recv.at[0], partner)
            pl.when(jnp.where(z < 3, 3, 3 - y) == n)(copy.wait_send)
            copy = remote(ref, ref, sends.at[5], back_recv.at[0], partner)
            pl.when(3 - z == n)(copy.wait_send)

    def halo(s):
        return remote(
            E.at[s, :, SPAN : SPAN + 8, :],
            E.at[s, :, 0:8, :],
            sends.at[3],
            halo_recv.at[s],
            following,
        )

    def token_pair(s):
        half = T.at[s, 0:256, :]
        remote(half, half, sends.at[0], pair_recv.at[s], partner).wait_recv()

    def halo_in(s):
        pl.when(sp > 0)(halo(s).wait_recv)

    def state_in(s):
        for n in (1, 2, 3):
            ref = RS.at[s, 0:n]
            copy = remote(ref, ref, sends.at[4], state_recv.at[s], partner)
            pl.when(jnp.where(z < 3, 3, y) == n)(copy.wait_recv)

    def back_in(s):
        for n in (1, 2, 3):
            ref = RR.at[s, 0:n]
            copy = remote(ref, ref, sends.at[5], back_recv.at[s], partner)
            pl.when(z == n)(copy.wait_recv)

    def project(s):
        product = matmul(T[s], WA[...].reshape(WIDTH, 256))
        E[s, 0, 8 : SPAN + 8, :] = product[:, 0:128]
        E[s, 1, 8 : SPAN + 8, :] = product[:, 128:256]
        product = matmul(T[s], WB[...].reshape(WIDTH, 384))
        E[s, 2, 8 : SPAN + 8, :] = product[:, 0:128]
        Z[s] = product[:, 128:256]
        DT[s] = product[:, 256:384]
        pl.when(sp < 15)(halo(s).start)

    def gate(s):
        for rows in tiles:
            Z[s, rows, :] = silu(Z[s, rows, :]) * jnp.exp(CUM[s, rows, :])

    def steps(s):
        for rows in tiles:
            step = DT[s, rows, :] + bias
            step = jnp.maximum(step, 0.0) + jnp.log1p(jnp.exp(-jnp.abs(step)))
            DT[s, rows, :] = step
            XS[s, rows, :] = (-(step * rate) / LENGTH).astype(BF16)
        for k in range(2):
            rows = slice(k * CHUNK, (k + 1) * CHUNK)
            CUM[s, rows, :] = matmul(ones_below, XS[s, rows, :])

    def conv_tail(s):
        convolve(s, tiles[1:])
        gains(s, 1)

    def conv_head(s):
        for k in range(3):
            E[s, k, 0:8, :] = jnp.where(sp == 0, 0.0, E[s, k, 0:8, :])
        convolve(s, tiles[:1])

    def convolve(s, some):
        for k in range(3):
            taps = [taps_ref[k, offset : offset + 1, :] for offset in range(CONV)]
            for rows in some:
                start = rows.start + 5
                running = taps[0] * E[s, k, start : start + ROWS, :]
                for offset in range(1, CONV):
                    first = start + offset
                    running = running + taps[offset] * E[s, k, first : first + ROWS, :]
                running = silu(running)
                if k == 0:
                    decayed = DT[s, rows, :] * jnp.exp(-CUM[s, rows, :])
                    XS[s, rows, :] = (running * decayed).astype(BF16)
                elif k == 1:
                    BS[s, rows, :] = running.astype(BF16)
                else:
                    CS[s, rows, :] = running.astype(BF16)

    def gains(s, k):
        rows = slice(k * CHUNK, (k + 1) * CHUNK)
        U[s, k] = matmul(BS[s, rows, :], XS[s, rows, :], ((0,), (0,)))

    def states(s):
        gains(s, 0)
        first, second = CUM[s, CHUNK - 1 : CHUNK, :], CUM[s, SPAN - 1 : SPAN, :]
        final = jnp.exp(second) * (jnp.exp(first) * U[s, 0] + U[s, 1])
        SS[s] = packed(final, first + second)
        share_row(s)

    def inside(s):
        for k in range(2):
            rows = slice(k * CHUNK, (k + 1) * CHUNK)
            scores = matmul(CS[s, rows, :], BS[s, rows, :], ((1,), (1,)))
            scores = jnp.where(lower, scores, 0.0).astype(BF16)
            part = matmul(scores, XS[s, rows, :])
            if k:
                grown = jnp.exp(CUM[s, CHUNK - 1 : CHUNK, :])
                part = part + grown * matmul(CS[s, rows, :], U[s, 0].astype(BF16))
            Y[s, rows, :] = part

    def scan(s):
        before, before_log = jnp.zeros((LANES, LANES), F32), jnp.zeros((1, LANES), F32)
        total, total_log = before, before_log
        for i in range(4):
            piece = RS[s, i].astype(F32)
            log = piece[LANES : LANES + 1]
            total = jnp.exp(log) * total + piece[0:LANES]
            total_log = total_log + log
            if i < 3:
                before = jnp.where(i + 1 == y, total, before)
                before_log = jnp.where(i + 1 == y, total_log, before_log)
        ROW[s, 0:LANES] = before
        ROW[s, LANES : LANES + 1] = jnp.exp(before_log)
        SR[s] = packed(total, total_log)
        share_up(s)

    def finish(s):
        total = jnp.zeros((LANES, LANES), F32)
        entering = total
        for i in range(3):
            piece = RR[s, i].astype(F32)
            total = jnp.exp(piece[LANES : LANES + 1]) * total + piece[0:LANES]
            entering = jnp.where(i + 1 == z, total, entering)
        entering = ROW[s, LANES : LANES + 1] * entering + ROW[s, 0:LANES]
        carried = matmul(CS[s], entering.astype(BF16))
        grown = jnp.exp(CUM[s, CHUNK - 1 : CHUNK, :])
        for i in range(8):
            rows = tiles[i]
            part = carried[rows] if i < 4 else grown * carried[rows]
            gated = (Y[s, rows, :] + part) * Z[s, rows, :]
            scale = lax.rsqrt(jnp.mean(gated * gated, axis=-1, keepdims=True) + epsilon)
            GT[s, rows, :] = (gated * scale * og_ref[...]).astype(BF16)
            if i % 4 == 3:
                for j in range(i - 3, i + 1):
                    pl.when(tp != j)(mix_copy(s, j).start)
        own(s).start()

    def mix_copy(s, i):
        return remote(
            GT.at[s, i * ROWS : (i + 1) * ROWS, :],
            G.at[s, :, pl.ds(own_columns, LANES)],
            sends.at[6],
            mix_recv.at[s // 2],
            (z, y, i // 2, i % 2),
        )

    def own(s):
        return pltpu.make_async_copy(
            GT.at[s, pl.ds(pl.multiple_of(tp * ROWS, ROWS), ROWS), :],
            G.at[s, :, pl.ds(own_columns, LANES)],
            local_sem.at[0],
        )

    def mixed_in(pair):
        ref = G.at[2 * pair : 2 * pair + 2, :, 0:896]
        remote(ref, ref, sends.at[6], mix_recv.at[pair], partner).wait_recv()

    def owns_in():
        ref = G.at[:, :, 0:LANES]
        pltpu.make_async_copy(ref, ref, local_sem.at[0]).wait()

    def multiply(first, last):
        gathered = G[first:last].reshape((last - first) * ROWS, WIDTH)
        result = matmul(gathered, O[...].reshape(WIDTH, WIDTH))
        out_ref[first:last] = result.astype(BF16).reshape(last - first, ROWS, WIDTH)

    def sent(ref, group):
        return remote(ref, ref, sends.at[group], pair_recv.at[0], partner)

    def drain():
        sent(T.at[:, 0:448, :], 0).wait_send()
        sent(T.at[0:3, 0:240, :], 1).wait_send()
        pl.when(sp < 15)(sent(E.at[:, :, 0:8, :], 3).wait_send)
        states_out()

    def ox_drain():
        sent(T.at[0:2, 0:448, :], 2).wait_send()

    def out_drain():
        sent(G.at[:, :, 0:896], 6).wait_send()

    token_pair(0)
    project(0)
    token_last(1)
    steps(0)
    conv_tail(0)
    token_near(3)
    oz.near()
    oz.last()
    out_own()
    token_pair(1)
    project(1)
    token_last(2)
    halo_in(0)
    conv_head(0)
    states(0)
    steps(1)
    conv_tail(1)
    halo_in(1)
    conv_head(1)
    states(1)
    token_last(3)
    token_pair(2)
    project(2)
    steps(2)
    conv_tail(2)
    token_pair(3)
    project(3)
    steps(3)
    conv_tail(3)
    halo_in(2)
    conv_head(2)
    states(2)
    out_near()
    state_in(0)
    scan(0)
    halo_in(3)
    conv_head(3)
    states(3)
    state_in(1)
    scan(1)
    gate(0)
    inside(0)
    gate(1)
    inside(1)
    back_in(0)
    finish(0)
    gate(2)
    inside(2)
    state_in(2)
    scan(2)
    gate(3)
    inside(3)
    back_in(1)
    finish(1)
    state_in(3)
    scan(3)
    back_in(2)
    finish(2)
    back_in(3)
    finish(3)
    out_last()
    drain()
    owns_in()
    mixed_in(0)
    out_pairs()
    ox_drain()
    multiply(0, 2)
    mixed_in(1)
    multiply(2, 4)

    out_drain()


def local(
    tokens,
    norm_gain,
    x_weight,
    z_weight,
    b_weight,
    c_weight,
    dt_weight,
    x_conv,
    b_conv,
    c_conv,
    dt_bias,
    decay_rate,
    out_gain,
    out_weight,
):
    hbm = pl.BlockSpec(memory_space=pltpu.HBM)
    dma = pltpu.SemaphoreType.DMA
    return pl.pallas_call(
        kernel,
        out_shape=pltpu.VMEM(tokens.shape, BF16),
        in_specs=[hbm] * 14,
        out_specs=pl.BlockSpec(memory_space=pltpu.VMEM),
        scratch_shapes=[
            pltpu.SMEM((2,), F32),
            pltpu.SMEM((2,), F32),
            pltpu.VMEM((SEQS, ROWS, WIDTH), BF16),
            pltpu.VMEM((1, WIDTH), F32),
            pltpu.VMEM((2, ROWS), BF16),
            pltpu.VMEM((3, CONV, LANES), F32),
            pltpu.VMEM((1, LANES), F32),
            pltpu.VMEM((SEQS, SPAN, WIDTH), BF16),
            pltpu.VMEM((4, 4, ROWS, 256), BF16),
            pltpu.VMEM((4, 4, ROWS, 384), BF16),
            pltpu.VMEM((4, 4, ROWS, LANES), BF16),
            pltpu.VMEM((2, 512, WIDTH), BF16),
            pltpu.VMEM((SEQS, 3, SPAN + 8, LANES), F32),
            pltpu.VMEM((SEQS, SPAN, LANES), F32),
            pltpu.VMEM((SEQS, SPAN, LANES), F32),
            pltpu.VMEM((SEQS, SPAN, LANES), F32),
            pltpu.VMEM((SEQS, SPAN, LANES), BF16),
            pltpu.VMEM((SEQS, SPAN, LANES), BF16),
            pltpu.VMEM((SEQS, SPAN, LANES), BF16),
            pltpu.VMEM((SEQS, SPAN, LANES), F32),
            pltpu.VMEM((SEQS, 2, LANES, LANES), F32),
            pltpu.VMEM((SEQS, LANES + 16, LANES), BF16),
            pltpu.VMEM((SEQS, 4, LANES + 16, LANES), BF16),
            pltpu.VMEM((SEQS, LANES + 16, LANES), BF16),
            pltpu.VMEM((SEQS, 4, LANES + 16, LANES), BF16),
            pltpu.VMEM((SEQS, LANES + 8, LANES), F32),
            pltpu.VMEM((SEQS, SPAN, LANES), BF16),
            pltpu.VMEM((SEQS, ROWS, WIDTH), BF16),
            dma((7,)),
            dma((27,)),
            dma((SEQS + 1,)),
            dma((SEQS,)),
            dma((SEQS,)),
            dma((SEQS,)),
            dma((2,)),
            dma((1,)),
            dma((8,)),
        ],
        compiler_params=pltpu.CompilerParams(
            collective_id=0, has_side_effects=True, vmem_limit_bytes=60 * 1024 * 1024
        ),
        name="mixer",
    )(
        dt_bias,
        decay_rate,
        tokens,
        norm_gain.reshape(1, -1),
        x_weight,
        z_weight,
        b_weight,
        c_weight,
        dt_weight.T,
        x_conv,
        b_conv,
        c_conv,
        out_gain.reshape(1, -1),
        out_weight.T,
    )


def solution(mesh):
    torus = Mesh(mesh.devices.reshape(4, 4, 4, 2), SP_TP)
    return jax.shard_map(
        local,
        mesh=torus,
        in_specs=(
            P(None, SP_TP, None),
            P(),
            P(SP, TP),
            P(SP, TP),
            P(SP, TP),
            P(SP, TP),
            P(SP, TP),
            P(None, TP),
            P(None, TP),
            P(None, TP),
            P(TP),
            P(TP),
            P(TP),
            P(TP, SP),
        ),
        out_specs=P(None, SP_TP, None),
        check_vma=False,
    )
```
